512 devices in a mesh: sp: 128 (over z, y, core), tp: 4 (over x).
Axes of the slice: x: 4, y: 8, z: 8, core: 2. Of those that a mesh axis runs over, the one named last changes fastest.
Arguments:
- tokens: bfloat16 [32768, 4096], P('sp'), may hold values from -6 to 6
- norm_gain: float32 [4096], replicated, may hold values from 0.1 to 1.9
- w_query: bfloat16 [4096, 512], P('sp', 'tp'), may hold values from -0.09375 to 0.09375
- w_key: bfloat16 [4096, 512], P('sp', 'tp'), may hold values from -0.09375 to 0.09375
- w_value: bfloat16 [4096, 1024], P('sp', 'tp'), may hold values from -0.09375 to 0.09375
- w_gates: bfloat16 [4096, 2, 2, 4], P(None, None, None, 'tp'), may hold values from -0.09375 to 0.09375
- input_bias: float32 [2, 4], P(None, 'tp'), may hold values from -2 to 90
- forget_bias: float32 [2, 4], P(None, 'tp'), as said below
- decay_shift: float32 [2, 32768, 4], P(None, 'sp', 'tp'), may hold values from -2.5 to 0
- head_gain: float32 [1024], P('tp'), may hold values from 0.1 to 1.9
- w_conv_b: bfloat16 [4096, 1024], P('sp', 'tp'), may hold values from -0.09375 to 0.09375
- w_conv_c: bfloat16 [4096, 1024], P('sp', 'tp'), may hold values from -0.09375 to 0.09375
- w_conv_in: bfloat16 [4096, 1024], P('sp', 'tp'), may hold values from -0.09375 to 0.09375
- conv_taps: bfloat16 [3, 1024], P(None, 'tp'), may hold values from -3.5 to 3.5
- w_out: bfloat16 [2048, 4096], P('sp', 'tp'), may hold values from -0.125 to 0.125
Outputs:
- mixed_out: bfloat16 [32768, 4096], P('sp', 'tp')
The draws below stay inside these ranges and needn't reach their ends.
Inputs may be any that keep to these rules, and one draw needn't show every extreme that they name: `forget_bias`: at most the natural logarithm of 32768 plus 2.
All inputs are finite; a program needn't handle non-finite values.
Results may differ from the reference program's by a relative error of at most 0.02.
Values may be sent and summed in bfloat16 or wider, within the bound.
No kernel may reach another device: no remote copies, remote signals or barrier semaphores. Data moves between devices by JAX's collectives and lax.ppermute only.
A program may use at most 128 MiB of HBM per device.

```python
import jax
import jax.numpy as jnp
from jax import lax

D = 4096
HEADS = 4
DQK = 128
DV = 256
BLOCK = 128
TOK_DEV = 256
BW = 1024
SEQ = 32768


def lasting_heads(key):
    shuffled = jax.random.permutation(jax.random.fold_in(key, 7), 2 * HEADS)
    keep_mask = shuffled < HEADS
    return keep_mask.reshape(2, HEADS)


def forget_values(key):
    lasting_mask = lasting_heads(key)
    quick_bias = jax.random.uniform(jax.random.fold_in(key, 11), (2, HEADS), jnp.float32, 3.5, 4.5)
    lasting = jnp.log(jnp.float32(SEQ)) + 1.5 + jax.random.uniform(jax.random.fold_in(key, 12), (2, HEADS), jnp.float32, -0.5, 0.5)
    return jnp.where(lasting_mask, lasting, quick_bias)


def draw_forget_bias(key, part):
    return forget_values(key)


def draw_decay_shift(key, part):
    decay_speed = jax.nn.softplus(-forget_values(key))
    blocks = SEQ // TOK_DEV
    multiplier = jnp.exp(jax.random.uniform(jax.random.fold_in(key, 13), (2, blocks, HEADS), jnp.float32, 0.0, jnp.log(4.0)))
    multiplier = jnp.repeat(multiplier, TOK_DEV, axis=1)
    locations = jax.random.randint(jax.random.fold_in(key, 14), (3, 2, 1, HEADS), 0, SEQ)
    loss_values = -jnp.log1p(-jax.random.uniform(jax.random.fold_in(key, 15), (3, 2, 1, HEADS), jnp.float32, 0.2, 0.5))
    token_positions = jnp.arange(SEQ, dtype=jnp.int32)[None, None, :, None]
    spike_groups = jnp.sum(jnp.where(token_positions == locations, loss_values, 0.0), axis=0)
    return -(multiplier - 1.0) * decay_speed[:, None, :] - spike_groups


def draw_input_bias(key, part):
    base_values = jax.random.uniform(key, (2, HEADS), jnp.float32, -2.0, 1.0)
    return base_values


def levels(stream_key, extent, pieces, low, top_value):
    loudness, own = 1.0, jax.random.fold_in(stream_key, 6)
    for position, shards_of in pieces:
        heights = jnp.exp(jax.random.uniform(jax.random.fold_in(own, position), (shards_of,), jnp.float32, low / len(pieces), top_value / len(pieces)))
        loudness = loudness * jnp.repeat(heights, extent[position] // shards_of).reshape([-1 if axis == position else 1 for axis in range(len(extent))])
    return loudness


def scatter_about(stream_key, shape, spread, most, split=(), held_as=jnp.bfloat16):
    loudness = levels(stream_key, shape, split, -0.22, 0.18) if split else 1.0
    values = jax.random.normal(stream_key, shape, jnp.float32) * spread * loudness
    return jnp.minimum(jnp.maximum(values, -most), most).astype(held_as)


def setup_inputs(seed: int = 0) -> dict:
    keys = jax.random.split(jax.random.key(seed), 16)
    return {
        "tokens": scatter_about(keys[0], (SEQ, D), 1.0, 6.0, ((0, 128),)),
        "norm_gain": jnp.clip(1.0 + 0.18 * jax.random.normal(keys[1], (D,), jnp.float32), 0.1, 1.9),
        "w_query": scatter_about(keys[2], (D, HEADS * DQK), D ** -0.5, 0.09375, ((0, 128), (1, 4))),
        "w_key": scatter_about(keys[3], (D, HEADS * DQK), D ** -0.5, 0.09375, ((0, 128), (1, 4))),
        "w_value": scatter_about(keys[4], (D, BW), D ** -0.5, 0.09375, ((0, 128), (1, 4))),
        "w_gates": scatter_about(keys[5], (D, 2, 2, HEADS), D ** -0.5, 0.09375, ((3, 4),)),
        "input_bias": draw_input_bias(jax.random.fold_in(keys[15], 71), 0),
        "forget_bias": draw_forget_bias(jax.random.fold_in(keys[15], 71), 0),
        "decay_shift": draw_decay_shift(jax.random.fold_in(keys[15], 71), 0),
        "head_gain": jnp.clip(1.0 + 0.18 * jax.random.normal(keys[9], (BW,), jnp.float32), 0.1, 1.9),
        "w_conv_b": scatter_about(keys[10], (D, BW), D ** -0.5, 0.09375, ((0, 128), (1, 4))),
        "w_conv_c": scatter_about(keys[11], (D, BW), D ** -0.5, 0.09375, ((0, 128), (1, 4))),
        "w_conv_in": scatter_about(keys[12], (D, BW), D ** -0.5, 0.09375, ((0, 128), (1, 4))),
        "conv_taps": scatter_about(keys[13], (3, BW), 3 ** -0.5, 3.5, ((1, 4),)),
        "w_out": scatter_about(keys[14], (2 * BW, D), (2 * BW) ** -0.5, 0.125, ((0, 128), (1, 4))),
    }


EPS = 1e-06
HIGH = lax.Precision.HIGHEST

def row_norm(tokens, norm_gain):
    values = tokens.astype(jnp.float32)
    inverse_rms = lax.rsqrt(lax.optimization_barrier(jnp.mean(values * values, axis=-1, keepdims=True)) + EPS)
    return (values * inverse_rms * norm_gain).astype(jnp.bfloat16)

def project(normed, weight):
    return jnp.dot(normed, weight, preferred_element_type=jnp.float32).astype(jnp.bfloat16)

def to_heads(source, head_count):
    length = source.shape[0]
    return source.astype(jnp.float32).reshape(length, head_count, -1).transpose(1, 0, 2)

def direction_pass(queries, keys_all, values_all, in_gate, log_forget):
    head_count, length = in_gate.shape
    block_count = length // BLOCK

    def blocked(source):
        shaped = source.reshape((head_count, block_count, BLOCK) + source.shape[2:])
        return jnp.moveaxis(shaped, 1, 0)
    lower_mask = jnp.tril(jnp.ones((BLOCK, BLOCK), dtype=bool))

    def advance(carried_state, inputs):
        memory, normer, stable = carried_state
        query_block, key_blk, value_blk, gate_blk, forget_blk = inputs
        cumulative = jnp.cumsum(forget_blk, axis=-1)
        log_weight = jnp.where(lower_mask, cumulative[:, :, None] - cumulative[:, None, :] + gate_blk[:, None, :], -jnp.inf)
        carried = cumulative + stable[:, None]
        running_max = jnp.maximum(carried, lax.optimization_barrier(jnp.max(log_weight, axis=-1)))
        scores = jnp.einsum('htd,hsd->hts', query_block, key_blk, precision=HIGH) * jnp.exp(log_weight - running_max[:, :, None])
        carry_weight = jnp.exp(carried - running_max)
        numerator = jnp.einsum('hts,hsv->htv', scores, value_blk, precision=HIGH) + carry_weight[:, :, None] * jnp.einsum('hvd,htd->htv', memory, query_block, precision=HIGH)
        denominator = lax.optimization_barrier(jnp.sum(scores, axis=-1)) + carry_weight * jnp.einsum('hd,htd->ht', normer, query_block, precision=HIGH)
        output = numerator / jnp.maximum(jnp.abs(denominator), jnp.exp(-running_max))[:, :, None]
        block_total = cumulative[:, -1]
        log_update = block_total[:, None] - cumulative + gate_blk
        new_stable = jnp.maximum(block_total + stable, lax.optimization_barrier(jnp.max(log_update, axis=-1)))
        update = jnp.exp(log_update - new_stable[:, None])
        carry_decay = jnp.exp(block_total + stable - new_stable)
        memory = carry_decay[:, None, None] * memory + jnp.einsum('hsv,hsd->hvd', value_blk * update[:, :, None], key_blk, precision=HIGH)
        normer = carry_decay[:, None] * normer + jnp.einsum('hs,hsd->hd', update, key_blk, precision=HIGH)
        return ((memory, normer, new_stable), output)
    starting_value = (jnp.zeros((head_count, DV, DQK), jnp.float32), jnp.zeros((head_count, DQK), jnp.float32), jnp.full((head_count,), -1e+30, jnp.float32))
    ignored, outputs = lax.scan(advance, starting_value, (blocked(queries), blocked(keys_all), blocked(values_all), blocked(in_gate), blocked(log_forget)))
    return jnp.moveaxis(outputs, 0, 1).reshape(head_count, length, DV)

def flipped(source):
    return jnp.flip(source, axis=1)

def reference(tokens, norm_gain, w_query, w_key, w_value, w_gates, input_bias, forget_bias, decay_shift, head_gain, w_conv_b, w_conv_c, w_conv_in, conv_taps, w_out):
    normed = row_norm(tokens, norm_gain)
    length = normed.shape[0]
    queries = to_heads(project(normed, w_query), HEADS) * DQK ** (-0.5)
    keys_all = to_heads(project(normed, w_key), HEADS)
    values_all = to_heads(project(normed, w_value), HEADS)
    gate_pre = jnp.dot(normed, w_gates.reshape(D, 4 * HEADS), preferred_element_type=jnp.float32).reshape(length, 2, 2, HEADS)
    summed = jnp.zeros((HEADS, length, DV), jnp.float32)
    for direction in range(2):
        in_gate = (gate_pre[:, direction, 0, :] + input_bias[direction]).T
        log_forget = (jax.nn.log_sigmoid(gate_pre[:, direction, 1, :] + forget_bias[direction]) + decay_shift[direction]).T
        if direction == 1:
            result = flipped(direction_pass(flipped(queries), flipped(keys_all), flipped(values_all), flipped(in_gate), flipped(log_forget)))
        else:
            result = direction_pass(queries, keys_all, values_all, in_gate, log_forget)
        summed = summed + result
    inverse_rms = lax.rsqrt(lax.optimization_barrier(jnp.mean(summed * summed, axis=-1, keepdims=True)) + EPS)
    lstm_out = ((summed * inverse_rms).transpose(1, 0, 2) * head_gain.reshape(HEADS, DV)).astype(jnp.bfloat16)
    gate_outer = project(normed, w_conv_b)
    gate_inner = project(normed, w_conv_c)
    conv_input = project(normed, w_conv_in)
    mixed_in = (gate_inner.astype(jnp.float32) * conv_input.astype(jnp.float32)).astype(jnp.bfloat16)
    padded = jnp.pad(mixed_in, ((1, 1), (0, 0))).astype(jnp.float32)
    taps_wide = conv_taps.astype(jnp.float32)
    filtered = taps_wide[0] * padded[:-2] + taps_wide[1] * padded[1:-1] + taps_wide[2] * padded[2:]
    conv_out = (gate_outer.astype(jnp.float32) * filtered).astype(jnp.bfloat16).reshape(length, HEADS, DV)
    joined = jnp.stack([lstm_out, conv_out], axis=2).reshape(length, 2 * HEADS * DV)
    return jnp.dot(joined, w_out, preferred_element_type=jnp.float32).astype(jnp.bfloat16)
```

```python
import jax
import jax.numpy as jnp
from jax import lax
from jax.sharding import Mesh
from jax.sharding import PartitionSpec as P

DQK = 128
DV = 256
SP = ("sp_0", "sp_1", "sp_2")
PLANE = ("sp_1", "sp_2")
EPS = 1e-06
LOWEST = -1e30
F32 = jnp.float32
BF16 = jnp.bfloat16


def row_norm(tokens, norm_gain):
    values = tokens.astype(F32)
    inverse_rms = lax.rsqrt(jnp.mean(values * values, axis=-1, keepdims=True) + EPS)
    return (values * inverse_rms * norm_gain).astype(BF16)


def swapped(value, axes):
    return lax.all_to_all(value, axes, split_axis=0, concat_axis=0, tiled=True)


def copies(value, axes, count):
    return swapped(jnp.broadcast_to(value, (count, *value.shape)), axes)


def neighbour_rows(normed):
    size = lax.axis_size(SP)
    up = [(i, i + 1) for i in range(size - 1)]
    before = lax.ppermute(normed[-1:], SP, up)
    after = lax.ppermute(normed[:1], SP, [(j, i) for i, j in up])
    return before, after


def combine_weights(total, most, plane, backward):
    planes, members = total.shape

    def before(a, b):
        return a > b if backward else a < b

    i = jnp.arange(members)
    k = jnp.arange(planes)
    own_total = lax.dynamic_index_in_dim(total, plane, 0, keepdims=False)
    own_most = lax.dynamic_index_in_dim(most, plane, 0, keepdims=False)
    earlier = before(i[None, :], i[:, None])
    between = before(i[:, None], i[None, :])[None] & earlier[:, None, :]
    inside = own_most[None, :] + jnp.sum(jnp.where(between, own_total, 0.0), -1)
    tail = most + jnp.sum(jnp.where(before(i[:, None], i[None, :]), total[:, None, :], 0.0), -1)
    plane_most = jnp.max(tail, -1)
    plane_total = jnp.sum(total, -1)
    plane_weight = jnp.exp(
        lax.dynamic_index_in_dim(tail, plane, 0, keepdims=False)
        - lax.dynamic_index_in_dim(plane_most, plane, 0, keepdims=False)
    )
    skipped = before(k[:, None], k[None, :]) & before(k, plane)[None, :]
    head = jnp.sum(jnp.where(earlier, own_total[None, :], 0.0), -1)
    outside = plane_most + jnp.sum(jnp.where(skipped, plane_total[None, :], 0.0), -1)
    outside = outside[None, :] + head[:, None]
    earlier_plane = before(k, plane)[None, :]
    inside = jnp.where(earlier, inside, LOWEST)
    outside = jnp.where(earlier_plane, outside, LOWEST)
    stable = jnp.maximum(jnp.max(inside, -1), jnp.max(outside, -1))
    inside = jnp.where(earlier, jnp.exp(inside - stable[:, None]), 0.0)
    outside = jnp.where(earlier_plane, jnp.exp(outside - stable[:, None]), 0.0)
    return inside, plane_weight, outside, stable


def body(
    tokens,
    norm_gain,
    w_query,
    w_key,
    w_value,
    w_gates,
    input_bias,
    forget_bias,
    decay_shift,
    head_gain,
    w_conv_b,
    w_conv_c,
    w_conv_in,
    conv_taps,
    w_out,
):
    length = tokens.shape[0]
    size = lax.axis_size(SP)
    planes = lax.axis_size("sp_0")
    members = size // planes
    plane = lax.axis_index("sp_0")
    member = lax.axis_index(PLANE)
    depth = w_out.shape[0]
    half = w_out.shape[1] // 2
    out_rows = jnp.concatenate([w_out[:, :half], w_out[:, half:]], axis=0)
    packed = jnp.concatenate(
        [w_key, w_value, w_query, w_conv_c, w_conv_in, w_conv_b, out_rows], axis=1
    )
    whole = lax.all_gather(packed, SP, axis=0, tiled=True)

    normed = row_norm(tokens, norm_gain)
    before, after = neighbour_rows(normed)
    gates = lax.dot_general(
        w_gates.reshape(-1, 4), normed, (((0,), (1,)), ((), ())), preferred_element_type=F32
    ).reshape(2, 2, length)
    in_gate = gates[:, 0] + input_bias
    log_forget = jax.nn.log_sigmoid(gates[:, 1] + forget_bias) + decay_shift[:, :, 0]
    running = jnp.stack(
        [jnp.cumsum(log_forget[0]), jnp.flip(jnp.cumsum(jnp.flip(log_forget[1])))]
    )
    total = jnp.stack([running[0, -1], running[1, 0]])
    log_update = total[:, None] - running + in_gate
    most = jnp.max(log_update, -1)
    update = jnp.exp(log_update - most[:, None])

    scalars = jnp.pad(jnp.concatenate([total, most]), (0, 124))[None]
    everyone = copies(scalars, SP, size).reshape(planes, members, 128)
    weights = [
        combine_weights(everyone[..., d], everyone[..., 2 + d], plane, d == 1) for d in range(2)
    ]
    inside, plane_weight, outside, stable = (jnp.stack(w) for w in zip(*weights))
    stable = lax.dynamic_index_in_dim(stable, member, 1, keepdims=False)

    keys_values = jnp.dot(normed, whole[:, :384], preferred_element_type=F32).astype(BF16)
    keys, values = keys_values[:, :DQK], keys_values[:, DQK:]
    weighted = keys.astype(F32)[None] * update[:, :, None]
    memory = jnp.einsum(
        "sv,dsk->dvk", values, weighted.astype(BF16), preferred_element_type=F32
    )
    normer = jnp.sum(weighted, axis=1)
    share = DV // members
    state = jnp.concatenate(
        [
            memory.reshape(2, members, share, DQK),
            jnp.broadcast_to(normer[:, None, None, :], (2, members, 1, DQK)),
        ],
        axis=2,
    ).astype(BF16)
    state = swapped(state.swapaxes(0, 1), PLANE).astype(F32)
    near = jnp.einsum("dij,jdrc->idrc", inside, state)
    plane_state = jnp.einsum("dj,jdrc->drc", plane_weight, state).astype(BF16)
    far = copies(plane_state, "sp_0", planes).astype(F32)
    start = (near + jnp.einsum("diz,zdrc->idrc", outside, far)).astype(BF16)
    start = swapped(start, PLANE)
    start_memory = start[:, :, :share].swapaxes(0, 1).reshape(2, DV, DQK)
    start_normer = start[0, :, share]

    queries = jnp.dot(normed, whole[:, 384:512], preferred_element_type=F32).astype(BF16)
    queries = (queries.astype(F32) * DQK ** (-0.5)).astype(BF16)
    products = lax.dot_general(
        queries, keys, (((1,), (1,)), ((), ())), preferred_element_type=F32
    )
    t = jnp.arange(length)
    seen = jnp.stack([t[:, None] >= t[None, :], t[:, None] <= t[None, :]])
    log_weight = jnp.where(
        seen, running[:, :, None] - running[:, None, :] + in_gate[:, None, :], -jnp.inf
    )
    carried = running + stable[:, None]
    highest = jnp.maximum(carried, jnp.max(log_weight, axis=-1))
    scores = products[None] * jnp.exp(log_weight - highest[..., None])
    carry_weight = jnp.exp(carried - highest)
    local = jnp.einsum(
        "dts,sv->dtv", scores.astype(BF16), values, preferred_element_type=F32
    )
    local_sum = jnp.sum(scores, -1)
    numerator = local + carry_weight[..., None] * jnp.einsum(
        "tk,dvk->dtv", queries, start_memory, preferred_element_type=F32
    )
    denominator = local_sum + carry_weight * jnp.einsum(
        "tk,dk->dt", queries, start_normer, preferred_element_type=F32
    )
    result = numerator / jnp.maximum(jnp.abs(denominator), jnp.exp(-highest))[..., None]
    summed = result[0] + result[1]
    inverse_rms = lax.rsqrt(jnp.mean(summed * summed, axis=-1, keepdims=True) + EPS)
    lstm_out = (summed * inverse_rms * head_gain).astype(BF16)

    inner = whole[:, 512:1024]
    pair = jnp.dot(normed, inner, preferred_element_type=F32).astype(BF16).astype(F32)
    mixed_in = (pair[:, :DV] * pair[:, DV:]).astype(BF16).astype(F32)
    edge = jnp.concatenate([before, after], axis=0)
    pair = jnp.dot(edge, inner, preferred_element_type=F32).astype(BF16).astype(F32)
    edge = (pair[:, :DV] * pair[:, DV:]).astype(BF16).astype(F32)
    padded = jnp.concatenate([edge[:1], mixed_in, edge[1:]], axis=0)
    taps = conv_taps.astype(F32)
    filtered = taps[0] * padded[:-2] + taps[1] * padded[1:-1] + taps[2] * padded[2:]
    outer = jnp.dot(normed, whole[:, 1024:1280], preferred_element_type=F32).astype(BF16)
    conv_out = (outer.astype(F32) * filtered).astype(BF16)

    joined = copies(jnp.concatenate([lstm_out, conv_out], axis=1), "tp", lax.axis_size("tp"))
    joined = joined.swapaxes(0, 1).reshape(length, -1)
    sides = whole[:, 1280:].reshape(size, 2, depth, half).swapaxes(0, 1).reshape(2, -1, half)
    return jnp.concatenate(
        [jnp.dot(joined, sides[s], preferred_element_type=F32).astype(BF16) for s in range(2)],
        axis=1,
    )


def solution(mesh):
    torus = Mesh(mesh.devices.reshape(8, 8, 2, mesh.shape["tp"]), (*SP, "tp"))
    placed = (
        P(SP, None),
        P(),
        P(SP, "tp"),
        P(SP, "tp"),
        P(SP, "tp"),
        P(None, None, None, "tp"),
        P(None, "tp"),
        P(None, "tp"),
        P(None, SP, "tp"),
        P("tp"),
        P(SP, "tp"),
        P(SP, "tp"),
        P(SP, "tp"),
        P(None, "tp"),
        P(SP, "tp"),
    )
    return jax.shard_map(body, mesh=torus, in_specs=placed, out_specs=P(SP, "tp"), check_vma=False)
```

```python
import jax
import jax.numpy as jnp
from jax import lax
from jax.experimental import pallas as pl
from jax.experimental.pallas import tpu as pltpu
from jax.sharding import Mesh
from jax.sharding import PartitionSpec as P

DQK = 128
DV = 256
SP = ("sp_0", "sp_1", "sp_2")
PLANE = ("sp_1", "sp_2")
CHIPS = ("sp_0", "sp_1")
EPS = 1e-06
LOWEST = -1e30
F32 = jnp.float32
BF16 = jnp.bfloat16


def row_norm(tokens, norm_gain):
    values = tokens.astype(F32)
    inverse_rms = lax.rsqrt(jnp.mean(values * values, axis=-1, keepdims=True) + EPS)
    return (values * inverse_rms * norm_gain).astype(BF16)


def swapped(value, axes):
    return lax.all_to_all(value, axes, split_axis=0, concat_axis=0, tiled=True)


def copies(value, axes, count):
    return swapped(jnp.broadcast_to(value, (count, *value.shape)), axes)


def neighbour_rows(normed):
    size = lax.axis_size(SP)
    up = [(i, i + 1) for i in range(size - 1)]
    before = lax.ppermute(normed[-1:], SP, up)
    after = lax.ppermute(normed[:1], SP, [(j, i) for i, j in up])
    return before, after


ROWS = 48
NORMERS = 32
NUMBERS = (34, 40)


def in_terms(number):
    high = number.astype(BF16)
    rest = number - high.astype(F32)
    middle = rest.astype(BF16)
    low = (rest - middle.astype(F32)).astype(BF16)
    return [high, middle, low]


def from_terms(block, row):
    return block[row : row + 1] + block[row + 1 : row + 2] + block[row + 2 : row + 3]


def numbered_rows(normers, numbers):
    rows = [n.astype(BF16) for n in normers]
    for pair in numbers:
        for number in pair:
            rows += in_terms(number)
    rows.append(jnp.zeros((ROWS - NORMERS - len(rows), 128), BF16))
    return jnp.concatenate(rows, axis=0)


def state_kernel(part_ref, normed_ref, weight_ref, update_ref, number_ref, state_ref, key_ref, value_ref):
    both = part_ref[...] + jnp.dot(normed_ref[...], weight_ref[...], preferred_element_type=F32)
    both = both.astype(BF16)
    keys, values = both[:, :DQK], both[:, DQK:]
    key_ref[...] = keys
    value_ref[...] = values
    members = state_ref.shape[0]
    share = DV // members
    normers = []
    for d in range(2):
        weighted = keys.astype(F32) * update_ref[:, d : d + 1]
        normers.append(jnp.sum(weighted, axis=0, keepdims=True))
        memory = lax.dot_general(
            values, weighted.astype(BF16), (((0,), (0,)), ((), ())), preferred_element_type=F32
        )
        state_ref[:, d * share : (d + 1) * share, :] = memory.astype(BF16).reshape(
            members, share, DQK
        )
    numbers = [[number_ref[2 * d + n : 2 * d + n + 1] for n in range(2)] for d in range(2)]
    rows = numbered_rows(normers, numbers)
    for j in range(members):
        state_ref[j, NORMERS:, :] = rows


def passed(carry, block, d):
    memory, normer, total, most = carry
    block_total = from_terms(block, NUMBERS[d])
    block_most = from_terms(block, NUMBERS[d] + 3)
    new = jnp.maximum(most + block_total, block_most)
    old_weight = jnp.exp(most + block_total - new)
    block_weight = jnp.exp(block_most - new)
    share = memory.shape[0]
    memory = old_weight * memory + block_weight * block[d * share : (d + 1) * share]
    normer = old_weight * normer + block_weight * block[NORMERS + d : NORMERS + d + 1]
    return memory, normer, total + block_total, new


def nothing(share):
    row = jnp.zeros((1, 128), F32)
    return jnp.zeros((share, 128), F32), row, row, jnp.full((1, 128), LOWEST, F32)


def plane_kernel(state_ref, near_ref, plane_ref):
    members = state_ref.shape[0]
    share = NORMERS // 2
    ends = []
    for d in range(2):
        carry = nothing(share)
        for i in reversed(range(members)) if d else range(members):
            near_ref[i, d * share : (d + 1) * share, :] = carry[0]
            for n in range(3):
                near_ref[i, NORMERS + 2 * n + d : NORMERS + 2 * n + d + 1, :] = carry[1 + n]
            carry = passed(carry, state_ref[i].astype(F32), d)
        ends.append(carry)
    rows = numbered_rows([e[1] for e in ends], [e[2:] for e in ends])
    for z in range(plane_ref.shape[0]):
        for d in range(2):
            plane_ref[z, d * share : (d + 1) * share, :] = ends[d][0].astype(BF16)
        plane_ref[z, NORMERS:, :] = rows


def far_kernel(place_ref, near_ref, planes_ref, start_ref):
    planes, members = planes_ref.shape[0], near_ref.shape[0]
    share = NORMERS // 2
    place = place_ref[0]
    far = []
    for d in range(2):
        carry = nothing(share)
        for z in reversed(range(planes)) if d else range(planes):
            earlier = (z > place) if d else (z < place)
            after = passed(carry, planes_ref[z].astype(F32), d)
            carry = tuple(jnp.where(earlier, a, c) for a, c in zip(after, carry))
        far.append(carry)
    for i in range(members):
        normers, numbers = [], []
        for d in range(2):
            memory, normer, _, most = far[d]
            at = [NORMERS + 2 * n + d for n in range(3)]
            near_normer, head, near_most = (near_ref[i, r : r + 1, :] for r in at)
            moved = most + head
            new = jnp.maximum(moved, near_most)
            far_weight = jnp.exp(moved - new)
            near_weight = jnp.exp(near_most - new)
            near = near_ref[i, d * share : (d + 1) * share, :]
            start_ref[i, d * share : (d + 1) * share, :] = (
                near_weight * near + far_weight * memory
            ).astype(BF16)
            normers.append(near_weight * near_normer + far_weight * normer)
            numbers.append([new])
        rows = [n.astype(BF16) for n in normers]
        for (number,) in numbers:
            rows += in_terms(number)
        rows.append(jnp.zeros((ROWS - NORMERS - len(rows), 128), BF16))
        start_ref[i, NORMERS:, :] = jnp.concatenate(rows, axis=0)


def read_kernel(query_ref, key_ref, value_ref, column_ref, row_ref, gain_ref, start_ref, out_ref):
    length = query_ref.shape[0]
    queries = query_ref[...]
    values = value_ref[...]
    scale = DQK ** (-0.5)
    products = scale * lax.dot_general(
        queries, key_ref[...], (((1,), (1,)), ((), ())), preferred_element_type=F32
    )
    t = lax.broadcasted_iota(jnp.int32, (length, length), 0)
    s = lax.broadcasted_iota(jnp.int32, (length, length), 1)
    share = NORMERS // 2
    last = start_ref[0, NORMERS:, :].astype(F32)
    summed = None
    for d in range(2):
        memory = start_ref[:, d * share : (d + 1) * share, :].reshape(DV, DQK)
        normer = last[d : d + 1]
        stable = from_terms(last, 2 + 3 * d)[:, :1]
        running = column_ref[:, d : d + 1]
        seen = (t <= s) if d else (t >= s)
        log_weight = jnp.where(
            seen, running - row_ref[d : d + 1, :] + row_ref[2 + d : 3 + d, :], -jnp.inf
        )
        carried = running + stable
        highest = jnp.maximum(carried, jnp.max(log_weight, axis=-1, keepdims=True))
        scores = products * jnp.exp(log_weight - highest)
        carry_weight = scale * jnp.exp(carried - highest)
        numerator = jnp.dot(scores.astype(BF16), values, preferred_element_type=F32)
        numerator += carry_weight * lax.dot_general(
            queries, memory, (((1,), (1,)), ((), ())), preferred_element_type=F32
        )
        denominator = jnp.sum(scores, axis=-1, keepdims=True)
        denominator += carry_weight * jnp.sum(
            queries.astype(F32) * normer, axis=-1, keepdims=True
        )
        result = numerator / jnp.maximum(jnp.abs(denominator), jnp.exp(-highest))
        summed = result if summed is None else summed + result
    inverse_rms = lax.rsqrt(jnp.mean(summed * summed, axis=-1, keepdims=True) + EPS)
    out_ref[...] = (summed * inverse_rms * gain_ref[...]).astype(BF16)


def on_core(kernel, out, *operands, scalars=0):
    vmem = pl.BlockSpec(memory_space=pltpu.VMEM)
    smem = pl.BlockSpec(memory_space=pltpu.SMEM)
    return pl.pallas_call(
        kernel,
        out_shape=out,
        in_specs=[smem] * scalars + [vmem] * (len(operands) - scalars),
        out_specs=jax.tree.map(lambda _: vmem, out),
        compiler_params=pltpu.CompilerParams(vmem_limit_bytes=40 * 2**20),
    )(*operands)


def body(
    tokens,
    norm_gain,
    w_query,
    w_key,
    w_value,
    w_gates,
    input_bias,
    forget_bias,
    decay_shift,
    head_gain,
    w_conv_b,
    w_conv_c,
    w_conv_in,
    conv_taps,
    w_out,
):
    length = tokens.shape[0]
    size = lax.axis_size(SP)
    planes = lax.axis_size("sp_0")
    members = size // planes
    plane = lax.axis_index("sp_0")
    depth = w_out.shape[0]
    half = w_out.shape[1] // 2
    out_rows = jnp.concatenate([w_out[:, :half], w_out[:, half:]], axis=0)
    packed = jnp.concatenate([w_query, w_conv_c, w_conv_in, w_conv_b, out_rows], axis=1)
    whole = lax.all_gather(packed, SP, axis=0, tiled=True)
    core = lax.axis_index("sp_2")
    mine = copies(jnp.concatenate([w_key, w_value], axis=1), CHIPS, size // 2)
    mine = mine.reshape(-1, mine.shape[-1])
    other = lax.ppermute(mine, "sp_2", [(0, 1), (1, 0)])

    normed = row_norm(tokens, norm_gain)
    paired = normed.reshape(length, size // 2, 2, -1)
    even, odd = (paired[:, :, k].reshape(length, -1) for k in range(2))
    normed_mine = jnp.where(core == 0, even, odd)
    normed_other = jnp.where(core == 0, odd, even)
    before, after = neighbour_rows(normed)
    gates = lax.dot_general(
        w_gates.reshape(-1, 4), normed, (((0,), (1,)), ((), ())), preferred_element_type=F32
    ).reshape(2, 2, length)
    in_gate = gates[:, 0] + input_bias
    log_forget = jax.nn.log_sigmoid(gates[:, 1] + forget_bias) + decay_shift[:, :, 0]
    running = jnp.stack(
        [jnp.cumsum(log_forget[0]), jnp.flip(jnp.cumsum(jnp.flip(log_forget[1])))]
    )
    total = jnp.stack([running[0, -1], running[1, 0]])
    log_update = total[:, None] - running + in_gate
    most = jnp.max(log_update, -1)
    update = jnp.exp(log_update - most[:, None])

    numbers = jnp.stack([total[0], most[0], total[1], most[1]])
    numbers = jnp.broadcast_to(numbers[:, None], (4, 128))
    part = jnp.dot(normed_mine, mine, preferred_element_type=F32)
    block = jax.ShapeDtypeStruct((members, ROWS, 128), BF16)
    state, keys, values = on_core(
        state_kernel,
        (
            block,
            jax.ShapeDtypeStruct((length, DQK), BF16),
            jax.ShapeDtypeStruct((length, DV), BF16),
        ),
        part,
        normed_other,
        other,
        update.T,
        numbers,
    )
    state = swapped(state, PLANE)
    near, plane_state = on_core(
        plane_kernel,
        (
            jax.ShapeDtypeStruct((members, ROWS, 128), F32),
            jax.ShapeDtypeStruct((planes, ROWS, 128), BF16),
        ),
        state,
    )
    far = swapped(plane_state, "sp_0")
    start = on_core(far_kernel, block, plane[None], near, far, scalars=1)
    start = swapped(start, PLANE)
    queries = jnp.dot(normed, whole[:, :128], preferred_element_type=F32).astype(BF16)
    lstm_out = on_core(
        read_kernel,
        jax.ShapeDtypeStruct((length, DV), BF16),
        queries,
        keys,
        values,
        running.T,
        jnp.concatenate([running, in_gate], axis=0),
        head_gain[None],
        start,
    )

    inner = whole[:, 128:640]
    pair = jnp.dot(normed, inner, preferred_element_type=F32).astype(BF16).astype(F32)
    mixed_in = (pair[:, :DV] * pair[:, DV:]).astype(BF16).astype(F32)
    edge = jnp.concatenate([before, after], axis=0)
    pair = jnp.dot(edge, inner, preferred_element_type=F32).astype(BF16).astype(F32)
    edge = (pair[:, :DV] * pair[:, DV:]).astype(BF16).astype(F32)
    padded = jnp.concatenate([edge[:1], mixed_in, edge[1:]], axis=0)
    taps = conv_taps.astype(F32)
    filtered = taps[0] * padded[:-2] + taps[1] * padded[1:-1] + taps[2] * padded[2:]
    outer = jnp.dot(normed, whole[:, 640:896], preferred_element_type=F32).astype(BF16)
    conv_out = (outer.astype(F32) * filtered).astype(BF16)

    joined = copies(jnp.concatenate([lstm_out, conv_out], axis=1), "tp", lax.axis_size("tp"))
    joined = joined.swapaxes(0, 1).reshape(length, -1)
    sides = whole[:, 896:].reshape(size, 2, depth, half).swapaxes(0, 1).reshape(2, -1, half)
    return jnp.concatenate(
        [jnp.dot(joined, sides[s], preferred_element_type=F32).astype(BF16) for s in range(2)],
        axis=1,
    )


def solution(mesh):
    torus = Mesh(mesh.devices.reshape(8, 8, 2, mesh.shape["tp"]), (*SP, "tp"))
    placed = (
        P(SP, None),
        P(),
        P(SP, "tp"),
        P(SP, "tp"),
        P(SP, "tp"),
        P(None, None, None, "tp"),
        P(None, "tp"),
        P(None, "tp"),
        P(None, SP, "tp"),
        P("tp"),
        P(SP, "tp"),
        P(SP, "tp"),
        P(SP, "tp"),
        P(None, "tp"),
        P(SP, "tp"),
    )
    return jax.shard_map(body, mesh=torus, in_specs=placed, out_specs=P(SP, "tp"), check_vma=False)
```

```python
import jax
import jax.numpy as jnp
from jax import lax
from jax.experimental import pallas as pl
from jax.experimental.pallas import tpu as pltpu
from jax.sharding import Mesh
from jax.sharding import PartitionSpec as P

DQK = 128
DV = 256
SP = ("sp_0", "sp_1", "sp_2")
PLANE = ("sp_1", "sp_2")
EPS = 1e-06
LOWEST = -1e30
F32 = jnp.float32
BF16 = jnp.bfloat16


def row_norm(tokens, norm_gain):
    values = tokens.astype(F32)
    inverse_rms = lax.rsqrt(jnp.mean(values * values, axis=-1, keepdims=True) + EPS)
    return (values * inverse_rms * norm_gain).astype(BF16)


def swapped(value, axes):
    return lax.all_to_all(value, axes, split_axis=0, concat_axis=0, tiled=True)


def copies(value, axes, count):
    return swapped(jnp.broadcast_to(value, (count, *value.shape)), axes)


def neighbour_rows(normed):
    size = lax.axis_size(SP)
    up = [(i, i + 1) for i in range(size - 1)]
    before = lax.ppermute(normed[-1:], SP, up)
    after = lax.ppermute(normed[:1], SP, [(j, i) for i, j in up])
    return before, after


ROWS = 48
NORMERS = 32
NUMBERS = (34, 40)


def in_terms(number):
    high = number.astype(BF16)
    rest = number - high.astype(F32)
    middle = rest.astype(BF16)
    low = (rest - middle.astype(F32)).astype(BF16)
    return [high, middle, low]


def from_terms(block, row):
    return block[row : row + 1] + block[row + 1 : row + 2] + block[row + 2 : row + 3]


def numbered_rows(normers, numbers):
    rows = [n.astype(BF16) for n in normers]
    for pair in numbers:
        for number in pair:
            rows += in_terms(number)
    rows.append(jnp.zeros((ROWS - NORMERS - len(rows), 128), BF16))
    return jnp.concatenate(rows, axis=0)


def state_kernel(place_ref, normed_ref, update_ref, number_ref, *refs):
    pieces = (refs[:4], refs[4:8])
    state_ref, key_ref, value_ref, weight_ref = refs[8:]
    core, row = place_ref[0], place_ref[1]
    pair, odd = row // 2, row % 2
    found = (pair, (pair + 3 - 2 * odd) % 4, (pair + 1 + 2 * odd) % 4, (pair + 2) % 4)
    depth = refs[0].shape[2]
    for side in range(2):
        cell = 1 - core if side else core
        for piece, at in zip(pieces[side], found):
            for y in range(2):
                for z in range(piece.shape[1]):
                    start = (((z * 4 + at) * 2 + y) * 2 + cell) * depth
                    weight_ref[pl.ds(pl.multiple_of(start, depth), depth), :] = piece[y, z]
    both = jnp.dot(normed_ref[...], weight_ref[...], preferred_element_type=F32)
    both = both.astype(BF16)
    keys, values = both[:, :DQK], both[:, DQK:]
    key_ref[...] = keys
    value_ref[...] = values
    members = state_ref.shape[0]
    share = DV // members
    normers = []
    for d in range(2):
        weighted = keys.astype(F32) * update_ref[:, d : d + 1]
        normers.append(jnp.sum(weighted, axis=0, keepdims=True))
        memory = lax.dot_general(
            values, weighted.astype(BF16), (((0,), (0,)), ((), ())), preferred_element_type=F32
        )
        state_ref[:, d * share : (d + 1) * share, :] = memory.astype(BF16).reshape(
            members, share, DQK
        )
    numbers = [[number_ref[2 * d + n : 2 * d + n + 1] for n in range(2)] for d in range(2)]
    rows = numbered_rows(normers, numbers)
    for j in range(members):
        state_ref[j, NORMERS:, :] = rows


def passed(carry, block, d):
    memory, normer, total, most = carry
    block_total = from_terms(block, NUMBERS[d])
    block_most = from_terms(block, NUMBERS[d] + 3)
    new = jnp.maximum(most + block_total, block_most)
    old_weight = jnp.exp(most + block_total - new)
    block_weight = jnp.exp(block_most - new)
    share = memory.shape[0]
    memory = old_weight * memory + block_weight * block[d * share : (d + 1) * share]
    normer = old_weight * normer + block_weight * block[NORMERS + d : NORMERS + d + 1]
    return memory, normer, total + block_total, new


def nothing(share):
    row = jnp.zeros((1, 128), F32)
    return jnp.zeros((share, 128), F32), row, row, jnp.full((1, 128), LOWEST, F32)


def plane_kernel(state_ref, near_ref, plane_ref):
    members = state_ref.shape[0]
    share = NORMERS // 2
    ends = []
    for d in range(2):
        carry = nothing(share)
        for i in reversed(range(members)) if d else range(members):
            near_ref[i, d * share : (d + 1) * share, :] = carry[0]
            for n in range(3):
                near_ref[i, NORMERS + 2 * n + d : NORMERS + 2 * n + d + 1, :] = carry[1 + n]
            carry = passed(carry, state_ref[i].astype(F32), d)
        ends.append(carry)
    rows = numbered_rows([e[1] for e in ends], [e[2:] for e in ends])
    for z in range(plane_ref.shape[0]):
        for d in range(2):
            plane_ref[z, d * share : (d + 1) * share, :] = ends[d][0].astype(BF16)
        plane_ref[z, NORMERS:, :] = rows


def far_kernel(place_ref, near_ref, planes_ref, start_ref):
    planes, members = planes_ref.shape[0], near_ref.shape[0]
    share = NORMERS // 2
    place = place_ref[0]
    far = []
    for d in range(2):
        carry = nothing(share)
        for z in reversed(range(planes)) if d else range(planes):
            earlier = (z > place) if d else (z < place)
            after = passed(carry, planes_ref[z].astype(F32), d)
            carry = tuple(jnp.where(earlier, a, c) for a, c in zip(after, carry))
        far.append(carry)
    for i in range(members):
        normers, numbers = [], []
        for d in range(2):
            memory, normer, _, most = far[d]
            at = [NORMERS + 2 * n + d for n in range(3)]
            near_normer, head, near_most = (near_ref[i, r : r + 1, :] for r in at)
            moved = most + head
            new = jnp.maximum(moved, near_most)
            far_weight = jnp.exp(moved - new)
            near_weight = jnp.exp(near_most - new)
            near = near_ref[i, d * share : (d + 1) * share, :]
            start_ref[i, d * share : (d + 1) * share, :] = (
                near_weight * near + far_weight * memory
            ).astype(BF16)
            normers.append(near_weight * near_normer + far_weight * normer)
            numbers.append([new])
        rows = [n.astype(BF16) for n in normers]
        for (number,) in numbers:
            rows += in_terms(number)
        rows.append(jnp.zeros((ROWS - NORMERS - len(rows), 128), BF16))
        start_ref[i, NORMERS:, :] = jnp.concatenate(rows, axis=0)


def read_kernel(query_ref, key_ref, value_ref, column_ref, row_ref, gain_ref, start_ref, out_ref):
    length = query_ref.shape[0]
    queries = query_ref[...]
    values = value_ref[...]
    scale = DQK ** (-0.5)
    products = scale * lax.dot_general(
        queries, key_ref[...], (((1,), (1,)), ((), ())), preferred_element_type=F32
    )
    t = lax.broadcasted_iota(jnp.int32, (length, length), 0)
    s = lax.broadcasted_iota(jnp.int32, (length, length), 1)
    share = NORMERS // 2
    last = start_ref[0, NORMERS:, :].astype(F32)
    summed = None
    for d in range(2):
        memory = start_ref[:, d * share : (d + 1) * share, :].reshape(DV, DQK)
        normer = last[d : d + 1]
        stable = from_terms(last, 2 + 3 * d)[:, :1]
        running = column_ref[:, d : d + 1]
        seen = (t <= s) if d else (t >= s)
        log_weight = jnp.where(
            seen, running - row_ref[d : d + 1, :] + row_ref[2 + d : 3 + d, :], -jnp.inf
        )
        carried = running + stable
        highest = jnp.maximum(carried, jnp.max(log_weight, axis=-1, keepdims=True))
        scores = products * jnp.exp(log_weight - highest)
        carry_weight = scale * jnp.exp(carried - highest)
        numerator = jnp.dot(scores.astype(BF16), values, preferred_element_type=F32)
        numerator += carry_weight * lax.dot_general(
            queries, memory, (((1,), (1,)), ((), ())), preferred_element_type=F32
        )
        denominator = jnp.sum(scores, axis=-1, keepdims=True)
        denominator += carry_weight * jnp.sum(
            queries.astype(F32) * normer, axis=-1, keepdims=True
        )
        result = numerator / jnp.maximum(jnp.abs(denominator), jnp.exp(-highest))
        summed = result if summed is None else summed + result
    inverse_rms = lax.rsqrt(jnp.mean(summed * summed, axis=-1, keepdims=True) + EPS)
    out_ref[...] = (summed * inverse_rms * gain_ref[...]).astype(BF16)


def project_kernel(normed_ref, weight_ref, tap_ref, query_ref, conv_ref, total_ref):
    step = pl.program_id(0)
    product = jnp.dot(normed_ref[...], weight_ref[...], preferred_element_type=F32)

    @pl.when(step == 0)
    def _():
        total_ref[...] = product

    @pl.when(step > 0)
    def _():
        total_ref[...] += product

    @pl.when(step == pl.num_programs(0) - 1)
    def _():
        length = query_ref.shape[0]
        query_ref[...] = total_ref[:length, :DQK].astype(BF16)
        inner = total_ref[:, DQK : DQK + DV].astype(BF16).astype(F32)
        given = total_ref[:, DQK + DV : DQK + 2 * DV].astype(BF16).astype(F32)
        outer = total_ref[:length, DQK + 2 * DV :].astype(BF16).astype(F32)
        mixed = (inner * given).astype(BF16).astype(F32)
        here = mixed[:length]
        at = lax.broadcasted_iota(jnp.int32, (length, DV), 0)
        before = jnp.where(at == 0, mixed[length : length + 1], pltpu.roll(here, 1, 0))
        after = jnp.where(
            at == length - 1, mixed[length + 1 : length + 2], pltpu.roll(here, length - 1, 0)
        )
        taps = tap_ref[...].astype(F32)
        filtered = taps[0:1] * before + taps[1:2] * here + taps[2:3] * after
        conv_ref[...] = (outer * filtered).astype(BF16)


def projected(normed, whole, taps, length):
    rows, features = normed.shape
    wide = DQK + 3 * DV
    depth = 512
    return pl.pallas_call(
        project_kernel,
        grid=(features // depth,),
        in_specs=[
            pl.BlockSpec((rows, depth), lambda k: (0, k)),
            pl.BlockSpec((depth, wide), lambda k: (k, 0)),
            pl.BlockSpec(taps.shape, lambda k: (0, 0)),
        ],
        out_specs=[
            pl.BlockSpec((length, DQK), lambda k: (0, 0)),
            pl.BlockSpec((length, DV), lambda k: (0, 0)),
        ],
        out_shape=[
            jax.ShapeDtypeStruct((length, DQK), BF16),
            jax.ShapeDtypeStruct((length, DV), BF16),
        ],
        scratch_shapes=[pltpu.VMEM((rows, wide), F32)],
        compiler_params=pltpu.CompilerParams(vmem_limit_bytes=40 * 2**20),
    )(normed, whole, taps)


def output_kernel(place_ref, joined_ref, *refs):
    weights, rest = refs[:4], refs[4:]
    joined = jnp.concatenate([joined_ref[0], joined_ref[1]], axis=1)
    half = 4 * weights[0].shape[-1]
    for side in range(2):
        weight = jnp.concatenate(
            [w[:, side].reshape(joined.shape[1], w.shape[-1]) for w in weights], axis=1
        )
        product = jnp.dot(joined, weight, preferred_element_type=F32)
        at = slice(side * half, (side + 1) * half)
        if len(rest) == 1:
            rest[0][:, at] = product
        else:
            rest[1][:, at] = (rest[0][:, at] + product).astype(BF16)


def output(joined, whole, pair, first_column, earlier=None):
    _, length, width = joined.shape
    devices, sides, depth, _ = whole.shape
    share = 2 * width // depth

    def column(n):
        return pl.BlockSpec(
            (share, sides, depth, 128), lambda i, p, n=n: (p[0], 0, 0, first_column // 128 + n)
        )

    wide = 2 * 512
    flat = pl.BlockSpec((length, wide), lambda i, p: (0, 0))
    return pl.pallas_call(
        output_kernel,
        grid_spec=pltpu.PrefetchScalarGridSpec(
            num_scalar_prefetch=1,
            grid=(1,),
            in_specs=[pl.BlockSpec(joined.shape, lambda i, p: (0, 0, 0))]
            + [column(n) for n in range(4)]
            + [flat] * (earlier is not None),
            out_specs=flat,
        ),
        out_shape=jax.ShapeDtypeStruct((length, wide), F32 if earlier is None else BF16),
        compiler_params=pltpu.CompilerParams(vmem_limit_bytes=40 * 2**20),
    )(pair, joined, *([whole] * 4), *([] if earlier is None else [earlier]))


def pairs(size, odd):
    return [e for i in range(odd, size + odd, 2) for e in ((i % size, (i + 1) % size), ((i + 1) % size, i % size))]


def in_order(own, other, second):
    return jnp.where(second, jnp.stack([other, own]), jnp.stack([own, other]))


def on_core(kernel, out, *operands, scalars=0, scratch=()):
    vmem = pl.BlockSpec(memory_space=pltpu.VMEM)
    smem = pl.BlockSpec(memory_space=pltpu.SMEM)
    return pl.pallas_call(
        kernel,
        out_shape=out,
        in_specs=[smem] * scalars + [vmem] * (len(operands) - scalars),
        out_specs=jax.tree.map(lambda _: vmem, out),
        scratch_shapes=scratch,
        compiler_params=pltpu.CompilerParams(vmem_limit_bytes=40 * 2**20),
    )(*operands)


def body(
    tokens,
    norm_gain,
    w_query,
    w_key,
    w_value,
    w_gates,
    input_bias,
    forget_bias,
    decay_shift,
    head_gain,
    w_conv_b,
    w_conv_c,
    w_conv_in,
    conv_taps,
    w_out,
):
    length = tokens.shape[0]
    size = lax.axis_size(SP)
    planes = lax.axis_size("sp_0")
    members = size // planes
    plane = lax.axis_index("sp_0")
    depth = w_out.shape[0]
    half = w_out.shape[1] // 2
    out_rows = jnp.concatenate([w_out[:, :half], w_out[:, half:]], axis=0)
    packed = jnp.concatenate([w_query, w_conv_c, w_conv_in, w_conv_b, out_rows], axis=1)
    whole = lax.all_gather(packed, SP, axis=0, tiled=True)
    core = lax.axis_index("sp_2")
    row = lax.axis_index("sp_1")
    rows = lax.axis_size("sp_1")
    first, second = pairs(rows, 0), pairs(rows, 1)
    block = copies(jnp.concatenate([w_key, w_value], axis=1), "sp_0", planes)
    pieces = [in_order(block, lax.ppermute(block, "sp_1", first), row % 2 == 1)]
    for ring in (second, first, second):
        pieces.append(lax.ppermute(pieces[-1], "sp_1", ring))
    pieces += [lax.ppermute(p, "sp_2", pairs(2, 0)[:2]) for p in pieces]

    normed = row_norm(tokens, norm_gain)
    before, after = neighbour_rows(normed)
    edges = jnp.zeros((14, normed.shape[1]), BF16)
    extended = jnp.concatenate([normed, before, after, edges], axis=0)
    gates = lax.dot_general(
        w_gates.reshape(-1, 4), normed, (((0,), (1,)), ((), ())), preferred_element_type=F32
    ).reshape(2, 2, length)
    in_gate = gates[:, 0] + input_bias
    log_forget = jax.nn.log_sigmoid(gates[:, 1] + forget_bias) + decay_shift[:, :, 0]
    running = jnp.stack(
        [jnp.cumsum(log_forget[0]), jnp.flip(jnp.cumsum(jnp.flip(log_forget[1])))]
    )
    total = jnp.stack([running[0, -1], running[1, 0]])
    log_update = total[:, None] - running + in_gate
    most = jnp.max(log_update, -1)
    update = jnp.exp(log_update - most[:, None])

    numbers = jnp.stack([total[0], most[0], total[1], most[1]])
    numbers = jnp.broadcast_to(numbers[:, None], (4, 128))
    block = jax.ShapeDtypeStruct((members, ROWS, 128), BF16)
    state, keys, values = on_core(
        state_kernel,
        (
            block,
            jax.ShapeDtypeStruct((length, DQK), BF16),
            jax.ShapeDtypeStruct((length, DV), BF16),
        ),
        jnp.stack([core, row]),
        normed,
        update.T,
        numbers,
        *pieces,
        scalars=1,
        scratch=[pltpu.VMEM((normed.shape[1], DQK + DV), BF16)],
    )
    state = swapped(state, PLANE)
    near, plane_state = on_core(
        plane_kernel,
        (
            jax.ShapeDtypeStruct((members, ROWS, 128), F32),
            jax.ShapeDtypeStruct((planes, ROWS, 128), BF16),
        ),
        state,
    )
    far = swapped(plane_state, "sp_0")
    start = on_core(far_kernel, block, plane[None], near, far, scalars=1)
    start = swapped(start, PLANE)
    queries, conv_out = projected(extended, whole, conv_taps, length)
    lstm_out = on_core(
        read_kernel,
        jax.ShapeDtypeStruct((length, DV), BF16),
        queries,
        keys,
        values,
        running.T,
        jnp.concatenate([running, in_gate], axis=0),
        head_gain[None],
        start,
    )

    joined = jnp.concatenate([lstm_out, conv_out], axis=1)
    tp = lax.axis_index("tp")
    joined = in_order(joined, lax.ppermute(joined, "tp", pairs(4, 0)), tp % 2 == 1)
    rest = lax.ppermute(joined, "tp", pairs(4, 1))
    whole = whole.reshape(size, 2, depth, -1)
    pair = tp // 2
    done = output(joined, whole, pair[None], DQK + 3 * DV)
    return output(rest, whole, 1 - pair[None], DQK + 3 * DV, done)


def solution(mesh):
    torus = Mesh(mesh.devices.reshape(8, 8, 2, mesh.shape["tp"]), (*SP, "tp"))
    placed = (
        P(SP, None),
        P(),
        P(SP, "tp"),
        P(SP, "tp"),
        P(SP, "tp"),
        P(None, None, None, "tp"),
        P(None, "tp"),
        P(None, "tp"),
        P(None, SP, "tp"),
        P("tp"),
        P(SP, "tp"),
        P(SP, "tp"),
        P(SP, "tp"),
        P(None, "tp"),
        P(SP, "tp"),
    )
    return jax.shard_map(body, mesh=torus, in_specs=placed, out_specs=P(SP, "tp"), check_vma=False)
```

```python
import jax
import jax.numpy as jnp
from jax import lax
from jax.experimental import pallas as pl
from jax.experimental.pallas import tpu as pltpu
from jax.sharding import Mesh
from jax.sharding import PartitionSpec as P

DQK = 128
DV = 256
SP = ("sp_0", "sp_1", "sp_2")
PLANE = ("sp_1", "sp_2")
EPS = 1e-06
LOWEST = -1e30
F32 = jnp.float32
BF16 = jnp.bfloat16


def row_norm(tokens, norm_gain):
    values = tokens.astype(F32)
    inverse_rms = lax.rsqrt(jnp.mean(values * values, axis=-1, keepdims=True) + EPS)
    return (values * inverse_rms * norm_gain).astype(BF16)


def swapped(value, axes):
    return lax.all_to_all(value, axes, split_axis=0, concat_axis=0, tiled=True)


def copies(value, axes, count):
    return swapped(jnp.broadcast_to(value, (count, *value.shape)), axes)


def neighbour_rows(normed):
    size = lax.axis_size(SP)
    up = [(i, i + 1) for i in range(size - 1)]
    before = lax.ppermute(normed[-1:], SP, up)
    after = lax.ppermute(normed[:1], SP, [(j, i) for i, j in up])
    return before, after


ROWS = 48
NORMERS = 32
NUMBERS = (34, 40)


def in_terms(number):
    high = number.astype(BF16)
    rest = number - high.astype(F32)
    middle = rest.astype(BF16)
    low = (rest - middle.astype(F32)).astype(BF16)
    return [high, middle, low]


def from_terms(block, row):
    return block[row : row + 1] + block[row + 1 : row + 2] + block[row + 2 : row + 3]


def numbered_rows(normers, numbers):
    rows = [n.astype(BF16) for n in normers]
    for pair in numbers:
        for number in pair:
            rows += in_terms(number)
    rows.append(jnp.zeros((ROWS - NORMERS - len(rows), 128), BF16))
    return jnp.concatenate(rows, axis=0)


ARRIVAL = (0, -1, 1, -2, 2, -3, 3, -4)
GROUPS = (3, 4, 1)


def gate_kernel(forget_ref, gate_ref, row_ref, column_ref, number_ref):
    length = forget_ref.shape[1]
    at = lax.broadcasted_iota(jnp.int32, (1, length), 1)
    running, update, numbers = [], [], []
    for d in range(2):
        value = forget_ref[d : d + 1]
        step = 1
        while step < length:
            moved = pltpu.roll(value, length - step if d else step, 1)
            inside = (at < length - step) if d else (at >= step)
            value = value + jnp.where(inside, moved, 0.0)
            step *= 2
        total = value[:, :1] if d else value[:, length - 1 :]
        log_update = total - value + gate_ref[d : d + 1]
        most = jnp.max(log_update, axis=1, keepdims=True)
        running.append(value)
        update.append(jnp.exp(log_update - most))
        numbers += [total, most]
    row_ref[...] = jnp.concatenate([*running, gate_ref[...]], axis=0)
    column_ref[...] = jnp.concatenate([*update, *running, *update, *running], axis=0).T
    for n, number in enumerate(numbers):
        number_ref[n : n + 1] = jnp.broadcast_to(number, (1, 128))


def state_kernel(place_ref, normed_ref, update_ref, number_ref, *refs):
    groups = len(GROUPS)
    state_ref, key_ref, value_ref, weight_ref = refs[2 * groups :]
    core, row = place_ref[0], place_ref[1]
    length = key_ref.shape[0]
    for side in range(2):
        cell = 1 - core if side else core
        arrivals = iter(ARRIVAL)
        for group_ref in refs[side * groups : (side + 1) * groups]:
            _, planes, depth, _ = group_ref.shape
            for k in range(group_ref.shape[0]):
                y = (row + next(arrivals) + 8) % 8
                for z in range(planes):
                    start = ((z * 8 + y) * 2 + cell) * depth
                    weight_ref[pl.ds(pl.multiple_of(start, depth), depth), :] = group_ref[k, z]
    both = jnp.dot(normed_ref[:length], weight_ref[...], preferred_element_type=F32)
    both = both.astype(BF16)
    keys, values = both[:, :DQK], both[:, DQK:]
    key_ref[...] = keys
    value_ref[...] = values
    members = state_ref.shape[0]
    share = DV // members
    normers = []
    for d in range(2):
        weighted = keys.astype(F32) * update_ref[:, d : d + 1]
        normers.append(jnp.sum(weighted, axis=0, keepdims=True))
        memory = lax.dot_general(
            values, weighted.astype(BF16), (((0,), (0,)), ((), ())), preferred_element_type=F32
        )
        state_ref[:, d * share : (d + 1) * share, :] = memory.astype(BF16).reshape(
            members, share, DQK
        )
    numbers = [[number_ref[2 * d + n : 2 * d + n + 1] for n in range(2)] for d in range(2)]
    rows = numbered_rows(normers, numbers)
    for j in range(members):
        state_ref[j, NORMERS:, :] = rows


def passed(carry, block, d):
    memory, normer, total, most = carry
    block_total = from_terms(block, NUMBERS[d])
    block_most = from_terms(block, NUMBERS[d] + 3)
    new = jnp.maximum(most + block_total, block_most)
    old_weight = jnp.exp(most + block_total - new)
    block_weight = jnp.exp(block_most - new)
    share = memory.shape[0]
    memory = old_weight * memory + block_weight * block[d * share : (d + 1) * share]
    normer = old_weight * normer + block_weight * block[NORMERS + d : NORMERS + d + 1]
    return memory, normer, total + block_total, new


def nothing(share):
    row = jnp.zeros((1, 128), F32)
    return jnp.zeros((share, 128), F32), row, row, jnp.full((1, 128), LOWEST, F32)


def plane_kernel(state_ref, near_ref, plane_ref):
    members = state_ref.shape[0]
    share = NORMERS // 2
    ends = []
    for d in range(2):
        carry = nothing(share)
        for i in reversed(range(members)) if d else range(members):
            near_ref[i, d * share : (d + 1) * share, :] = carry[0]
            for n in range(3):
                near_ref[i, NORMERS + 2 * n + d : NORMERS + 2 * n + d + 1, :] = carry[1 + n]
            carry = passed(carry, state_ref[i].astype(F32), d)
        ends.append(carry)
    rows = numbered_rows([e[1] for e in ends], [e[2:] for e in ends])
    for z in range(plane_ref.shape[0]):
        for d in range(2):
            plane_ref[z, d * share : (d + 1) * share, :] = ends[d][0].astype(BF16)
        plane_ref[z, NORMERS:, :] = rows


def far_kernel(place_ref, near_ref, planes_ref, start_ref):
    planes, members = planes_ref.shape[0], near_ref.shape[0]
    share = NORMERS // 2
    place = place_ref[0]
    far = []
    for d in range(2):
        carry = nothing(share)
        for z in reversed(range(planes)) if d else range(planes):
            earlier = (z > place) if d else (z < place)
            after = passed(carry, planes_ref[z].astype(F32), d)
            carry = tuple(jnp.where(earlier, a, c) for a, c in zip(after, carry))
        far.append(carry)
    for i in range(members):
        normers, numbers = [], []
        for d in range(2):
            memory, normer, _, most = far[d]
            at = [NORMERS + 2 * n + d for n in range(3)]
            near_normer, head, near_most = (near_ref[i, r : r + 1, :] for r in at)
            moved = most + head
            new = jnp.maximum(moved, near_most)
            far_weight = jnp.exp(moved - new)
            near_weight = jnp.exp(near_most - new)
            near = near_ref[i, d * share : (d + 1) * share, :]
            start_ref[i, d * share : (d + 1) * share, :] = (
                near_weight * near + far_weight * memory
            ).astype(BF16)
            normers.append(near_weight * near_normer + far_weight * normer)
            numbers.append([new])
        rows = [n.astype(BF16) for n in normers]
        for (number,) in numbers:
            rows += in_terms(number)
        rows.append(jnp.zeros((ROWS - NORMERS - len(rows), 128), BF16))
        start_ref[i, NORMERS:, :] = jnp.concatenate(rows, axis=0)


def read_kernel(query_ref, key_ref, value_ref, column_ref, row_ref, gain_ref, start_ref, out_ref):
    length = query_ref.shape[0]
    queries = query_ref[...]
    values = value_ref[...]
    scale = DQK ** (-0.5)
    products = scale * lax.dot_general(
        queries, key_ref[...], (((1,), (1,)), ((), ())), preferred_element_type=F32
    )
    t = lax.broadcasted_iota(jnp.int32, (length, length), 0)
    s = lax.broadcasted_iota(jnp.int32, (length, length), 1)
    share = NORMERS // 2
    last = start_ref[0, NORMERS:, :].astype(F32)
    summed = None
    for d in range(2):
        memory = start_ref[:, d * share : (d + 1) * share, :].reshape(DV, DQK)
        normer = last[d : d + 1]
        stable = from_terms(last, 2 + 3 * d)[:, :1]
        running = column_ref[:, 2 + d : 3 + d]
        seen = (t <= s) if d else (t >= s)
        log_weight = jnp.where(
            seen, running - row_ref[d : d + 1, :] + row_ref[2 + d : 3 + d, :], -jnp.inf
        )
        carried = running + stable
        highest = jnp.maximum(carried, jnp.max(log_weight, axis=-1, keepdims=True))
        scores = products * jnp.exp(log_weight - highest)
        carry_weight = scale * jnp.exp(carried - highest)
        numerator = jnp.dot(scores.astype(BF16), values, preferred_element_type=F32)
        numerator += carry_weight * lax.dot_general(
            queries, memory, (((1,), (1,)), ((), ())), preferred_element_type=F32
        )
        denominator = jnp.sum(scores, axis=-1, keepdims=True)
        denominator += carry_weight * jnp.sum(
            queries.astype(F32) * normer, axis=-1, keepdims=True
        )
        result = numerator / jnp.maximum(jnp.abs(denominator), jnp.exp(-highest))
        summed = result if summed is None else summed + result
    inverse_rms = lax.rsqrt(jnp.mean(summed * summed, axis=-1, keepdims=True) + EPS)
    out = (summed * inverse_rms * gain_ref[...]).astype(BF16)
    for k in range(out_ref.shape[0]):
        out_ref[k] = out


WIDE = DQK + 3 * DV
CHUNKS = 8


def project_kernel(normed_ref, tap_ref, whole_ref, query_ref, conv_ref, weight_ref, total_ref, sems):
    depth = weight_ref.shape[1]
    length = query_ref.shape[0]

    def fetch(k):
        return pltpu.make_async_copy(
            whole_ref.at[pl.ds(k * depth, depth), pl.ds(0, WIDE)], weight_ref.at[k], sems.at[k]
        )

    for k in range(CHUNKS):
        fetch(k).start()
    for k in range(CHUNKS):
        fetch(k).wait()
        product = jnp.dot(
            normed_ref[:, k * depth : (k + 1) * depth], weight_ref[k], preferred_element_type=F32
        )
        if k:
            total_ref[...] += product
        else:
            total_ref[...] = product
    query_ref[...] = total_ref[:length, :DQK].astype(BF16)
    inner = total_ref[:, DQK : DQK + DV].astype(BF16).astype(F32)
    given = total_ref[:, DQK + DV : DQK + 2 * DV].astype(BF16).astype(F32)
    outer = total_ref[:length, DQK + 2 * DV :].astype(BF16).astype(F32)
    mixed = (inner * given).astype(BF16).astype(F32)
    here = mixed[:length]
    at = lax.broadcasted_iota(jnp.int32, (length, DV), 0)
    before = jnp.where(at == 0, mixed[length : length + 1], pltpu.roll(here, 1, 0))
    after = jnp.where(
        at == length - 1, mixed[length + 1 : length + 2], pltpu.roll(here, length - 1, 0)
    )
    taps = tap_ref[...].astype(F32)
    filtered = taps[0:1] * before + taps[1:2] * here + taps[2:3] * after
    conv_ref[...] = (outer * filtered).astype(BF16)


def fetch_rows(whole_ref, weight_ref, sems, device, slot):
    return [
        pltpu.make_async_copy(
            whole_ref.at[pl.ds(device, 16), side, :, pl.ds(WIDE, 512)],
            weight_ref.at[slot, side],
            sems.at[slot, side],
        )
        for side in range(2)
    ]


def convolved_kernel(place_ref, *refs):
    parts = refs[:4]
    whole_ref, out_ref, later_ref, weight_ref, sems, later_sems = refs[4:]
    place = place_ref[0]
    copies_in = []
    for n, offset in enumerate((0, -1, 1, 2)):
        source = (place + offset + 4) % 4
        copies_in.append(fetch_rows(whole_ref, weight_ref, sems, source * 32 + 16, n))
    later = [fetch_rows(whole_ref, later_ref, later_sems, k * 32, k) for k in range(4)]
    for pair in copies_in + later:
        for copy in pair:
            copy.start()
    for n, part_ref in enumerate(parts):
        for side in range(2):
            copies_in[n][side].wait()
            weight = weight_ref[n, side].reshape(DV, 512)
            product = jnp.dot(part_ref[...], weight, preferred_element_type=F32)
            at = slice(side * 512, (side + 1) * 512)
            if n:
                out_ref[:, at] += product
            else:
                out_ref[:, at] = product
    for pair in later:
        for copy in pair:
            copy.wait()


def output_kernel(joined_ref, weight_ref, earlier_ref, out_ref):
    for side in range(2):
        at = slice(side * 512, (side + 1) * 512)
        total = earlier_ref[:, at]
        for k in range(4):
            weight = weight_ref[k, side].reshape(DV, 512)
            total += jnp.dot(joined_ref[k], weight, preferred_element_type=F32)
        out_ref[:, at] = total.astype(BF16)


def ring(size, step):
    return [(i, (i + step) % size) for i in range(size)]


def on_core(kernel, out, *operands, scalars=0, remote=0, scratch=()):
    vmem = pl.BlockSpec(memory_space=pltpu.VMEM)
    smem = pl.BlockSpec(memory_space=pltpu.SMEM)
    return pl.pallas_call(
        kernel,
        out_shape=out,
        in_specs=[smem] * scalars
        + [vmem] * (len(operands) - scalars - remote)
        + [pl.BlockSpec(memory_space=pltpu.HBM)] * remote,
        out_specs=jax.tree.map(lambda _: vmem, out),
        scratch_shapes=scratch,
        compiler_params=pltpu.CompilerParams(vmem_limit_bytes=40 * 2**20),
    )(*operands)


def body(
    tokens,
    norm_gain,
    w_query,
    w_key,
    w_value,
    w_gates,
    input_bias,
    forget_bias,
    decay_shift,
    head_gain,
    w_conv_b,
    w_conv_c,
    w_conv_in,
    conv_taps,
    w_out,
):
    length = tokens.shape[0]
    size = lax.axis_size(SP)
    planes = lax.axis_size("sp_0")
    members = size // planes
    plane = lax.axis_index("sp_0")
    depth = w_out.shape[0]
    half = w_out.shape[1] // 2
    out_rows = jnp.concatenate([w_out[:, :half], w_out[:, half:]], axis=0)
    packed = jnp.concatenate([w_query, w_conv_c, w_conv_in, w_conv_b, out_rows], axis=1)
    whole = lax.all_gather(packed, SP, axis=0, tiled=True)
    core = lax.axis_index("sp_2")
    row = lax.axis_index("sp_1")
    block = copies(jnp.concatenate([w_key, w_value], axis=1), "sp_0", planes)

    normed = row_norm(tokens, norm_gain)
    before, after = neighbour_rows(normed)
    edges = jnp.zeros((14, normed.shape[1]), BF16)
    block, before, after = lax.optimization_barrier((block, before, after))
    extended = jnp.concatenate([normed, before, after, edges], axis=0)

    up = down = block
    pieces = [block]
    for k in range(4):
        up = lax.ppermute(up, "sp_1", ring(8, 1))
        pieces.append(up)
        if k < 3:
            down = lax.ppermute(down, "sp_1", ring(8, -1))
            pieces.append(down)
    groups, at = [], 0
    for count in GROUPS:
        groups.append(jnp.stack(pieces[at : at + count]))
        at += count
    groups += [lax.ppermute(g, "sp_2", ring(2, 1)) for g in groups]

    gates = lax.dot_general(
        w_gates.reshape(-1, 4), normed, (((0,), (1,)), ((), ())), preferred_element_type=F32
    ).reshape(2, 2, length)
    in_gate = gates[:, 0] + input_bias
    log_forget = jax.nn.log_sigmoid(gates[:, 1] + forget_bias) + decay_shift[:, :, 0]
    rows, columns, numbers = on_core(
        gate_kernel,
        (
            jax.ShapeDtypeStruct((4, length), F32),
            jax.ShapeDtypeStruct((length, 8), F32),
            jax.ShapeDtypeStruct((4, 128), F32),
        ),
        log_forget,
        in_gate,
    )
    block = jax.ShapeDtypeStruct((members, ROWS, 128), BF16)
    state, keys, values = on_core(
        state_kernel,
        (
            block,
            jax.ShapeDtypeStruct((length, DQK), BF16),
            jax.ShapeDtypeStruct((length, DV), BF16),
        ),
        jnp.stack([core, row]),
        extended,
        columns,
        numbers,
        *groups,
        scalars=1,
        scratch=[pltpu.VMEM((normed.shape[1], DQK + DV), BF16)],
    )
    state = swapped(state, PLANE)
    near, plane_state = on_core(
        plane_kernel,
        (
            jax.ShapeDtypeStruct((members, ROWS, 128), F32),
            jax.ShapeDtypeStruct((planes, ROWS, 128), BF16),
        ),
        state,
    )
    far = swapped(plane_state, "sp_0")
    start = on_core(far_kernel, block, plane[None], near, far, scalars=1)
    start = swapped(start, PLANE)
    queries, conv_out = on_core(
        project_kernel,
        (
            jax.ShapeDtypeStruct((length, DQK), BF16),
            jax.ShapeDtypeStruct((length, DV), BF16),
        ),
        extended,
        conv_taps,
        whole,
        remote=1,
        scratch=[
            pltpu.VMEM((CHUNKS, whole.shape[0] // CHUNKS, WIDE), BF16),
            pltpu.VMEM((extended.shape[0], WIDE), F32),
            pltpu.SemaphoreType.DMA((CHUNKS,)),
        ],
    )
    parts = [conv_out] + [lax.ppermute(conv_out, "tp", ring(4, n)) for n in (1, -1, 2)]
    lstm_out = on_core(
        read_kernel,
        jax.ShapeDtypeStruct((4, length, DV), BF16),
        queries,
        keys,
        values,
        columns,
        rows,
        head_gain[None],
        start,
    )
    lstm_all = swapped(lstm_out, "tp")
    whole = whole.reshape(size, 2, depth, -1)
    done, out_weights = on_core(
        convolved_kernel,
        (
            jax.ShapeDtypeStruct((length, 2 * half), F32),
            jax.ShapeDtypeStruct((4, 2, 16, depth, half), BF16),
        ),
        lax.axis_index("tp")[None],
        *parts,
        whole,
        scalars=1,
        remote=1,
        scratch=[
            pltpu.VMEM((4, 2, 16, depth, half), BF16),
            pltpu.SemaphoreType.DMA((4, 2)),
            pltpu.SemaphoreType.DMA((4, 2)),
        ],
    )
    return on_core(
        output_kernel,
        jax.ShapeDtypeStruct((length, 2 * half), BF16),
        lstm_all,
        out_weights,
        done,
    )


def solution(mesh):
    torus = Mesh(mesh.devices.reshape(8, 8, 2, mesh.shape["tp"]), (*SP, "tp"))
    placed = (
        P(SP, None),
        P(),
        P(SP, "tp"),
        P(SP, "tp"),
        P(SP, "tp"),
        P(None, None, None, "tp"),
        P(None, "tp"),
        P(None, "tp"),
        P(None, SP, "tp"),
        P("tp"),
        P(SP, "tp"),
        P(SP, "tp"),
        P(SP, "tp"),
        P(None, "tp"),
        P(SP, "tp"),
    )
    return jax.shard_map(body, mesh=torus, in_specs=placed, out_specs=P(SP, "tp"), check_vma=False)
```

```python
import jax
import jax.numpy as jnp
from jax import lax
from jax.experimental import pallas as pl
from jax.experimental.pallas import tpu as pltpu
from jax.sharding import Mesh
from jax.sharding import PartitionSpec as P


DQK = 128
DV = 256
SP = ("sp_0", "sp_1", "sp_2")
PLANE = ("sp_1", "sp_2")
EPS = 1e-06
LOWEST = -1e30
F32 = jnp.float32
BF16 = jnp.bfloat16


def row_norm(tokens, norm_gain):
    values = tokens.astype(F32)
    inverse_rms = lax.rsqrt(jnp.mean(values * values, axis=-1, keepdims=True) + EPS)
    return (values * inverse_rms * norm_gain).astype(BF16)


def swapped(value, axes):
    return lax.all_to_all(value, axes, split_axis=0, concat_axis=0, tiled=True)


def neighbour_rows(last, initial):
    size = lax.axis_size(SP)
    up = [(i, i + 1) for i in range(size - 1)]
    before = lax.ppermute(last, SP, up)
    after = lax.ppermute(initial, SP, [(j, i) for i, j in up])
    return before, after


ROWS = 48
NORMERS = 32
NUMBERS = (34, 40)


def in_terms(number):
    high = number.astype(BF16)
    rest = number - high.astype(F32)
    middle = rest.astype(BF16)
    low = (rest - middle.astype(F32)).astype(BF16)
    return [high, middle, low]


def from_terms(block, row):
    return block[row : row + 1] + block[row + 1 : row + 2] + block[row + 2 : row + 3]


def numbered_rows(normers, numbers):
    rows = [n.astype(BF16) for n in normers]
    for pair in numbers:
        for number in pair:
            rows += in_terms(number)
    rows.append(jnp.zeros((ROWS - NORMERS - len(rows), 128), BF16))
    return jnp.concatenate(rows, axis=0)


ARRIVAL = (0, -1, 1, -2, 2, -3, 3, -4)
GROUPS = (3, 4, 1)


def pack_kernel(query_ref, key_ref, value_ref, outer_ref, inner_ref, given_ref, out_ref, whole_ref, block_ref):
    at = 0
    for ref in (query_ref, inner_ref, given_ref, outer_ref):
        whole_ref[:, at : at + ref.shape[1]] = ref[...]
        at += ref.shape[1]
    depth, columns = out_ref.shape
    for side in range(2):
        whole_ref[side * depth : (side + 1) * depth, at:] = out_ref[
            :, side * columns // 2 : (side + 1) * columns // 2
        ]
    for z in range(block_ref.shape[0]):
        block_ref[z, :, :DQK] = key_ref[...]
        block_ref[z, :, DQK:] = value_ref[...]


def gate_kernel(forget_ref, gate_ref, row_ref, column_ref, number_ref):
    length = forget_ref.shape[1]
    at = lax.broadcasted_iota(jnp.int32, (1, length), 1)
    running, update, numbers = [], [], []
    for d in range(2):
        value = forget_ref[d : d + 1]
        step = 1
        while step < length:
            moved = pltpu.roll(value, length - step if d else step, 1)
            inside = (at < length - step) if d else (at >= step)
            value = value + jnp.where(inside, moved, 0.0)
            step *= 2
        total = value[:, :1] if d else value[:, length - 1 :]
        log_update = total - value + gate_ref[d : d + 1]
        most = jnp.max(log_update, axis=1, keepdims=True)
        running.append(value)
        update.append(jnp.exp(log_update - most))
        numbers += [total, most]
    row_ref[...] = jnp.concatenate([*running, gate_ref[...]], axis=0)
    column_ref[...] = jnp.concatenate([*update, *running, *update, *running], axis=0).T
    for n, number in enumerate(numbers):
        number_ref[n : n + 1] = jnp.broadcast_to(number, (1, 128))


def state_kernel(place_ref, normed_ref, update_ref, number_ref, *refs):
    groups = len(GROUPS)
    state_ref, key_ref, value_ref, weight_ref = refs[2 * groups :]
    core, row = place_ref[0], place_ref[1]
    for side in range(2):
        cell = 1 - core if side else core
        arrivals = iter(ARRIVAL)
        for group_ref in refs[side * groups : (side + 1) * groups]:
            _, planes, depth, _ = group_ref.shape
            for k in range(group_ref.shape[0]):
                y = (row + next(arrivals) + 8) % 8
                for z in range(planes):
                    start = ((z * 8 + y) * 2 + cell) * depth
                    weight_ref[pl.ds(pl.multiple_of(start, depth), depth), :] = group_ref[k, z]
    both = jnp.dot(normed_ref[...], weight_ref[...], preferred_element_type=F32)
    both = both.astype(BF16)
    keys, values = both[:, :DQK], both[:, DQK:]
    key_ref[...] = keys
    value_ref[...] = values
    members = state_ref.shape[0]
    share = DV // members
    normers = []
    for d in range(2):
        weighted = keys.astype(F32) * update_ref[:, d : d + 1]
        normers.append(jnp.sum(weighted, axis=0, keepdims=True))
        memory = lax.dot_general(
            values, weighted.astype(BF16), (((0,), (0,)), ((), ())), preferred_element_type=F32
        )
        state_ref[:, d * share : (d + 1) * share, :] = memory.astype(BF16).reshape(
            members, share, DQK
        )
    numbers = [[number_ref[2 * d + n : 2 * d + n + 1] for n in range(2)] for d in range(2)]
    rows = numbered_rows(normers, numbers)
    for j in range(members):
        state_ref[j, NORMERS:, :] = rows


def passed(carry, block, d):
    memory, normer, total, most = carry
    block_total = from_terms(block, NUMBERS[d])
    block_most = from_terms(block, NUMBERS[d] + 3)
    new = jnp.maximum(most + block_total, block_most)
    old_weight = jnp.exp(most + block_total - new)
    block_weight = jnp.exp(block_most - new)
    share = memory.shape[0]
    memory = old_weight * memory + block_weight * block[d * share : (d + 1) * share]
    normer = old_weight * normer + block_weight * block[NORMERS + d : NORMERS + d + 1]
    return memory, normer, total + block_total, new


def nothing(share):
    row = jnp.zeros((1, 128), F32)
    return jnp.zeros((share, 128), F32), row, row, jnp.full((1, 128), LOWEST, F32)


def plane_kernel(state_ref, near_ref, plane_ref):
    members = state_ref.shape[0]
    share = NORMERS // 2
    ends = []
    for d in range(2):
        carry = nothing(share)
        for i in reversed(range(members)) if d else range(members):
            near_ref[i, d * share : (d + 1) * share, :] = carry[0]
            for n in range(3):
                near_ref[i, NORMERS + 2 * n + d : NORMERS + 2 * n + d + 1, :] = carry[1 + n]
            carry = passed(carry, state_ref[i].astype(F32), d)
        ends.append(carry)
    rows = numbered_rows([e[1] for e in ends], [e[2:] for e in ends])
    for z in range(plane_ref.shape[0]):
        for d in range(2):
            plane_ref[z, d * share : (d + 1) * share, :] = ends[d][0].astype(BF16)
        plane_ref[z, NORMERS:, :] = rows


def far_kernel(place_ref, near_ref, planes_ref, start_ref):
    planes, members = planes_ref.shape[0], near_ref.shape[0]
    share = NORMERS // 2
    place = place_ref[0]
    far = []
    for d in range(2):
        carry = nothing(share)
        for z in reversed(range(planes)) if d else range(planes):
            earlier = (z > place) if d else (z < place)
            after = passed(carry, planes_ref[z].astype(F32), d)
            carry = tuple(jnp.where(earlier, a, c) for a, c in zip(after, carry))
        far.append(carry)
    for i in range(members):
        normers, numbers = [], []
        for d in range(2):
            memory, normer, _, most = far[d]
            at = [NORMERS + 2 * n + d for n in range(3)]
            near_normer, head, near_most = (near_ref[i, r : r + 1, :] for r in at)
            moved = most + head
            new = jnp.maximum(moved, near_most)
            far_weight = jnp.exp(moved - new)
            near_weight = jnp.exp(near_most - new)
            near = near_ref[i, d * share : (d + 1) * share, :]
            start_ref[i, d * share : (d + 1) * share, :] = (
                near_weight * near + far_weight * memory
            ).astype(BF16)
            normers.append(near_weight * near_normer + far_weight * normer)
            numbers.append([new])
        rows = [n.astype(BF16) for n in normers]
        for (number,) in numbers:
            rows += in_terms(number)
        rows.append(jnp.zeros((ROWS - NORMERS - len(rows), 128), BF16))
        start_ref[i, NORMERS:, :] = jnp.concatenate(rows, axis=0)


def read_kernel(query_ref, key_ref, value_ref, column_ref, row_ref, gain_ref, start_ref, out_ref):
    length = query_ref.shape[0]
    queries = query_ref[...]
    values = value_ref[...]
    scale = DQK ** (-0.5)
    products = scale * lax.dot_general(
        queries, key_ref[...], (((1,), (1,)), ((), ())), preferred_element_type=F32
    )
    t = lax.broadcasted_iota(jnp.int32, (length, length), 0)
    s = lax.broadcasted_iota(jnp.int32, (length, length), 1)
    share = NORMERS // 2
    last = start_ref[0, NORMERS:, :].astype(F32)
    summed = None
    for d in range(2):
        memory = start_ref[:, d * share : (d + 1) * share, :].reshape(DV, DQK)
        normer = last[d : d + 1]
        stable = from_terms(last, 2 + 3 * d)[:, :1]
        running = column_ref[:, 2 + d : 3 + d]
        seen = (t <= s) if d else (t >= s)
        log_weight = jnp.where(
            seen, running - row_ref[d : d + 1, :] + row_ref[2 + d : 3 + d, :], -jnp.inf
        )
        carried = running + stable
        highest = jnp.maximum(carried, jnp.max(log_weight, axis=-1, keepdims=True))
        scores = products * jnp.exp(log_weight - highest)
        carry_weight = scale * jnp.exp(carried - highest)
        numerator = jnp.dot(scores.astype(BF16), values, preferred_element_type=F32)
        numerator += carry_weight * lax.dot_general(
            queries, memory, (((1,), (1,)), ((), ())), preferred_element_type=F32
        )
        denominator = jnp.sum(scores, axis=-1, keepdims=True)
        denominator += carry_weight * jnp.sum(
            queries.astype(F32) * normer, axis=-1, keepdims=True
        )
        result = numerator / jnp.maximum(jnp.abs(denominator), jnp.exp(-highest))
        summed = result if summed is None else summed + result
    inverse_rms = lax.rsqrt(jnp.mean(summed * summed, axis=-1, keepdims=True) + EPS)
    out = (summed * inverse_rms * gain_ref[...]).astype(BF16)
    for k in range(out_ref.shape[0]):
        out_ref[k] = out


WIDE = DQK + 3 * DV
CHUNKS = 8


def project_kernel(
    normed_ref, edge_ref, tap_ref, whole_ref, query_ref, conv_ref, weight_ref, total_ref, sems
):
    depth = weight_ref.shape[1]
    length = query_ref.shape[0]

    def fetch(k):
        return pltpu.make_async_copy(
            whole_ref.at[pl.ds(k * depth, depth), pl.ds(0, WIDE)], weight_ref.at[k], sems.at[k]
        )

    for k in range(CHUNKS):
        fetch(k).start()
    for k in range(CHUNKS):
        fetch(k).wait()
        at = slice(k * depth, (k + 1) * depth)
        rows = jnp.concatenate([normed_ref[:, at], edge_ref[:, at]], axis=0)
        product = jnp.dot(rows, weight_ref[k], preferred_element_type=F32)
        if k:
            total_ref[...] += product
        else:
            total_ref[...] = product
    query_ref[...] = total_ref[:length, :DQK].astype(BF16)
    inner = total_ref[:, DQK : DQK + DV].astype(BF16).astype(F32)
    given = total_ref[:, DQK + DV : DQK + 2 * DV].astype(BF16).astype(F32)
    outer = total_ref[:length, DQK + 2 * DV :].astype(BF16).astype(F32)
    mixed = (inner * given).astype(BF16).astype(F32)
    here = mixed[:length]
    at = lax.broadcasted_iota(jnp.int32, (length, DV), 0)
    before = jnp.where(at == 0, mixed[length : length + 1], pltpu.roll(here, 1, 0))
    after = jnp.where(
        at == length - 1, mixed[length + 1 : length + 2], pltpu.roll(here, length - 1, 0)
    )
    taps = tap_ref[...].astype(F32)
    filtered = taps[0:1] * before + taps[1:2] * here + taps[2:3] * after
    conv_ref[...] = (outer * filtered).astype(BF16)


def output_kernel(place_ref, lstm_ref, *refs):
    parts, (whole_ref, out_ref, weight_ref, sems) = refs[:4], refs[4:]
    place = place_ref[0]
    sources = [(k * 32, lstm_ref.at[k]) for k in range(4)]
    for part_ref, offset in zip(parts, (0, -1, 1, 2)):
        sources.append(((place + offset + 4) % 4 * 32 + 16, part_ref))

    def fetch(n, side):
        return pltpu.make_async_copy(
            whole_ref.at[pl.ds(sources[n][0], 16), side, :, pl.ds(WIDE, 512)],
            weight_ref.at[n, side],
            sems.at[n, side],
        )

    for side in range(2):
        for n in range(8):
            fetch(n, side).start()
    for side in range(2):
        total = None
        for n in range(8):
            fetch(n, side).wait()
            weight = weight_ref[n, side].reshape(DV, 512)
            product = jnp.dot(sources[n][1][...], weight, preferred_element_type=F32)
            total = product if total is None else total + product
        out_ref[:, side * 512 : (side + 1) * 512] = total.astype(BF16)


def ring(size, step):
    return [(i, (i + step) % size) for i in range(size)]


def on_core(kernel, out, *operands, scalars=0, remote=0, scratch=(), limit=20):
    vmem = pl.BlockSpec(memory_space=pltpu.VMEM)
    smem = pl.BlockSpec(memory_space=pltpu.SMEM)
    return pl.pallas_call(
        kernel,
        out_shape=out,
        in_specs=[smem] * scalars
        + [vmem] * (len(operands) - scalars - remote)
        + [pl.BlockSpec(memory_space=pltpu.HBM)] * remote,
        out_specs=jax.tree.map(lambda _: vmem, out),
        scratch_shapes=scratch,
        compiler_params=pltpu.CompilerParams(vmem_limit_bytes=limit * 2**20),
    )(*operands)


def body(
    tokens,
    norm_gain,
    w_query,
    w_key,
    w_value,
    w_gates,
    input_bias,
    forget_bias,
    decay_shift,
    head_gain,
    w_conv_b,
    w_conv_c,
    w_conv_in,
    conv_taps,
    w_out,
):
    length = tokens.shape[0]
    size = lax.axis_size(SP)
    planes = lax.axis_size("sp_0")
    members = size // planes
    plane = lax.axis_index("sp_0")
    depth = w_out.shape[0]
    half = w_out.shape[1] // 2
    packed, block = on_core(
        pack_kernel,
        (
            jax.ShapeDtypeStruct((w_key.shape[0], WIDE + half), BF16),
            jax.ShapeDtypeStruct((planes, w_key.shape[0], DQK + DV), BF16),
        ),
        w_query,
        w_key,
        w_value,
        w_conv_b,
        w_conv_c,
        w_conv_in,
        w_out,
    )
    block = swapped(block, "sp_0")
    whole = lax.all_gather(packed, SP, axis=0, tiled=True)
    core = lax.axis_index("sp_2")
    row = lax.axis_index("sp_1")
    normed = row_norm(tokens, norm_gain)

    block, normed = lax.optimization_barrier((block, normed))
    up = down = block
    pieces = [block]
    for k in range(4):
        up = lax.ppermute(up, "sp_1", ring(8, 1))
        pieces.append(up)
        if k < 3:
            down = lax.ppermute(down, "sp_1", ring(8, -1))
            pieces.append(down)
    groups, at = [], 0
    for count in GROUPS:
        groups.append(jnp.stack(pieces[at : at + count]))
        at += count
    for count, group in zip(GROUPS, tuple(groups)):
        groups.append(lax.ppermute(group, "sp_2", ring(2, 1)))

    gates = lax.dot_general(
        w_gates.reshape(-1, 4), normed, (((0,), (1,)), ((), ())), preferred_element_type=F32
    ).reshape(2, 2, length)
    in_gate = gates[:, 0] + input_bias
    log_forget = jax.nn.log_sigmoid(gates[:, 1] + forget_bias) + decay_shift[:, :, 0]
    rows, columns, numbers = on_core(
        gate_kernel,
        (
            jax.ShapeDtypeStruct((4, length), F32),
            jax.ShapeDtypeStruct((length, 8), F32),
            jax.ShapeDtypeStruct((4, 128), F32),
        ),
        log_forget,
        in_gate,
    )
    block = jax.ShapeDtypeStruct((members, ROWS, 128), BF16)
    state, keys, values = on_core(
        state_kernel,
        (
            block,
            jax.ShapeDtypeStruct((length, DQK), BF16),
            jax.ShapeDtypeStruct((length, DV), BF16),
        ),
        jnp.stack([core, row]),
        normed,
        columns,
        numbers,
        *groups,
        scalars=1,
        scratch=[pltpu.VMEM((normed.shape[1], DQK + DV), BF16)],
    )
    last, initial, keys = lax.optimization_barrier((normed[-1:], normed[:1], keys))
    state = swapped(state, PLANE)
    before, after = neighbour_rows(last, initial)
    edges = jnp.concatenate([before, after, jnp.zeros((14, normed.shape[1]), BF16)], axis=0)
    near, plane_state = on_core(
        plane_kernel,
        (
            jax.ShapeDtypeStruct((members, ROWS, 128), F32),
            jax.ShapeDtypeStruct((planes, ROWS, 128), BF16),
        ),
        state,
    )
    far = swapped(plane_state, "sp_0")
    queries, conv_out = on_core(
        project_kernel,
        (
            jax.ShapeDtypeStruct((length, DQK), BF16),
            jax.ShapeDtypeStruct((length, DV), BF16),
        ),
        normed,
        edges,
        conv_taps,
        whole,
        remote=1,
        scratch=[
            pltpu.VMEM((CHUNKS, whole.shape[0] // CHUNKS, WIDE), BF16),
            pltpu.VMEM((length + edges.shape[0], WIDE), F32),
            pltpu.SemaphoreType.DMA((CHUNKS,)),
        ],
        limit=54,
    )
    far, queries, conv_out = lax.optimization_barrier((far, queries, conv_out))
    start = on_core(far_kernel, block, plane[None], near, far, scalars=1)
    start = swapped(start, PLANE)
    parts = [conv_out] + [lax.ppermute(conv_out, "tp", ring(4, n)) for n in (1, -1, 2)]
    start, *parts = lax.optimization_barrier((start, *parts))
    lstm_out = on_core(
        read_kernel,
        jax.ShapeDtypeStruct((4, length, DV), BF16),
        queries,
        keys,
        values,
        columns,
        rows,
        head_gain[None],
        start,
    )
    lstm_all = swapped(lstm_out, "tp")
    whole = whole.reshape(size, 2, depth, -1)
    return on_core(
        output_kernel,
        jax.ShapeDtypeStruct((length, 2 * half), BF16),
        lax.axis_index("tp")[None],
        lstm_all,
        *parts,
        whole,
        scalars=1,
        remote=1,
        scratch=[
            pltpu.VMEM((8, 2, 16, depth, half), BF16),
            pltpu.SemaphoreType.DMA((8, 2)),
        ],
        limit=58,
    )


def solution(mesh):
    torus = Mesh(mesh.devices.reshape(8, 8, 2, mesh.shape["tp"]), (*SP, "tp"))
    placed = (
        P(SP, None),
        P(),
        P(SP, "tp"),
        P(SP, "tp"),
        P(SP, "tp"),
        P(None, None, None, "tp"),
        P(None, "tp"),
        P(None, "tp"),
        P(None, SP, "tp"),
        P("tp"),
        P(SP, "tp"),
        P(SP, "tp"),
        P(SP, "tp"),
        P(None, "tp"),
        P(SP, "tp"),
    )

    return jax.shard_map(body, mesh=torus, in_specs=placed, out_specs=P(SP, "tp"), check_vma=False)
```

```python
import jax
import jax.numpy as jnp
from jax import lax
from jax.experimental import pallas as pl
from jax.experimental.pallas import tpu as pltpu
from jax.sharding import Mesh
from jax.sharding import PartitionSpec as P


DQK = 128
DV = 256
SP = ("sp_0", "sp_1", "sp_2")
PLANE = ("sp_1", "sp_2")
EPS = 1e-06
LOWEST = -1e30
F32 = jnp.float32
BF16 = jnp.bfloat16


def row_norm(tokens, norm_gain):
    values = tokens.astype(F32)
    inverse_rms = lax.rsqrt(jnp.mean(values * values, axis=-1, keepdims=True) + EPS)
    return (values * inverse_rms * norm_gain).astype(BF16)


def swapped(value, axes):
    return lax.all_to_all(value, axes, split_axis=0, concat_axis=0, tiled=True)


def neighbour_rows(last, initial):
    size = lax.axis_size(SP)
    up = [(i, i + 1) for i in range(size - 1)]
    before = lax.ppermute(last, SP, up)
    after = lax.ppermute(initial, SP, [(j, i) for i, j in up])
    return before, after


ROWS = 48
NORMERS = 32
NUMBERS = (34, 40)


def in_terms(number):
    high = number.astype(BF16)
    rest = number - high.astype(F32)
    middle = rest.astype(BF16)
    low = (rest - middle.astype(F32)).astype(BF16)
    return [high, middle, low]


def from_terms(block, row):
    return block[row : row + 1] + block[row + 1 : row + 2] + block[row + 2 : row + 3]


def numbered_rows(normers, numbers):
    rows = [n.astype(BF16) for n in normers]
    for pair in numbers:
        for number in pair:
            rows += in_terms(number)
    rows.append(jnp.zeros((ROWS - NORMERS - len(rows), 128), BF16))
    return jnp.concatenate(rows, axis=0)


ARRIVAL = (0, -1, 1, -2, 2, -3, 3, -4)
GROUPS = (3, 4, 1)


def pack_kernel(query_ref, key_ref, value_ref, outer_ref, inner_ref, given_ref, out_ref, whole_ref, block_ref, sems):
    moves = []
    for z in range(block_ref.shape[0]):
        moves.append((key_ref, block_ref.at[z, :, pl.ds(0, DQK)]))
        moves.append((value_ref, block_ref.at[z, :, pl.ds(DQK, DV)]))
    at = 0
    for ref in (query_ref, inner_ref, given_ref, outer_ref):
        moves.append((ref, whole_ref.at[:, pl.ds(at, ref.shape[1])]))
        at += ref.shape[1]
    depth, columns = out_ref.shape
    half = columns // 2
    for side in range(2):
        target = whole_ref.at[pl.ds(side * depth, depth), pl.ds(at, half)]
        moves.append((out_ref.at[:, pl.ds(side * half, half)], target))
    moves = moves[::-1]
    for n, (source, target) in enumerate(moves):
        pltpu.make_async_copy(source, target, sems.at[n]).start()
    for n, (source, target) in enumerate(moves):
        pltpu.make_async_copy(source, target, sems.at[n]).wait()


def gate_kernel(forget_ref, gate_ref, row_ref, column_ref, number_ref):
    length = forget_ref.shape[1]
    at = lax.broadcasted_iota(jnp.int32, (1, length), 1)
    running, update, numbers = [], [], []
    for d in range(2):
        value = forget_ref[d : d + 1]
        step = 1
        while step < length:
            moved = pltpu.roll(value, length - step if d else step, 1)
            inside = (at < length - step) if d else (at >= step)
            value = value + jnp.where(inside, moved, 0.0)
            step *= 2
        total = value[:, :1] if d else value[:, length - 1 :]
        log_update = total - value + gate_ref[d : d + 1]
        most = jnp.max(log_update, axis=1, keepdims=True)
        running.append(value)
        update.append(jnp.exp(log_update - most))
        numbers += [total, most]
    row_ref[...] = jnp.concatenate([*running, gate_ref[...]], axis=0)
    column_ref[...] = jnp.concatenate([*update, *running, *update, *running], axis=0).T
    for n, number in enumerate(numbers):
        number_ref[n : n + 1] = jnp.broadcast_to(number, (1, 128))


def state_kernel(place_ref, normed_ref, update_ref, number_ref, *refs):
    groups = len(GROUPS)
    state_ref, key_ref, value_ref, weight_ref = refs[2 * groups :]
    core, row = place_ref[0], place_ref[1]
    for side in range(2):
        cell = 1 - core if side else core
        arrivals = iter(ARRIVAL)
        for group_ref in refs[side * groups : (side + 1) * groups]:
            _, planes, depth, _ = group_ref.shape
            for k in range(group_ref.shape[0]):
                y = (row + next(arrivals) + 8) % 8
                for z in range(planes):
                    start = ((z * 8 + y) * 2 + cell) * depth
                    weight_ref[pl.ds(pl.multiple_of(start, depth), depth), :] = group_ref[k, z]
    both = jnp.dot(normed_ref[...], weight_ref[...], preferred_element_type=F32)
    both = both.astype(BF16)
    keys, values = both[:, :DQK], both[:, DQK:]
    key_ref[...] = keys
    value_ref[...] = values
    members = state_ref.shape[0]
    share = DV // members
    normers = []
    for d in range(2):
        weighted = keys.astype(F32) * update_ref[:, d : d + 1]
        normers.append(jnp.sum(weighted, axis=0, keepdims=True))
        memory = lax.dot_general(
            values, weighted.astype(BF16), (((0,), (0,)), ((), ())), preferred_element_type=F32
        )
        state_ref[:, d * share : (d + 1) * share, :] = memory.astype(BF16).reshape(
            members, share, DQK
        )
    numbers = [[number_ref[2 * d + n : 2 * d + n + 1] for n in range(2)] for d in range(2)]
    rows = numbered_rows(normers, numbers)
    for j in range(members):
        state_ref[j, NORMERS:, :] = rows


def passed(carry, block, d):
    memory, normer, total, most = carry
    block_total = from_terms(block, NUMBERS[d])
    block_most = from_terms(block, NUMBERS[d] + 3)
    new = jnp.maximum(most + block_total, block_most)
    old_weight = jnp.exp(most + block_total - new)
    block_weight = jnp.exp(block_most - new)
    share = memory.shape[0]
    memory = old_weight * memory + block_weight * block[d * share : (d + 1) * share]
    normer = old_weight * normer + block_weight * block[NORMERS + d : NORMERS + d + 1]
    return memory, normer, total + block_total, new


def nothing(share):
    row = jnp.zeros((1, 128), F32)
    return jnp.zeros((share, 128), F32), row, row, jnp.full((1, 128), LOWEST, F32)


def plane_kernel(state_ref, near_ref, plane_ref):
    members = state_ref.shape[0]
    share = NORMERS // 2
    ends = []
    for d in range(2):
        carry = nothing(share)
        for i in reversed(range(members)) if d else range(members):
            near_ref[i, d * share : (d + 1) * share, :] = carry[0]
            for n in range(3):
                near_ref[i, NORMERS + 2 * n + d : NORMERS + 2 * n + d + 1, :] = carry[1 + n]
            carry = passed(carry, state_ref[i].astype(F32), d)
        ends.append(carry)
    rows = numbered_rows([e[1] for e in ends], [e[2:] for e in ends])
    for z in range(plane_ref.shape[0]):
        for d in range(2):
            plane_ref[z, d * share : (d + 1) * share, :] = ends[d][0].astype(BF16)
        plane_ref[z, NORMERS:, :] = rows


def far_kernel(place_ref, near_ref, planes_ref, start_ref):
    planes, members = planes_ref.shape[0], near_ref.shape[0]
    share = NORMERS // 2
    place = place_ref[0]
    far = []
    for d in range(2):
        carry = nothing(share)
        for z in reversed(range(planes)) if d else range(planes):
            earlier = (z > place) if d else (z < place)
            after = passed(carry, planes_ref[z].astype(F32), d)
            carry = tuple(jnp.where(earlier, a, c) for a, c in zip(after, carry))
        far.append(carry)
    for i in range(members):
        normers, numbers = [], []
        for d in range(2):
            memory, normer, _, most = far[d]
            at = [NORMERS + 2 * n + d for n in range(3)]
            near_normer, head, near_most = (near_ref[i, r : r + 1, :] for r in at)
            moved = most + head
            new = jnp.maximum(moved, near_most)
            far_weight = jnp.exp(moved - new)
            near_weight = jnp.exp(near_most - new)
            near = near_ref[i, d * share : (d + 1) * share, :]
            start_ref[i, d * share : (d + 1) * share, :] = (
                near_weight * near + far_weight * memory
            ).astype(BF16)
            normers.append(near_weight * near_normer + far_weight * normer)
            numbers.append([new])
        rows = [n.astype(BF16) for n in normers]
        for (number,) in numbers:
            rows += in_terms(number)
        rows.append(jnp.zeros((ROWS - NORMERS - len(rows), 128), BF16))
        start_ref[i, NORMERS:, :] = jnp.concatenate(rows, axis=0)


def read_kernel(query_ref, key_ref, value_ref, column_ref, row_ref, gain_ref, start_ref, out_ref):
    length = query_ref.shape[0]
    queries = query_ref[...]
    values = value_ref[...]
    scale = DQK ** (-0.5)
    products = scale * lax.dot_general(
        queries, key_ref[...], (((1,), (1,)), ((), ())), preferred_element_type=F32
    )
    t = lax.broadcasted_iota(jnp.int32, (length, length), 0)
    s = lax.broadcasted_iota(jnp.int32, (length, length), 1)
    share = NORMERS // 2
    last = start_ref[0, NORMERS:, :].astype(F32)
    summed = None
    for d in range(2):
        memory = start_ref[:, d * share : (d + 1) * share, :].reshape(DV, DQK)
        normer = last[d : d + 1]
        stable = from_terms(last, 2 + 3 * d)[:, :1]
        running = column_ref[:, 2 + d : 3 + d]
        seen = (t <= s) if d else (t >= s)
        log_weight = jnp.where(
            seen, running - row_ref[d : d + 1, :] + row_ref[2 + d : 3 + d, :], -jnp.inf
        )
        carried = running + stable
        highest = jnp.maximum(carried, jnp.max(log_weight, axis=-1, keepdims=True))
        scores = products * jnp.exp(log_weight - highest)
        carry_weight = scale * jnp.exp(carried - highest)
        numerator = jnp.dot(scores.astype(BF16), values, preferred_element_type=F32)
        numerator += carry_weight * lax.dot_general(
            queries, memory, (((1,), (1,)), ((), ())), preferred_element_type=F32
        )
        denominator = jnp.sum(scores, axis=-1, keepdims=True)
        denominator += carry_weight * jnp.sum(
            queries.astype(F32) * normer, axis=-1, keepdims=True
        )
        result = numerator / jnp.maximum(jnp.abs(denominator), jnp.exp(-highest))
        summed = result if summed is None else summed + result
    inverse_rms = lax.rsqrt(jnp.mean(summed * summed, axis=-1, keepdims=True) + EPS)
    out = (summed * inverse_rms * gain_ref[...]).astype(BF16)
    for k in range(out_ref.shape[0]):
        out_ref[k] = out


WIDE = DQK + 3 * DV
CHUNKS = 8
AHEAD = 2


def project_kernel(
    normed_ref, edge_ref, tap_ref, whole_ref, query_ref, conv_ref, weight_ref, total_ref, sems
):
    depth = weight_ref.shape[1]
    length = query_ref.shape[0]

    def fetch(k):
        return pltpu.make_async_copy(
            whole_ref.at[pl.ds(k * depth, depth), pl.ds(0, WIDE)], weight_ref.at[k], sems.at[k]
        )

    for k in range(AHEAD):
        fetch(k).start()
    for k in range(CHUNKS):
        fetch(k).wait()
        if k + AHEAD < CHUNKS:
            fetch(k + AHEAD).start()
        at = slice(k * depth, (k + 1) * depth)
        rows = jnp.concatenate([normed_ref[:, at], edge_ref[:, at]], axis=0)
        product = jnp.dot(rows, weight_ref[k], preferred_element_type=F32)
        if k:
            total_ref[...] += product
        else:
            total_ref[...] = product
    query_ref[...] = total_ref[:length, :DQK].astype(BF16)
    inner = total_ref[:, DQK : DQK + DV].astype(BF16).astype(F32)
    given = total_ref[:, DQK + DV : DQK + 2 * DV].astype(BF16).astype(F32)
    outer = total_ref[:length, DQK + 2 * DV :].astype(BF16).astype(F32)
    mixed = (inner * given).astype(BF16).astype(F32)
    here = mixed[:length]
    at = lax.broadcasted_iota(jnp.int32, (length, DV), 0)
    before = jnp.where(at == 0, mixed[length : length + 1], pltpu.roll(here, 1, 0))
    after = jnp.where(
        at == length - 1, mixed[length + 1 : length + 2], pltpu.roll(here, length - 1, 0)
    )
    taps = tap_ref[...].astype(F32)
    filtered = taps[0:1] * before + taps[1:2] * here + taps[2:3] * after
    conv_ref[...] = (outer * filtered).astype(BF16)


def fetch_rows(whole_ref, weight_ref, sems, device, slot):
    return [
        pltpu.make_async_copy(
            whole_ref.at[pl.ds(device, 16), side, :, pl.ds(WIDE, 512)],
            weight_ref.at[slot, side],
            sems.at[slot, side],
        )
        for side in range(2)
    ]


def convolved_kernel(place_ref, *refs):
    parts, (whole_ref, out_ref, weight_ref, sems) = refs[:4], refs[4:]
    place = place_ref[0]
    now = []
    for n, offset in enumerate((0, -1, 1, 2)):
        now.append(fetch_rows(whole_ref, weight_ref, sems, (place + offset + 4) % 4 * 32 + 16, n))
    for pair in now:
        for copy in pair:
            copy.start()
    for n, part_ref in enumerate(parts):
        for side in range(2):
            now[n][side].wait()
            weight = weight_ref[n, side].reshape(DV, 512)
            product = jnp.dot(part_ref[...], weight, preferred_element_type=F32)
            at = slice(side * 512, (side + 1) * 512)
            if n:
                out_ref[:, at] += product
            else:
                out_ref[:, at] = product


def output_kernel(joined_ref, whole_ref, earlier_ref, out_ref, weight_ref, total_ref, sems, sem):
    parts = [fetch_rows(whole_ref, weight_ref, sems, k * 32, k) for k in range(4)]
    for side in range(2):
        for k in range(4):
            parts[k][side].start()
    fetch = pltpu.make_async_copy(earlier_ref, total_ref, sem)
    fetch.start()
    for side in range(2):
        at = slice(side * 512, (side + 1) * 512)
        total = None
        for k in range(4):
            parts[k][side].wait()
            weight = weight_ref[k, side].reshape(DV, 512)
            product = jnp.dot(joined_ref[k], weight, preferred_element_type=F32)
            total = product if total is None else total + product
        if not side:
            fetch.wait()
        out_ref[:, at] = (total + total_ref[:, at]).astype(BF16)


def ring(size, step):
    return [(i, (i + step) % size) for i in range(size)]


def on_core(kernel, out, *operands, scalars=0, remote=0, scratch=(), limit=20, outside=False):
    vmem = pl.BlockSpec(memory_space=pltpu.VMEM)
    smem = pl.BlockSpec(memory_space=pltpu.SMEM)
    hbm = pl.BlockSpec(memory_space=pltpu.HBM)
    return pl.pallas_call(
        kernel,
        out_shape=out,
        in_specs=[smem] * scalars
        + [vmem] * (len(operands) - scalars - remote)
        + [hbm] * remote,
        out_specs=jax.tree.map(lambda _: hbm if outside else vmem, out),
        scratch_shapes=scratch,
        compiler_params=pltpu.CompilerParams(vmem_limit_bytes=limit * 2**20),
    )(*operands)


def body(
    tokens,
    norm_gain,
    w_query,
    w_key,
    w_value,
    w_gates,
    input_bias,
    forget_bias,
    decay_shift,
    head_gain,
    w_conv_b,
    w_conv_c,
    w_conv_in,
    conv_taps,
    w_out,
):
    length = tokens.shape[0]
    size = lax.axis_size(SP)
    planes = lax.axis_size("sp_0")
    members = size // planes
    plane = lax.axis_index("sp_0")
    depth = w_out.shape[0]
    half = w_out.shape[1] // 2
    packed, block = on_core(
        pack_kernel,
        (
            jax.ShapeDtypeStruct((w_key.shape[0], WIDE + half), BF16),
            jax.ShapeDtypeStruct((planes, w_key.shape[0], DQK + DV), BF16),
        ),
        w_query,
        w_key,
        w_value,
        w_conv_b,
        w_conv_c,
        w_conv_in,
        w_out,
        remote=7,
        scratch=[pltpu.SemaphoreType.DMA((6 + 2 * planes,))],
        outside=True,
        limit=63,
    )
    block = swapped(block, "sp_0")
    whole = lax.all_gather(packed, SP, axis=0, tiled=True)
    core = lax.axis_index("sp_2")
    row = lax.axis_index("sp_1")
    normed = row_norm(tokens, norm_gain)

    block, normed = lax.optimization_barrier((block, normed))
    up = down = block
    pieces = [block]
    for k in range(4):
        up = lax.ppermute(up, "sp_1", ring(8, 1))
        pieces.append(up)
        if k < 3:
            down = lax.ppermute(down, "sp_1", ring(8, -1))
            pieces.append(down)
    groups, at = [], 0
    for count in GROUPS:
        groups.append(jnp.stack(pieces[at : at + count]))
        at += count
    for count, group in zip(GROUPS, tuple(groups)):
        groups.append(lax.ppermute(group, "sp_2", ring(2, 1)))

    gates = lax.dot_general(
        w_gates.reshape(-1, 4), normed, (((0,), (1,)), ((), ())), preferred_element_type=F32
    ).reshape(2, 2, length)
    in_gate = gates[:, 0] + input_bias
    log_forget = jax.nn.log_sigmoid(gates[:, 1] + forget_bias) + decay_shift[:, :, 0]
    rows, columns, numbers = on_core(
        gate_kernel,
        (
            jax.ShapeDtypeStruct((4, length), F32),
            jax.ShapeDtypeStruct((length, 8), F32),
            jax.ShapeDtypeStruct((4, 128), F32),
        ),
        log_forget,
        in_gate,
    )
    block = jax.ShapeDtypeStruct((members, ROWS, 128), BF16)
    state, keys, values = on_core(
        state_kernel,
        (
            block,
            jax.ShapeDtypeStruct((length, DQK), BF16),
            jax.ShapeDtypeStruct((length, DV), BF16),
        ),
        jnp.stack([core, row]),
        normed,
        columns,
        numbers,
        *groups,
        scalars=1,
        scratch=[pltpu.VMEM((normed.shape[1], DQK + DV), BF16)],
    )
    last, initial, keys = lax.optimization_barrier((normed[-1:], normed[:1], keys))
    state = swapped(state, PLANE)
    before, after = neighbour_rows(last, initial)
    edges = jnp.concatenate([before, after, jnp.zeros((14, normed.shape[1]), BF16)], axis=0)
    near, plane_state = on_core(
        plane_kernel,
        (
            jax.ShapeDtypeStruct((members, ROWS, 128), F32),
            jax.ShapeDtypeStruct((planes, ROWS, 128), BF16),
        ),
        state,
    )
    far = swapped(plane_state, "sp_0")
    queries, conv_out = on_core(
        project_kernel,
        (
            jax.ShapeDtypeStruct((length, DQK), BF16),
            jax.ShapeDtypeStruct((length, DV), BF16),
        ),
        normed,
        edges,
        conv_taps,
        whole,
        remote=1,
        scratch=[
            pltpu.VMEM((CHUNKS, whole.shape[0] // CHUNKS, WIDE), BF16),
            pltpu.VMEM((length + edges.shape[0], WIDE), F32),
            pltpu.SemaphoreType.DMA((CHUNKS,)),
        ],
        limit=54,
    )
    start = on_core(far_kernel, block, plane[None], near, far, scalars=1)
    start = swapped(start, PLANE)
    parts = [conv_out] + [lax.ppermute(conv_out, "tp", ring(4, n)) for n in (1, -1, 2)]
    start, *parts[:3] = lax.optimization_barrier((start, *parts[:3]))
    lstm_out = on_core(
        read_kernel,
        jax.ShapeDtypeStruct((4, length, DV), BF16),
        queries,
        keys,
        values,
        columns,
        rows,
        head_gain[None],
        start,
    )
    lstm_all = swapped(lstm_out, "tp")
    whole = whole.reshape(size, 2, depth, -1)
    done = on_core(
        convolved_kernel,
        jax.ShapeDtypeStruct((length, 2 * half), F32),
        lax.axis_index("tp")[None],
        *parts,
        whole,
        scalars=1,
        remote=1,
        scratch=[
            pltpu.VMEM((4, 2, 16, depth, half), BF16),
            pltpu.SemaphoreType.DMA((4, 2)),
        ],
        limit=54,
    )
    return on_core(
        output_kernel,
        jax.ShapeDtypeStruct((length, 2 * half), BF16),
        lstm_all,
        whole,
        done,
        remote=2,
        scratch=[
            pltpu.VMEM((4, 2, 16, depth, half), BF16),
            pltpu.VMEM(done.shape, F32),
            pltpu.SemaphoreType.DMA((4, 2)),
            pltpu.SemaphoreType.DMA,
        ],
        limit=53,
    )


def solution(mesh):
    torus = Mesh(mesh.devices.reshape(8, 8, 2, mesh.shape["tp"]), (*SP, "tp"))
    placed = (
        P(SP, None),
        P(),
        P(SP, "tp"),
        P(SP, "tp"),
        P(SP, "tp"),
        P(None, None, None, "tp"),
        P(None, "tp"),
        P(None, "tp"),
        P(None, SP, "tp"),
        P("tp"),
        P(SP, "tp"),
        P(SP, "tp"),
        P(SP, "tp"),
        P(None, "tp"),
        P(SP, "tp"),
    )

    return jax.shard_map(body, mesh=torus, in_specs=placed, out_specs=P(SP, "tp"), check_vma=False)
```

```python
import jax
import jax.numpy as jnp
from jax import lax
from jax.experimental import pallas as pl
from jax.experimental.pallas import tpu as pltpu
from jax.sharding import Mesh
from jax.sharding import PartitionSpec as P


DQK = 128
DV = 256
SP = ("sp_0", "sp_1", "sp_2")
PLANE = ("sp_1", "sp_2")
EPS = 1e-06
LOWEST = -1e30
F32 = jnp.float32
BF16 = jnp.bfloat16


def row_norm(tokens, norm_gain):
    values = tokens.astype(F32)
    inverse_rms = lax.rsqrt(jnp.mean(values * values, axis=-1, keepdims=True) + EPS)
    return (values * inverse_rms * norm_gain).astype(BF16)


def swapped(value, axes):
    return lax.all_to_all(value, axes, split_axis=0, concat_axis=0, tiled=True)


def neighbour_rows(last, initial):
    size = lax.axis_size(SP)
    up = [(i, i + 1) for i in range(size - 1)]
    before = lax.ppermute(last, SP, up)
    after = lax.ppermute(initial, SP, [(j, i) for i, j in up])
    return before, after


ROWS = 48
NORMERS = 32
NUMBERS = (34, 40)


def in_terms(number):
    high = number.astype(BF16)
    rest = number - high.astype(F32)
    middle = rest.astype(BF16)
    low = (rest - middle.astype(F32)).astype(BF16)
    return [high, middle, low]


def from_terms(block, row):
    return block[row : row + 1] + block[row + 1 : row + 2] + block[row + 2 : row + 3]


def numbered_rows(normers, numbers):
    rows = [n.astype(BF16) for n in normers]
    for pair in numbers:
        for number in pair:
            rows += in_terms(number)
    rows.append(jnp.zeros((ROWS - NORMERS - len(rows), 128), BF16))
    return jnp.concatenate(rows, axis=0)


ARRIVAL = (0, -1, 1, -2, 2, -3, 3, -4)
GROUPS = (3, 4, 1)


def gate_kernel(forget_ref, gate_ref, row_ref, column_ref, number_ref):
    length = forget_ref.shape[1]
    at = lax.broadcasted_iota(jnp.int32, (1, length), 1)
    running, update, numbers = [], [], []
    for d in range(2):
        value = forget_ref[d : d + 1]
        step = 1
        while step < length:
            moved = pltpu.roll(value, length - step if d else step, 1)
            inside = (at < length - step) if d else (at >= step)
            value = value + jnp.where(inside, moved, 0.0)
            step *= 2
        total = value[:, :1] if d else value[:, length - 1 :]
        log_update = total - value + gate_ref[d : d + 1]
        most = jnp.max(log_update, axis=1, keepdims=True)
        running.append(value)
        update.append(jnp.exp(log_update - most))
        numbers += [total, most]
    row_ref[...] = jnp.concatenate([*running, gate_ref[...]], axis=0)
    column_ref[...] = jnp.concatenate([*update, *running, *update, *running], axis=0).T
    for n, number in enumerate(numbers):
        number_ref[n : n + 1] = jnp.broadcast_to(number, (1, 128))


def state_kernel(place_ref, normed_ref, update_ref, number_ref, *refs):
    groups = len(GROUPS)
    state_ref, key_ref, value_ref, weight_ref = refs[2 * groups :]
    core, row = place_ref[0], place_ref[1]
    for side in range(2):
        cell = 1 - core if side else core
        arrivals = iter(ARRIVAL)
        for group_ref in refs[side * groups : (side + 1) * groups]:
            _, planes, depth, _ = group_ref.shape
            for k in range(group_ref.shape[0]):
                y = (row + next(arrivals) + 8) % 8
                for z in range(planes):
                    start = ((z * 8 + y) * 2 + cell) * depth
                    weight_ref[pl.ds(pl.multiple_of(start, depth), depth), :] = group_ref[k, z]
    both = jnp.dot(normed_ref[...], weight_ref[...], preferred_element_type=F32)
    both = both.astype(BF16)
    keys, values = both[:, :DQK], both[:, DQK:]
    key_ref[...] = keys
    value_ref[...] = values
    members = state_ref.shape[0]
    share = DV // members
    normers = []
    for d in range(2):
        weighted = keys.astype(F32) * update_ref[:, d : d + 1]
        normers.append(jnp.sum(weighted, axis=0, keepdims=True))
        memory = lax.dot_general(
            values, weighted.astype(BF16), (((0,), (0,)), ((), ())), preferred_element_type=F32
        )
        state_ref[:, d * share : (d + 1) * share, :] = memory.astype(BF16).reshape(
            members, share, DQK
        )
    numbers = [[number_ref[2 * d + n : 2 * d + n + 1] for n in range(2)] for d in range(2)]
    rows = numbered_rows(normers, numbers)
    for j in range(members):
        state_ref[j, NORMERS:, :] = rows


def passed(carry, block, d):
    memory, normer, total, most = carry
    block_total = from_terms(block, NUMBERS[d])
    block_most = from_terms(block, NUMBERS[d] + 3)
    new = jnp.maximum(most + block_total, block_most)
    old_weight = jnp.exp(most + block_total - new)
    block_weight = jnp.exp(block_most - new)
    share = memory.shape[0]
    memory = old_weight * memory + block_weight * block[d * share : (d + 1) * share]
    normer = old_weight * normer + block_weight * block[NORMERS + d : NORMERS + d + 1]
    return memory, normer, total + block_total, new


def nothing(share):
    row = jnp.zeros((1, 128), F32)
    return jnp.zeros((share, 128), F32), row, row, jnp.full((1, 128), LOWEST, F32)


def plane_kernel(state_ref, near_ref, plane_ref):
    members = state_ref.shape[0]
    share = NORMERS // 2
    ends = []
    for d in range(2):
        carry = nothing(share)
        for i in reversed(range(members)) if d else range(members):
            near_ref[i, d * share : (d + 1) * share, :] = carry[0]
            for n in range(3):
                near_ref[i, NORMERS + 2 * n + d : NORMERS + 2 * n + d + 1, :] = carry[1 + n]
            carry = passed(carry, state_ref[i].astype(F32), d)
        ends.append(carry)
    rows = numbered_rows([e[1] for e in ends], [e[2:] for e in ends])
    for z in range(plane_ref.shape[0]):
        for d in range(2):
            plane_ref[z, d * share : (d + 1) * share, :] = ends[d][0].astype(BF16)
        plane_ref[z, NORMERS:, :] = rows


def far_kernel(place_ref, near_ref, planes_ref, start_ref):
    planes, members = planes_ref.shape[0], near_ref.shape[0]
    share = NORMERS // 2
    place = place_ref[0]
    far = []
    for d in range(2):
        carry = nothing(share)
        for z in reversed(range(planes)) if d else range(planes):
            earlier = (z > place) if d else (z < place)
            after = passed(carry, planes_ref[z].astype(F32), d)
            carry = tuple(jnp.where(earlier, a, c) for a, c in zip(after, carry))
        far.append(carry)
    for i in range(members):
        normers, numbers = [], []
        for d in range(2):
            memory, normer, _, most = far[d]
            at = [NORMERS + 2 * n + d for n in range(3)]
            near_normer, head, near_most = (near_ref[i, r : r + 1, :] for r in at)
            moved = most + head
            new = jnp.maximum(moved, near_most)
            far_weight = jnp.exp(moved - new)
            near_weight = jnp.exp(near_most - new)
            near = near_ref[i, d * share : (d + 1) * share, :]
            start_ref[i, d * share : (d + 1) * share, :] = (
                near_weight * near + far_weight * memory
            ).astype(BF16)
            normers.append(near_weight * near_normer + far_weight * normer)
            numbers.append([new])
        rows = [n.astype(BF16) for n in normers]
        for (number,) in numbers:
            rows += in_terms(number)
        rows.append(jnp.zeros((ROWS - NORMERS - len(rows), 128), BF16))
        start_ref[i, NORMERS:, :] = jnp.concatenate(rows, axis=0)


def read_kernel(query_ref, key_ref, value_ref, column_ref, row_ref, gain_ref, conv_ref, start_ref, out_ref):
    length = query_ref.shape[0]
    queries = query_ref[...]
    values = value_ref[...]
    scale = DQK ** (-0.5)
    products = scale * lax.dot_general(
        queries, key_ref[...], (((1,), (1,)), ((), ())), preferred_element_type=F32
    )
    t = lax.broadcasted_iota(jnp.int32, (length, length), 0)
    s = lax.broadcasted_iota(jnp.int32, (length, length), 1)
    share = NORMERS // 2
    last = start_ref[0, NORMERS:, :].astype(F32)
    summed = None
    for d in range(2):
        memory = start_ref[:, d * share : (d + 1) * share, :].reshape(DV, DQK)
        normer = last[d : d + 1]
        stable = from_terms(last, 2 + 3 * d)[:, :1]
        running = column_ref[:, 2 + d : 3 + d]
        seen = (t <= s) if d else (t >= s)
        log_weight = jnp.where(
            seen, running - row_ref[d : d + 1, :] + row_ref[2 + d : 3 + d, :], -jnp.inf
        )
        carried = running + stable
        highest = jnp.maximum(carried, jnp.max(log_weight, axis=-1, keepdims=True))
        scores = products * jnp.exp(log_weight - highest)
        carry_weight = scale * jnp.exp(carried - highest)
        numerator = jnp.dot(scores.astype(BF16), values, preferred_element_type=F32)
        numerator += carry_weight * lax.dot_general(
            queries, memory, (((1,), (1,)), ((), ())), preferred_element_type=F32
        )
        denominator = jnp.sum(scores, axis=-1, keepdims=True)
        denominator += carry_weight * jnp.sum(
            queries.astype(F32) * normer, axis=-1, keepdims=True
        )
        result = numerator / jnp.maximum(jnp.abs(denominator), jnp.exp(-highest))
        summed = result if summed is None else summed + result
    inverse_rms = lax.rsqrt(jnp.mean(summed * summed, axis=-1, keepdims=True) + EPS)
    out = (summed * inverse_rms * gain_ref[...]).astype(BF16)
    for k in range(out_ref.shape[0]):
        out_ref[k, :, :DV] = out
        out_ref[k, :, DV:] = conv_ref[...]


WIDE = DQK + 3 * DV
CHUNKS = 8
AHEAD = 4


def project_kernel(
    normed_ref, edge_ref, tap_ref, whole_ref, query_ref, conv_ref, weight_ref, total_ref, sems
):
    depth = weight_ref.shape[1]
    length = query_ref.shape[0]

    def fetch(k):
        return pltpu.make_async_copy(
            whole_ref.at[pl.ds(k * depth, depth), pl.ds(0, WIDE)], weight_ref.at[k], sems.at[k]
        )

    for k in range(AHEAD):
        fetch(k).start()
    for k in range(CHUNKS):
        fetch(k).wait()
        if k + AHEAD < CHUNKS:
            fetch(k + AHEAD).start()
        at = slice(k * depth, (k + 1) * depth)
        rows = jnp.concatenate([normed_ref[:, at], edge_ref[:, at]], axis=0)
        product = jnp.dot(rows, weight_ref[k], preferred_element_type=F32)
        if k:
            total_ref[...] += product
        else:
            total_ref[...] = product
    query_ref[...] = total_ref[:length, :DQK].astype(BF16)
    inner = total_ref[:, DQK : DQK + DV].astype(BF16).astype(F32)
    given = total_ref[:, DQK + DV : DQK + 2 * DV].astype(BF16).astype(F32)
    outer = total_ref[:length, DQK + 2 * DV :].astype(BF16).astype(F32)
    mixed = (inner * given).astype(BF16).astype(F32)
    here = mixed[:length]
    at = lax.broadcasted_iota(jnp.int32, (length, DV), 0)
    before = jnp.where(at == 0, mixed[length : length + 1], pltpu.roll(here, 1, 0))
    after = jnp.where(
        at == length - 1, mixed[length + 1 : length + 2], pltpu.roll(here, length - 1, 0)
    )
    taps = tap_ref[...].astype(F32)
    filtered = taps[0:1] * before + taps[1:2] * here + taps[2:3] * after
    conv_ref[...] = (outer * filtered).astype(BF16)


def output_kernel(joined_ref, whole_ref, out_ref, weight_ref, sems):
    blocks = joined_ref.shape[0]
    share = whole_ref.shape[0] // blocks

    def fetch(n):
        side, k = divmod(n, blocks)
        return pltpu.make_async_copy(
            whole_ref.at[pl.ds(k * share, share), side, :, pl.ds(WIDE, 512)],
            weight_ref.at[n],
            sems.at[n],
        )

    for n in range(3):
        fetch(n).start()
    for side in range(2):
        total = None
        for k in range(blocks):
            n = side * blocks + k
            fetch(n).wait()
            if n + 3 < 2 * blocks:
                fetch(n + 3).start()
            weight = weight_ref[n].reshape(2 * DV, 512)
            product = jnp.dot(joined_ref[k], weight, preferred_element_type=F32)
            total = product if total is None else total + product
        out_ref[:, side * 512 : (side + 1) * 512] = total.astype(BF16)


def ring(size, step):
    return [(i, (i + step) % size) for i in range(size)]


def on_core(kernel, out, *operands, scalars=0, remote=0, scratch=(), limit=20):
    vmem = pl.BlockSpec(memory_space=pltpu.VMEM)
    smem = pl.BlockSpec(memory_space=pltpu.SMEM)
    hbm = pl.BlockSpec(memory_space=pltpu.HBM)
    return pl.pallas_call(
        kernel,
        out_shape=out,
        in_specs=[smem] * scalars
        + [vmem] * (len(operands) - scalars - remote)
        + [hbm] * remote,
        out_specs=jax.tree.map(lambda _: vmem, out),
        scratch_shapes=scratch,
        compiler_params=pltpu.CompilerParams(vmem_limit_bytes=limit * 2**20),
    )(*operands)


def body(
    tokens,
    norm_gain,
    w_query,
    w_key,
    w_value,
    w_gates,
    input_bias,
    forget_bias,
    decay_shift,
    head_gain,
    w_conv_b,
    w_conv_c,
    w_conv_in,
    conv_taps,
    w_out,
):
    length = tokens.shape[0]
    size = lax.axis_size(SP)
    planes = lax.axis_size("sp_0")
    members = size // planes
    plane = lax.axis_index("sp_0")
    depth = w_out.shape[0]
    half = w_out.shape[1] // 2
    out_rows = jnp.concatenate([w_out[:, :half], w_out[:, half:]], axis=0)
    packed = jnp.concatenate([w_query, w_conv_c, w_conv_in, w_conv_b, out_rows], axis=1)
    block = jnp.concatenate([w_key, w_value], axis=1)
    block = jnp.broadcast_to(block, (planes, *block.shape))
    block = swapped(block, "sp_0")
    whole = lax.all_gather(packed, SP, axis=0, tiled=True)
    core = lax.axis_index("sp_2")
    row = lax.axis_index("sp_1")
    normed = row_norm(tokens, norm_gain)

    block, normed = lax.optimization_barrier((block, normed))
    up = down = block
    pieces = [block]
    for k in range(4):
        up = lax.ppermute(up, "sp_1", ring(8, 1))
        pieces.append(up)
        if k < 3:
            down = lax.ppermute(down, "sp_1", ring(8, -1))
            pieces.append(down)
    groups, at = [], 0
    for count in GROUPS:
        groups.append(jnp.stack(pieces[at : at + count]))
        at += count
    for count, group in zip(GROUPS, tuple(groups)):
        groups.append(lax.ppermute(group, "sp_2", ring(2, 1)))

    gates = lax.dot_general(
        w_gates.reshape(-1, 4), normed, (((0,), (1,)), ((), ())), preferred_element_type=F32
    ).reshape(2, 2, length)
    in_gate = gates[:, 0] + input_bias
    log_forget = jax.nn.log_sigmoid(gates[:, 1] + forget_bias) + decay_shift[:, :, 0]
    rows, columns, numbers = on_core(
        gate_kernel,
        (
            jax.ShapeDtypeStruct((4, length), F32),
            jax.ShapeDtypeStruct((length, 8), F32),
            jax.ShapeDtypeStruct((4, 128), F32),
        ),
        log_forget,
        in_gate,
    )
    block = jax.ShapeDtypeStruct((members, ROWS, 128), BF16)
    state, keys, values = on_core(
        state_kernel,
        (
            block,
            jax.ShapeDtypeStruct((length, DQK), BF16),
            jax.ShapeDtypeStruct((length, DV), BF16),
        ),
        jnp.stack([core, row]),
        normed,
        columns,
        numbers,
        *groups,
        scalars=1,
        scratch=[pltpu.VMEM((normed.shape[1], DQK + DV), BF16)],
    )
    last, initial, keys = lax.optimization_barrier((normed[-1:], normed[:1], keys))
    state = swapped(state, PLANE)
    before, after = neighbour_rows(last, initial)
    edges = jnp.concatenate([before, after, jnp.zeros((14, normed.shape[1]), BF16)], axis=0)
    near, plane_state = on_core(
        plane_kernel,
        (
            jax.ShapeDtypeStruct((members, ROWS, 128), F32),
            jax.ShapeDtypeStruct((planes, ROWS, 128), BF16),
        ),
        state,
    )
    far = swapped(plane_state, "sp_0")
    queries, conv_out = on_core(
        project_kernel,
        (
            jax.ShapeDtypeStruct((length, DQK), BF16),
            jax.ShapeDtypeStruct((length, DV), BF16),
        ),
        normed,
        edges,
        conv_taps,
        whole,
        remote=1,
        scratch=[
            pltpu.VMEM((CHUNKS, whole.shape[0] // CHUNKS, WIDE), BF16),
            pltpu.VMEM((length + edges.shape[0], WIDE), F32),
            pltpu.SemaphoreType.DMA((CHUNKS,)),
        ],
        limit=54,
    )
    start = on_core(far_kernel, block, plane[None], near, far, scalars=1)
    start = swapped(start, PLANE)
    joined = on_core(
        read_kernel,
        jax.ShapeDtypeStruct((4, length, 2 * DV), BF16),
        queries,
        keys,
        values,
        columns,
        rows,
        head_gain[None],
        conv_out,
        start,
    )
    joined = swapped(joined, "tp")
    return on_core(
        output_kernel,
        jax.ShapeDtypeStruct((length, 2 * half), BF16),
        joined,
        whole.reshape(size, 2, depth, -1),
        remote=1,
        scratch=[
            pltpu.VMEM((8, size // 4, depth, half), BF16),
            pltpu.SemaphoreType.DMA((8,)),
        ],
        limit=53,
    )


def solution(mesh):
    torus = Mesh(mesh.devices.reshape(8, 8, 2, mesh.shape["tp"]), (*SP, "tp"))
    placed = (
        P(SP, None),
        P(),
        P(SP, "tp"),
        P(SP, "tp"),
        P(SP, "tp"),
        P(None, None, None, "tp"),
        P(None, "tp"),
        P(None, "tp"),
        P(None, SP, "tp"),
        P("tp"),
        P(SP, "tp"),
        P(SP, "tp"),
        P(SP, "tp"),
        P(None, "tp"),
        P(SP, "tp"),
    )

    return jax.shard_map(body, mesh=torus, in_specs=placed, out_specs=P(SP, "tp"), check_vma=False)
```

```python
import jax
import jax.numpy as jnp
from jax import lax
from jax.experimental import pallas as pl
from jax.experimental.pallas import tpu as pltpu
from jax.sharding import Mesh
from jax.sharding import PartitionSpec as P


DQK = 128
DV = 256
SP = ("sp_0", "sp_1", "sp_2")
PLANE = ("sp_1", "sp_2")
EPS = 1e-06
LOWEST = -1e30
F32 = jnp.float32
BF16 = jnp.bfloat16


def row_norm(tokens, norm_gain):
    values = tokens.astype(F32)
    inverse_rms = lax.rsqrt(jnp.mean(values * values, axis=-1, keepdims=True) + EPS)
    return (values * inverse_rms * norm_gain).astype(BF16)


def swapped(value, axes):
    return lax.all_to_all(value, axes, split_axis=0, concat_axis=0, tiled=True)


def neighbour_rows(last, initial):
    size = lax.axis_size(SP)
    up = [(i, i + 1) for i in range(size - 1)]
    before = lax.ppermute(last, SP, up)
    after = lax.ppermute(initial, SP, [(j, i) for i, j in up])
    return before, after


ROWS = 48
NORMERS = 32
NUMBERS = (34, 40)


def in_terms(number):
    high = number.astype(BF16)
    rest = number - high.astype(F32)
    middle = rest.astype(BF16)
    low = (rest - middle.astype(F32)).astype(BF16)
    return [high, middle, low]


def from_terms(block, row):
    return block[row : row + 1] + block[row + 1 : row + 2] + block[row + 2 : row + 3]


def numbered_rows(normers, numbers):
    rows = [n.astype(BF16) for n in normers]
    for pair in numbers:
        for number in pair:
            rows += in_terms(number)
    rows.append(jnp.zeros((ROWS - NORMERS - len(rows), 128), BF16))
    return jnp.concatenate(rows, axis=0)


ARRIVAL = (0, -1, 1, -2, 2, -3, 3, -4)
GROUPS = (3, 4, 1)


def pack_kernel(query_ref, key_ref, value_ref, outer_ref, inner_ref, given_ref, out_ref, whole_ref, block_ref):
    at = 0
    for ref in (query_ref, inner_ref, given_ref, outer_ref):
        whole_ref[:, at : at + ref.shape[1]] = ref[...]
        at += ref.shape[1]
    depth, columns = out_ref.shape
    for side in range(2):
        whole_ref[side * depth : (side + 1) * depth, at:] = out_ref[
            :, side * columns // 2 : (side + 1) * columns // 2
        ]
    for z in range(block_ref.shape[0]):
        block_ref[z, :, :DQK] = key_ref[...]
        block_ref[z, :, DQK:] = value_ref[...]


def gate_kernel(forget_ref, gate_ref, row_ref, column_ref, number_ref):
    length = forget_ref.shape[1]
    at = lax.broadcasted_iota(jnp.int32, (1, length), 1)
    running, update, numbers = [], [], []
    for d in range(2):
        value = forget_ref[d : d + 1]
        step = 1
        while step < length:
            moved = pltpu.roll(value, length - step if d else step, 1)
            inside = (at < length - step) if d else (at >= step)
            value = value + jnp.where(inside, moved, 0.0)
            step *= 2
        total = value[:, :1] if d else value[:, length - 1 :]
        log_update = total - value + gate_ref[d : d + 1]
        most = jnp.max(log_update, axis=1, keepdims=True)
        running.append(value)
        update.append(jnp.exp(log_update - most))
        numbers += [total, most]
    row_ref[...] = jnp.concatenate([*running, gate_ref[...]], axis=0)
    column_ref[...] = jnp.concatenate([*update, *running, *update, *running], axis=0).T
    for n, number in enumerate(numbers):
        number_ref[n : n + 1] = jnp.broadcast_to(number, (1, 128))


def state_kernel(place_ref, normed_ref, update_ref, number_ref, *refs):
    groups = len(GROUPS)
    state_ref, key_ref, value_ref, weight_ref = refs[2 * groups :]
    core, row = place_ref[0], place_ref[1]
    for side in range(2):
        cell = 1 - core if side else core
        arrivals = iter(ARRIVAL)
        for group_ref in refs[side * groups : (side + 1) * groups]:
            _, planes, depth, _ = group_ref.shape
            for k in range(group_ref.shape[0]):
                y = (row + next(arrivals) + 8) % 8
                for z in range(planes):
                    start = ((z * 8 + y) * 2 + cell) * depth
                    weight_ref[pl.ds(pl.multiple_of(start, depth), depth), :] = group_ref[k, z]
    both = jnp.dot(normed_ref[...], weight_ref[...], preferred_element_type=F32)
    both = both.astype(BF16)
    keys, values = both[:, :DQK], both[:, DQK:]
    key_ref[...] = keys
    value_ref[...] = values
    members = state_ref.shape[0]
    share = DV // members
    normers = []
    for d in range(2):
        weighted = keys.astype(F32) * update_ref[:, d : d + 1]
        normers.append(jnp.sum(weighted, axis=0, keepdims=True))
        memory = lax.dot_general(
            values, weighted.astype(BF16), (((0,), (0,)), ((), ())), preferred_element_type=F32
        )
        state_ref[:, d * share : (d + 1) * share, :] = memory.astype(BF16).reshape(
            members, share, DQK
        )
    numbers = [[number_ref[2 * d + n : 2 * d + n + 1] for n in range(2)] for d in range(2)]
    rows = numbered_rows(normers, numbers)
    for j in range(members):
        state_ref[j, NORMERS:, :] = rows


def passed(carry, block, d):
    memory, normer, total, most = carry
    block_total = from_terms(block, NUMBERS[d])
    block_most = from_terms(block, NUMBERS[d] + 3)
    new = jnp.maximum(most + block_total, block_most)
    old_weight = jnp.exp(most + block_total - new)
    block_weight = jnp.exp(block_most - new)
    share = memory.shape[0]
    memory = old_weight * memory + block_weight * block[d * share : (d + 1) * share]
    normer = old_weight * normer + block_weight * block[NORMERS + d : NORMERS + d + 1]
    return memory, normer, total + block_total, new


def nothing(share):
    row = jnp.zeros((1, 128), F32)
    return jnp.zeros((share, 128), F32), row, row, jnp.full((1, 128), LOWEST, F32)


def plane_kernel(state_ref, near_ref, plane_ref):
    members = state_ref.shape[0]
    share = NORMERS // 2
    ends = []
    for d in range(2):
        carry = nothing(share)
        for i in reversed(range(members)) if d else range(members):
            near_ref[i, d * share : (d + 1) * share, :] = carry[0]
            for n in range(3):
                near_ref[i, NORMERS + 2 * n + d : NORMERS + 2 * n + d + 1, :] = carry[1 + n]
            carry = passed(carry, state_ref[i].astype(F32), d)
        ends.append(carry)
    rows = numbered_rows([e[1] for e in ends], [e[2:] for e in ends])
    for z in range(plane_ref.shape[0]):
        for d in range(2):
            plane_ref[z, d * share : (d + 1) * share, :] = ends[d][0].astype(BF16)
        plane_ref[z, NORMERS:, :] = rows


def far_kernel(place_ref, near_ref, planes_ref, start_ref):
    planes, members = planes_ref.shape[0], near_ref.shape[0]
    share = NORMERS // 2
    place = place_ref[0]
    far = []
    for d in range(2):
        carry = nothing(share)
        for z in reversed(range(planes)) if d else range(planes):
            earlier = (z > place) if d else (z < place)
            after = passed(carry, planes_ref[z].astype(F32), d)
            carry = tuple(jnp.where(earlier, a, c) for a, c in zip(after, carry))
        far.append(carry)
    for i in range(members):
        normers, numbers = [], []
        for d in range(2):
            memory, normer, _, most = far[d]
            at = [NORMERS + 2 * n + d for n in range(3)]
            near_normer, head, near_most = (near_ref[i, r : r + 1, :] for r in at)
            moved = most + head
            new = jnp.maximum(moved, near_most)
            far_weight = jnp.exp(moved - new)
            near_weight = jnp.exp(near_most - new)
            near = near_ref[i, d * share : (d + 1) * share, :]
            start_ref[i, d * share : (d + 1) * share, :] = (
                near_weight * near + far_weight * memory
            ).astype(BF16)
            normers.append(near_weight * near_normer + far_weight * normer)
            numbers.append([new])
        rows = [n.astype(BF16) for n in normers]
        for (number,) in numbers:
            rows += in_terms(number)
        rows.append(jnp.zeros((ROWS - NORMERS - len(rows), 128), BF16))
        start_ref[i, NORMERS:, :] = jnp.concatenate(rows, axis=0)


def read_kernel(query_ref, key_ref, value_ref, column_ref, row_ref, gain_ref, conv_ref, start_ref, out_ref):
    length = query_ref.shape[0]
    queries = query_ref[...]
    values = value_ref[...]
    scale = DQK ** (-0.5)
    products = scale * lax.dot_general(
        queries, key_ref[...], (((1,), (1,)), ((), ())), preferred_element_type=F32
    )
    t = lax.broadcasted_iota(jnp.int32, (length, length), 0)
    s = lax.broadcasted_iota(jnp.int32, (length, length), 1)
    share = NORMERS // 2
    last = start_ref[0, NORMERS:, :].astype(F32)
    summed = None
    for d in range(2):
        memory = start_ref[:, d * share : (d + 1) * share, :].reshape(DV, DQK)
        normer = last[d : d + 1]
        stable = from_terms(last, 2 + 3 * d)[:, :1]
        running = column_ref[:, 2 + d : 3 + d]
        seen = (t <= s) if d else (t >= s)
        log_weight = jnp.where(
            seen, running - row_ref[d : d + 1, :] + row_ref[2 + d : 3 + d, :], -jnp.inf
        )
        carried = running + stable
        highest = jnp.maximum(carried, jnp.max(log_weight, axis=-1, keepdims=True))
        scores = products * jnp.exp(log_weight - highest)
        carry_weight = scale * jnp.exp(carried - highest)
        numerator = jnp.dot(scores.astype(BF16), values, preferred_element_type=F32)
        numerator += carry_weight * lax.dot_general(
            queries, memory, (((1,), (1,)), ((), ())), preferred_element_type=F32
        )
        denominator = jnp.sum(scores, axis=-1, keepdims=True)
        denominator += carry_weight * jnp.sum(
            queries.astype(F32) * normer, axis=-1, keepdims=True
        )
        result = numerator / jnp.maximum(jnp.abs(denominator), jnp.exp(-highest))
        summed = result if summed is None else summed + result
    inverse_rms = lax.rsqrt(jnp.mean(summed * summed, axis=-1, keepdims=True) + EPS)
    out = (summed * inverse_rms * gain_ref[...]).astype(BF16)
    for k in range(out_ref.shape[0]):
        out_ref[k, :, :DV] = out
        out_ref[k, :, DV:] = conv_ref[...]


WIDE = DQK + 3 * DV
CHUNKS = 8
AHEAD = 4


def project_kernel(
    normed_ref, edge_ref, tap_ref, whole_ref, query_ref, conv_ref, weight_ref, total_ref, sems
):
    depth = weight_ref.shape[1]
    length = query_ref.shape[0]

    def fetch(k):
        return pltpu.make_async_copy(
            whole_ref.at[pl.ds(k * depth, depth)], weight_ref.at[k], sems.at[k]
        )

    for k in range(AHEAD):
        fetch(k).start()
    for k in range(CHUNKS):
        fetch(k).wait()
        if k + AHEAD < CHUNKS:
            fetch(k + AHEAD).start()
        at = slice(k * depth, (k + 1) * depth)
        rows = jnp.concatenate([normed_ref[:, at], edge_ref[:, at]], axis=0)
        product = jnp.dot(rows, weight_ref[k, :, :WIDE], preferred_element_type=F32)
        if k:
            total_ref[...] += product
        else:
            total_ref[...] = product
    query_ref[...] = total_ref[:length, :DQK].astype(BF16)
    inner = total_ref[:, DQK : DQK + DV].astype(BF16).astype(F32)
    given = total_ref[:, DQK + DV : DQK + 2 * DV].astype(BF16).astype(F32)
    outer = total_ref[:length, DQK + 2 * DV :].astype(BF16).astype(F32)
    mixed = (inner * given).astype(BF16).astype(F32)
    here = mixed[:length]
    at = lax.broadcasted_iota(jnp.int32, (length, DV), 0)
    before = jnp.where(at == 0, mixed[length : length + 1], pltpu.roll(here, 1, 0))
    after = jnp.where(
        at == length - 1, mixed[length + 1 : length + 2], pltpu.roll(here, length - 1, 0)
    )
    taps = tap_ref[...].astype(F32)
    filtered = taps[0:1] * before + taps[1:2] * here + taps[2:3] * after
    conv_ref[...] = (outer * filtered).astype(BF16)


def output_kernel(joined_ref, left_ref, right_ref, out_ref):
    for side, weight_ref in enumerate((left_ref, right_ref)):
        total = None
        for k in range(joined_ref.shape[0]):
            product = jnp.dot(joined_ref[k], weight_ref[k], preferred_element_type=F32)
            total = product if total is None else total + product
        out_ref[:, side * 512 : (side + 1) * 512] = total.astype(BF16)


def ring(size, step):
    return [(i, (i + step) % size) for i in range(size)]


def on_core(kernel, out, *operands, scalars=0, remote=0, scratch=(), limit=20):
    vmem = pl.BlockSpec(memory_space=pltpu.VMEM)
    smem = pl.BlockSpec(memory_space=pltpu.SMEM)
    hbm = pl.BlockSpec(memory_space=pltpu.HBM)
    return pl.pallas_call(
        kernel,
        out_shape=out,
        in_specs=[smem] * scalars
        + [vmem] * (len(operands) - scalars - remote)
        + [hbm] * remote,
        out_specs=jax.tree.map(lambda _: vmem, out),
        scratch_shapes=scratch,
        compiler_params=pltpu.CompilerParams(vmem_limit_bytes=limit * 2**20),
    )(*operands)


def body(
    tokens,
    norm_gain,
    w_query,
    w_key,
    w_value,
    w_gates,
    input_bias,
    forget_bias,
    decay_shift,
    head_gain,
    w_conv_b,
    w_conv_c,
    w_conv_in,
    conv_taps,
    w_out,
):
    length = tokens.shape[0]
    size = lax.axis_size(SP)
    planes = lax.axis_size("sp_0")
    members = size // planes
    plane = lax.axis_index("sp_0")
    depth = w_out.shape[0]
    half = w_out.shape[1] // 2
    packed, block = on_core(
        pack_kernel,
        (
            jax.ShapeDtypeStruct((w_key.shape[0], WIDE + half), BF16),
            jax.ShapeDtypeStruct((planes, w_key.shape[0], DQK + DV), BF16),
        ),
        w_query,
        w_key,
        w_value,
        w_conv_b,
        w_conv_c,
        w_conv_in,
        w_out,
        limit=63,
    )
    block = swapped(block, "sp_0")
    whole = lax.all_gather(packed, SP, axis=0, tiled=True)
    core = lax.axis_index("sp_2")
    row = lax.axis_index("sp_1")
    normed = row_norm(tokens, norm_gain)

    block, normed = lax.optimization_barrier((block, normed))
    up = down = block
    pieces = [block]
    for k in range(4):
        up = lax.ppermute(up, "sp_1", ring(8, 1))
        pieces.append(up)
        if k < 3:
            down = lax.ppermute(down, "sp_1", ring(8, -1))
            pieces.append(down)
    groups, at = [], 0
    for count in GROUPS:
        groups.append(jnp.stack(pieces[at : at + count]))
        at += count
    for count, group in zip(GROUPS, tuple(groups)):
        groups.append(lax.ppermute(group, "sp_2", ring(2, 1)))

    gates = lax.dot_general(
        w_gates.reshape(-1, 4), normed, (((0,), (1,)), ((), ())), preferred_element_type=F32
    ).reshape(2, 2, length)
    in_gate = gates[:, 0] + input_bias
    log_forget = jax.nn.log_sigmoid(gates[:, 1] + forget_bias) + decay_shift[:, :, 0]
    rows, columns, numbers = on_core(
        gate_kernel,
        (
            jax.ShapeDtypeStruct((4, length), F32),
            jax.ShapeDtypeStruct((length, 8), F32),
            jax.ShapeDtypeStruct((4, 128), F32),
        ),
        log_forget,
        in_gate,
    )
    block = jax.ShapeDtypeStruct((members, ROWS, 128), BF16)
    state, keys, values = on_core(
        state_kernel,
        (
            block,
            jax.ShapeDtypeStruct((length, DQK), BF16),
            jax.ShapeDtypeStruct((length, DV), BF16),
        ),
        jnp.stack([core, row]),
        normed,
        columns,
        numbers,
        *groups,
        scalars=1,
        scratch=[pltpu.VMEM((normed.shape[1], DQK + DV), BF16)],
    )
    last, initial, keys = lax.optimization_barrier((normed[-1:], normed[:1], keys))
    state = swapped(state, PLANE)
    before, after = neighbour_rows(last, initial)
    edges = jnp.concatenate([before, after, jnp.zeros((14, normed.shape[1]), BF16)], axis=0)
    near, plane_state = on_core(
        plane_kernel,
        (
            jax.ShapeDtypeStruct((members, ROWS, 128), F32),
            jax.ShapeDtypeStruct((planes, ROWS, 128), BF16),
        ),
        state,
    )
    far = swapped(plane_state, "sp_0")
    queries, conv_out = on_core(
        project_kernel,
        (
            jax.ShapeDtypeStruct((length, DQK), BF16),
            jax.ShapeDtypeStruct((length, DV), BF16),
        ),
        normed,
        edges,
        conv_taps,
        whole,
        remote=1,
        scratch=[
            pltpu.VMEM((CHUNKS, whole.shape[0] // CHUNKS, whole.shape[1]), BF16),
            pltpu.VMEM((length + edges.shape[0], WIDE), F32),
            pltpu.SemaphoreType.DMA((CHUNKS,)),
        ],
        limit=50,
    )
    start = on_core(far_kernel, block, plane[None], near, far, scalars=1)
    start = swapped(start, PLANE)
    joined = on_core(
        read_kernel,
        jax.ShapeDtypeStruct((4, length, 2 * DV), BF16),
        queries,
        keys,
        values,
        columns,
        rows,
        head_gain[None],
        conv_out,
        start,
    )
    joined = swapped(joined, "tp")
    sides = whole[:, WIDE:].reshape(size, 2, depth, half)
    return on_core(
        output_kernel,
        jax.ShapeDtypeStruct((length, 2 * half), BF16),
        joined,
        *(sides[:, side].reshape(4, 2 * DV, half) for side in range(2)),
    )


def solution(mesh):
    torus = Mesh(mesh.devices.reshape(8, 8, 2, mesh.shape["tp"]), (*SP, "tp"))
    placed = (
        P(SP, None),
        P(),
        P(SP, "tp"),
        P(SP, "tp"),
        P(SP, "tp"),
        P(None, None, None, "tp"),
        P(None, "tp"),
        P(None, "tp"),
        P(None, SP, "tp"),
        P("tp"),
        P(SP, "tp"),
        P(SP, "tp"),
        P(SP, "tp"),
        P(None, "tp"),
        P(SP, "tp"),
    )

    return jax.shard_map(body, mesh=torus, in_specs=placed, out_specs=P(SP, "tp"), check_vma=False)
```

```python
import jax
import jax.numpy as jnp
from jax import lax
from jax.experimental import pallas as pl
from jax.experimental.pallas import tpu as pltpu
from jax.sharding import Mesh
from jax.sharding import PartitionSpec as P


DQK = 128
DV = 256
SP = ("sp_0", "sp_1", "sp_2")
PLANE = ("sp_1", "sp_2")
EPS = 1e-06
LOWEST = -1e30
F32 = jnp.float32
BF16 = jnp.bfloat16


def row_norm(tokens, norm_gain):
    values = tokens.astype(F32)
    inverse_rms = lax.rsqrt(jnp.mean(values * values, axis=-1, keepdims=True) + EPS)
    return (values * inverse_rms * norm_gain).astype(BF16)


def swapped(value, axes):
    return lax.all_to_all(value, axes, split_axis=0, concat_axis=0, tiled=True)


def neighbour_rows(last, initial):
    size = lax.axis_size(SP)
    up = [(i, i + 1) for i in range(size - 1)]
    before = lax.ppermute(last, SP, up)
    after = lax.ppermute(initial, SP, [(j, i) for i, j in up])
    return before, after


ROWS = 48
NORMERS = 32
NUMBERS = (34, 40)


def in_terms(number):
    high = number.astype(BF16)
    rest = number - high.astype(F32)
    middle = rest.astype(BF16)
    low = (rest - middle.astype(F32)).astype(BF16)
    return [high, middle, low]


def from_terms(block, row):
    return block[row : row + 1] + block[row + 1 : row + 2] + block[row + 2 : row + 3]


def numbered_rows(normers, numbers):
    rows = [n.astype(BF16) for n in normers]
    for pair in numbers:
        for number in pair:
            rows += in_terms(number)
    rows.append(jnp.zeros((ROWS - NORMERS - len(rows), 128), BF16))
    return jnp.concatenate(rows, axis=0)


def pack_kernel(query_ref, key_ref, value_ref, outer_ref, inner_ref, given_ref, out_ref, whole_ref, block_ref):
    at = 0
    for ref in (query_ref, inner_ref, given_ref, outer_ref):
        whole_ref[:, at : at + ref.shape[1]] = ref[...]
        at += ref.shape[1]
    depth, columns = out_ref.shape
    for side in range(2):
        whole_ref[side * depth : (side + 1) * depth, at:] = out_ref[
            :, side * columns // 2 : (side + 1) * columns // 2
        ]
    for z in range(block_ref.shape[0]):
        block_ref[z, :, :DQK] = key_ref[...]
        block_ref[z, :, DQK:] = value_ref[...]


def gate_kernel(forget_ref, gate_ref, row_ref, column_ref, number_ref):
    length = forget_ref.shape[1]
    at = lax.broadcasted_iota(jnp.int32, (1, length), 1)
    running, update, numbers = [], [], []
    for d in range(2):
        value = forget_ref[d : d + 1]
        step = 1
        while step < length:
            moved = pltpu.roll(value, length - step if d else step, 1)
            inside = (at < length - step) if d else (at >= step)
            value = value + jnp.where(inside, moved, 0.0)
            step *= 2
        total = value[:, :1] if d else value[:, length - 1 :]
        log_update = total - value + gate_ref[d : d + 1]
        most = jnp.max(log_update, axis=1, keepdims=True)
        running.append(value)
        update.append(jnp.exp(log_update - most))
        numbers += [total, most]
    row_ref[...] = jnp.concatenate([*running, gate_ref[...]], axis=0)
    column_ref[...] = jnp.concatenate([*update, *running, *update, *running], axis=0).T
    for n, number in enumerate(numbers):
        number_ref[n : n + 1] = jnp.broadcast_to(number, (1, 128))


def state_kernel(place_ref, normed_ref, update_ref, number_ref, *refs):
    blocks = refs[:8]
    state_ref, key_ref, value_ref, weight_ref = refs[8:]
    way, row = place_ref[0], place_ref[1]
    for n, block_ref in enumerate(blocks):
        offset = (n if n < 4 else 3 - n) if n < 7 else 4
        y = (row + way * offset + 8) % 8
        planes, depth, _ = block_ref.shape
        for z in range(planes):
            start = (z * 8 + y) * depth
            weight_ref[pl.ds(pl.multiple_of(start, depth), depth), :] = block_ref[z]
    both = jnp.dot(normed_ref[...], weight_ref[...], preferred_element_type=F32)
    both = both.astype(BF16)
    keys, values = both[:, :DQK], both[:, DQK:]
    key_ref[...] = keys
    value_ref[...] = values
    members = state_ref.shape[0]
    share = DV // members
    normers = []
    for d in range(2):
        weighted = keys.astype(F32) * update_ref[:, d : d + 1]
        normers.append(jnp.sum(weighted, axis=0, keepdims=True))
        memory = lax.dot_general(
            values, weighted.astype(BF16), (((0,), (0,)), ((), ())), preferred_element_type=F32
        )
        state_ref[:, d * share : (d + 1) * share, :] = memory.astype(BF16).reshape(
            members, share, DQK
        )
    numbers = [[number_ref[2 * d + n : 2 * d + n + 1] for n in range(2)] for d in range(2)]
    rows = numbered_rows(normers, numbers)
    for j in range(members):
        state_ref[j, NORMERS:, :] = rows


def passed(carry, block, d):
    memory, normer, total, most = carry
    block_total = from_terms(block, NUMBERS[d])
    block_most = from_terms(block, NUMBERS[d] + 3)
    new = jnp.maximum(most + block_total, block_most)
    old_weight = jnp.exp(most + block_total - new)
    block_weight = jnp.exp(block_most - new)
    share = memory.shape[0]
    memory = old_weight * memory + block_weight * block[d * share : (d + 1) * share]
    normer = old_weight * normer + block_weight * block[NORMERS + d : NORMERS + d + 1]
    return memory, normer, total + block_total, new


def nothing(share):
    row = jnp.zeros((1, 128), F32)
    return jnp.zeros((share, 128), F32), row, row, jnp.full((1, 128), LOWEST, F32)


def plane_kernel(state_ref, near_ref, plane_ref):
    members = state_ref.shape[0]
    share = NORMERS // 2
    ends = []
    for d in range(2):
        carry = nothing(share)
        for i in reversed(range(members)) if d else range(members):
            near_ref[i, d * share : (d + 1) * share, :] = carry[0]
            for n in range(3):
                near_ref[i, NORMERS + 2 * n + d : NORMERS + 2 * n + d + 1, :] = carry[1 + n]
            carry = passed(carry, state_ref[i].astype(F32), d)
        ends.append(carry)
    rows = numbered_rows([e[1] for e in ends], [e[2:] for e in ends])
    for z in range(plane_ref.shape[0]):
        for d in range(2):
            plane_ref[z, d * share : (d + 1) * share, :] = ends[d][0].astype(BF16)
        plane_ref[z, NORMERS:, :] = rows


def far_kernel(place_ref, near_ref, planes_ref, start_ref):
    planes, members = planes_ref.shape[0], near_ref.shape[0]
    share = NORMERS // 2
    place = place_ref[0]
    far = []
    for d in range(2):
        carry = nothing(share)
        for z in reversed(range(planes)) if d else range(planes):
            earlier = (z > place) if d else (z < place)
            after = passed(carry, planes_ref[z].astype(F32), d)
            carry = tuple(jnp.where(earlier, a, c) for a, c in zip(after, carry))
        far.append(carry)
    for i in range(members):
        normers, numbers = [], []
        for d in range(2):
            memory, normer, _, most = far[d]
            at = [NORMERS + 2 * n + d for n in range(3)]
            near_normer, head, near_most = (near_ref[i, r : r + 1, :] for r in at)
            moved = most + head
            new = jnp.maximum(moved, near_most)
            far_weight = jnp.exp(moved - new)
            near_weight = jnp.exp(near_most - new)
            near = near_ref[i, d * share : (d + 1) * share, :]
            start_ref[i, d * share : (d + 1) * share, :] = (
                near_weight * near + far_weight * memory
            ).astype(BF16)
            normers.append(near_weight * near_normer + far_weight * normer)
            numbers.append([new])
        rows = [n.astype(BF16) for n in normers]
        for (number,) in numbers:
            rows += in_terms(number)
        rows.append(jnp.zeros((ROWS - NORMERS - len(rows), 128), BF16))
        start_ref[i, NORMERS:, :] = jnp.concatenate(rows, axis=0)


def read_kernel(query_ref, key_ref, value_ref, column_ref, row_ref, gain_ref, conv_ref, start_ref, out_ref):
    length = query_ref.shape[0]
    queries = query_ref[...]
    values = value_ref[...]
    scale = DQK ** (-0.5)
    products = scale * lax.dot_general(
        queries, key_ref[...], (((1,), (1,)), ((), ())), preferred_element_type=F32
    )
    t = lax.broadcasted_iota(jnp.int32, (length, length), 0)
    s = lax.broadcasted_iota(jnp.int32, (length, length), 1)
    share = NORMERS // 2
    last = start_ref[0, NORMERS:, :].astype(F32)
    summed = None
    for d in range(2):
        memory = start_ref[:, d * share : (d + 1) * share, :].reshape(DV, DQK)
        normer = last[d : d + 1]
        stable = from_terms(last, 2 + 3 * d)[:, :1]
        running = column_ref[:, 2 + d : 3 + d]
        seen = (t <= s) if d else (t >= s)
        log_weight = jnp.where(
            seen, running - row_ref[d : d + 1, :] + row_ref[2 + d : 3 + d, :], -jnp.inf
        )
        carried = running + stable
        highest = jnp.maximum(carried, jnp.max(log_weight, axis=-1, keepdims=True))
        scores = products * jnp.exp(log_weight - highest)
        carry_weight = scale * jnp.exp(carried - highest)
        numerator = jnp.dot(scores.astype(BF16), values, preferred_element_type=F32)
        numerator += carry_weight * lax.dot_general(
            queries, memory, (((1,), (1,)), ((), ())), preferred_element_type=F32
        )
        denominator = jnp.sum(scores, axis=-1, keepdims=True)
        denominator += carry_weight * jnp.sum(
            queries.astype(F32) * normer, axis=-1, keepdims=True
        )
        result = numerator / jnp.maximum(jnp.abs(denominator), jnp.exp(-highest))
        summed = result if summed is None else summed + result
    inverse_rms = lax.rsqrt(jnp.mean(summed * summed, axis=-1, keepdims=True) + EPS)
    out = (summed * inverse_rms * gain_ref[...]).astype(BF16)
    for k in range(out_ref.shape[0]):
        out_ref[k, :, :DV] = out
        out_ref[k, :, DV:] = conv_ref[...]


WIDE = DQK + 3 * DV
CHUNKS = 8
AHEAD = 4


def project_kernel(
    normed_ref, edge_ref, tap_ref, whole_ref, query_ref, conv_ref, weight_ref, total_ref, sems
):
    depth = weight_ref.shape[1]
    length = query_ref.shape[0]

    def fetch(k):
        return pltpu.make_async_copy(
            whole_ref.at[pl.ds(k * depth, depth)], weight_ref.at[k], sems.at[k]
        )

    for k in range(AHEAD):
        fetch(k).start()
    for k in range(CHUNKS):
        fetch(k).wait()
        if k + AHEAD < CHUNKS:
            fetch(k + AHEAD).start()
        at = slice(k * depth, (k + 1) * depth)
        rows = jnp.concatenate([normed_ref[:, at], edge_ref[:, at]], axis=0)
        product = jnp.dot(rows, weight_ref[k, :, :WIDE], preferred_element_type=F32)
        if k:
            total_ref[...] += product
        else:
            total_ref[...] = product
    query_ref[...] = total_ref[:length, :DQK].astype(BF16)
    inner = total_ref[:, DQK : DQK + DV].astype(BF16).astype(F32)
    given = total_ref[:, DQK + DV : DQK + 2 * DV].astype(BF16).astype(F32)
    outer = total_ref[:length, DQK + 2 * DV :].astype(BF16).astype(F32)
    mixed = (inner * given).astype(BF16).astype(F32)
    here = mixed[:length]
    at = lax.broadcasted_iota(jnp.int32, (length, DV), 0)
    before = jnp.where(at == 0, mixed[length : length + 1], pltpu.roll(here, 1, 0))
    after = jnp.where(
        at == length - 1, mixed[length + 1 : length + 2], pltpu.roll(here, length - 1, 0)
    )
    taps = tap_ref[...].astype(F32)
    filtered = taps[0:1] * before + taps[1:2] * here + taps[2:3] * after
    conv_ref[...] = (outer * filtered).astype(BF16)


def output_kernel(joined_ref, weight_ref, *refs):
    total = None
    for k in range(joined_ref.shape[0]):
        product = jnp.dot(joined_ref[k], weight_ref[k], preferred_element_type=F32)
        total = product if total is None else total + product
    if len(refs) == 1:
        refs[0][...] = total.astype(BF16)
    else:
        refs[1][:, : total.shape[1]] = refs[0][...]
        refs[1][:, total.shape[1] :] = total.astype(BF16)


def ring(size, step):
    return [(i, (i + step) % size) for i in range(size)]


def on_core(kernel, out, *operands, scalars=0, remote=0, scratch=(), limit=20):
    vmem = pl.BlockSpec(memory_space=pltpu.VMEM)
    smem = pl.BlockSpec(memory_space=pltpu.SMEM)
    hbm = pl.BlockSpec(memory_space=pltpu.HBM)
    return pl.pallas_call(
        kernel,
        out_shape=out,
        in_specs=[smem] * scalars
        + [vmem] * (len(operands) - scalars - remote)
        + [hbm] * remote,
        out_specs=jax.tree.map(lambda _: vmem, out),
        scratch_shapes=scratch,
        compiler_params=pltpu.CompilerParams(vmem_limit_bytes=limit * 2**20),
    )(*operands)


def body(
    tokens,
    norm_gain,
    w_query,
    w_key,
    w_value,
    w_gates,
    input_bias,
    forget_bias,
    decay_shift,
    head_gain,
    w_conv_b,
    w_conv_c,
    w_conv_in,
    conv_taps,
    w_out,
):
    length = tokens.shape[0]
    size = lax.axis_size(SP)
    planes = lax.axis_size("sp_0")
    members = size // planes
    plane = lax.axis_index("sp_0")
    depth = w_out.shape[0]
    half = w_out.shape[1] // 2
    packed, block = on_core(
        pack_kernel,
        (
            jax.ShapeDtypeStruct((w_key.shape[0], WIDE + half), BF16),
            jax.ShapeDtypeStruct((2 * planes, w_key.shape[0], DQK + DV), BF16),
        ),
        w_query,
        w_key,
        w_value,
        w_conv_b,
        w_conv_c,
        w_conv_in,
        w_out,
        limit=63,
    )
    block = swapped(block, ("sp_0", "sp_2")).reshape(planes, -1, DQK + DV)
    whole = lax.all_gather(packed, SP, axis=0, tiled=True)
    core = lax.axis_index("sp_2")
    row = lax.axis_index("sp_1")
    normed = row_norm(tokens, norm_gain)

    block, normed = lax.optimization_barrier((block, normed))
    apart = [(2 * y + c, (y + 1 - 2 * c) % 8 * 2 + c) for y in range(8) for c in range(2)]
    pieces, swaps = [block], []
    for k in range(4):
        pieces.append(lax.ppermute(pieces[-1], PLANE, apart))
        if k < 3:
            swaps.append(lax.ppermute(pieces[-1], "sp_2", ring(2, 1)))
    pieces = pieces[:4] + swaps + pieces[4:]

    gates = lax.dot_general(
        w_gates.reshape(-1, 4), normed, (((0,), (1,)), ((), ())), preferred_element_type=F32
    ).reshape(2, 2, length)
    in_gate = gates[:, 0] + input_bias
    log_forget = jax.nn.log_sigmoid(gates[:, 1] + forget_bias) + decay_shift[:, :, 0]
    rows, columns, numbers = on_core(
        gate_kernel,
        (
            jax.ShapeDtypeStruct((4, length), F32),
            jax.ShapeDtypeStruct((length, 8), F32),
            jax.ShapeDtypeStruct((4, 128), F32),
        ),
        log_forget,
        in_gate,
    )
    block = jax.ShapeDtypeStruct((members, ROWS, 128), BF16)
    state, keys, values = on_core(
        state_kernel,
        (
            block,
            jax.ShapeDtypeStruct((length, DQK), BF16),
            jax.ShapeDtypeStruct((length, DV), BF16),
        ),
        jnp.stack([2 * core - 1, row]),
        normed,
        columns,
        numbers,
        *pieces,
        scalars=1,
        scratch=[pltpu.VMEM((normed.shape[1], DQK + DV), BF16)],
    )
    last, initial, keys = lax.optimization_barrier((normed[-1:], normed[:1], keys))
    state = swapped(state, PLANE)
    before, after = neighbour_rows(last, initial)
    edges = jnp.concatenate([before, after, jnp.zeros((14, normed.shape[1]), BF16)], axis=0)
    near, plane_state = on_core(
        plane_kernel,
        (
            jax.ShapeDtypeStruct((members, ROWS, 128), F32),
            jax.ShapeDtypeStruct((planes, ROWS, 128), BF16),
        ),
        state,
    )
    far = swapped(plane_state, "sp_0")
    queries, conv_out = on_core(
        project_kernel,
        (
            jax.ShapeDtypeStruct((length, DQK), BF16),
            jax.ShapeDtypeStruct((length, DV), BF16),
        ),
        normed,
        edges,
        conv_taps,
        whole,
        remote=1,
        scratch=[
            pltpu.VMEM((CHUNKS, whole.shape[0] // CHUNKS, whole.shape[1]), BF16),
            pltpu.VMEM((length + edges.shape[0], WIDE), F32),
            pltpu.SemaphoreType.DMA((CHUNKS,)),
        ],
        limit=50,
    )
    start = on_core(far_kernel, block, plane[None], near, far, scalars=1)
    start = swapped(start, PLANE)
    joined = on_core(
        read_kernel,
        jax.ShapeDtypeStruct((4, length, 2 * DV), BF16),
        queries,
        keys,
        values,
        columns,
        rows,
        head_gain[None],
        conv_out,
        start,
    )
    joined = swapped(joined, "tp")
    sides = whole[:, WIDE:].reshape(size, 2, depth, half)
    left, right = (sides[:, side].reshape(4, 2 * DV, half) for side in range(2))
    first = on_core(output_kernel, jax.ShapeDtypeStruct((length, half), BF16), joined, left)
    return on_core(
        output_kernel,
        jax.ShapeDtypeStruct((length, 2 * half), BF16),
        joined,
        right,
        first,
    )


def solution(mesh):
    torus = Mesh(mesh.devices.reshape(8, 8, 2, mesh.shape["tp"]), (*SP, "tp"))
    placed = (
        P(SP, None),
        P(),
        P(SP, "tp"),
        P(SP, "tp"),
        P(SP, "tp"),
        P(None, None, None, "tp"),
        P(None, "tp"),
        P(None, "tp"),
        P(None, SP, "tp"),
        P("tp"),
        P(SP, "tp"),
        P(SP, "tp"),
        P(SP, "tp"),
        P(None, "tp"),
        P(SP, "tp"),
    )

    return jax.shard_map(body, mesh=torus, in_specs=placed, out_specs=P(SP, "tp"), check_vma=False)
```

```python
import jax
import jax.numpy as jnp
from jax import lax
from jax.experimental import pallas as pl
from jax.experimental.pallas import tpu as pltpu
from jax.sharding import Mesh
from jax.sharding import PartitionSpec as P


DQK = 128
DV = 256
SP = ("sp_0", "sp_1", "sp_2")
PLANE = ("sp_1", "sp_2")
EPS = 1e-06
LOWEST = -1e30
F32 = jnp.float32
BF16 = jnp.bfloat16


def row_norm(tokens, norm_gain):
    values = tokens.astype(F32)
    inverse_rms = lax.rsqrt(jnp.mean(values * values, axis=-1, keepdims=True) + EPS)
    return (values * inverse_rms * norm_gain).astype(BF16)


def swapped(value, axes):
    return lax.all_to_all(value, axes, split_axis=0, concat_axis=0, tiled=True)


def neighbour_rows(last, initial):
    size = lax.axis_size(SP)
    up = [(i, i + 1) for i in range(size - 1)]
    before = lax.ppermute(last, SP, up)
    after = lax.ppermute(initial, SP, [(j, i) for i, j in up])
    return before, after


ROWS = 48
NORMERS = 32
NUMBERS = (34, 40)


def in_terms(number):
    high = number.astype(BF16)
    rest = number - high.astype(F32)
    middle = rest.astype(BF16)
    low = (rest - middle.astype(F32)).astype(BF16)
    return [high, middle, low]


def from_terms(block, row):
    return block[row : row + 1] + block[row + 1 : row + 2] + block[row + 2 : row + 3]


def numbered_rows(normers, numbers):
    rows = [n.astype(BF16) for n in normers]
    for pair in numbers:
        for number in pair:
            rows += in_terms(number)
    rows.append(jnp.zeros((ROWS - NORMERS - len(rows), 128), BF16))
    return jnp.concatenate(rows, axis=0)


ARRIVAL = (0, -1, 1, -2, 2, -3, 3, -4)
GROUPS = (7, 1)


def pack_kernel(query_ref, key_ref, value_ref, outer_ref, inner_ref, given_ref, out_ref, whole_ref, block_ref):
    at = 0
    for ref in (query_ref, inner_ref, given_ref, outer_ref):
        whole_ref[:, at : at + ref.shape[1]] = ref[...]
        at += ref.shape[1]
    depth, columns = out_ref.shape
    for side in range(2):
        whole_ref[side * depth : (side + 1) * depth, at:] = out_ref[
            :, side * columns // 2 : (side + 1) * columns // 2
        ]
    for z in range(block_ref.shape[0]):
        block_ref[z, :, :DQK] = key_ref[...]
        block_ref[z, :, DQK:] = value_ref[...]


def gate_kernel(forget_ref, gate_ref, row_ref, column_ref, number_ref):
    length = forget_ref.shape[1]
    at = lax.broadcasted_iota(jnp.int32, (1, length), 1)
    running, update, numbers = [], [], []
    for d in range(2):
        value = forget_ref[d : d + 1]
        step = 1
        while step < length:
            moved = pltpu.roll(value, length - step if d else step, 1)
            inside = (at < length - step) if d else (at >= step)
            value = value + jnp.where(inside, moved, 0.0)
            step *= 2
        total = value[:, :1] if d else value[:, length - 1 :]
        log_update = total - value + gate_ref[d : d + 1]
        most = jnp.max(log_update, axis=1, keepdims=True)
        running.append(value)
        update.append(jnp.exp(log_update - most))
        numbers += [total, most]
    row_ref[...] = jnp.concatenate([*running, gate_ref[...]], axis=0)
    column_ref[...] = jnp.concatenate([*update, *running, *update, *running], axis=0).T
    for n, number in enumerate(numbers):
        number_ref[n : n + 1] = jnp.broadcast_to(number, (1, 128))


def state_kernel(place_ref, normed_ref, update_ref, number_ref, *refs):
    groups = len(GROUPS)
    state_ref, key_ref, value_ref, weight_ref = refs[2 * groups :]
    core, row = place_ref[0], place_ref[1]
    for side in range(2):
        cell = 1 - core if side else core
        arrivals = iter(ARRIVAL)
        for group_ref in refs[side * groups : (side + 1) * groups]:
            _, planes, depth, _ = group_ref.shape
            for k in range(group_ref.shape[0]):
                y = (row + next(arrivals) + 8) % 8
                for z in range(planes):
                    start = ((z * 8 + y) * 2 + cell) * depth
                    weight_ref[pl.ds(pl.multiple_of(start, depth), depth), :] = group_ref[k, z]
    both = jnp.dot(normed_ref[...], weight_ref[...], preferred_element_type=F32)
    both = both.astype(BF16)
    keys, values = both[:, :DQK], both[:, DQK:]
    key_ref[...] = keys
    value_ref[...] = values
    members = state_ref.shape[0]
    share = DV // members
    normers = []
    for d in range(2):
        weighted = keys.astype(F32) * update_ref[:, d : d + 1]
        normers.append(jnp.sum(weighted, axis=0, keepdims=True))
        memory = lax.dot_general(
            values, weighted.astype(BF16), (((0,), (0,)), ((), ())), preferred_element_type=F32
        )
        state_ref[:, d * share : (d + 1) * share, :] = memory.astype(BF16).reshape(
            members, share, DQK
        )
    numbers = [[number_ref[2 * d + n : 2 * d + n + 1] for n in range(2)] for d in range(2)]
    rows = numbered_rows(normers, numbers)
    for j in range(members):
        state_ref[j, NORMERS:, :] = rows


def passed(carry, block, d):
    memory, normer, total, most = carry
    block_total = from_terms(block, NUMBERS[d])
    block_most = from_terms(block, NUMBERS[d] + 3)
    new = jnp.maximum(most + block_total, block_most)
    old_weight = jnp.exp(most + block_total - new)
    block_weight = jnp.exp(block_most - new)
    share = memory.shape[0]
    memory = old_weight * memory + block_weight * block[d * share : (d + 1) * share]
    normer = old_weight * normer + block_weight * block[NORMERS + d : NORMERS + d + 1]
    return memory, normer, total + block_total, new


def nothing(share):
    row = jnp.zeros((1, 128), F32)
    return jnp.zeros((share, 128), F32), row, row, jnp.full((1, 128), LOWEST, F32)


def plane_kernel(state_ref, near_ref, plane_ref):
    members = state_ref.shape[0]
    share = NORMERS // 2
    ends = []
    for d in range(2):
        carry = nothing(share)
        for i in reversed(range(members)) if d else range(members):
            near_ref[i, d * share : (d + 1) * share, :] = carry[0]
            for n in range(3):
                near_ref[i, NORMERS + 2 * n + d : NORMERS + 2 * n + d + 1, :] = carry[1 + n]
            carry = passed(carry, state_ref[i].astype(F32), d)
        ends.append(carry)
    rows = numbered_rows([e[1] for e in ends], [e[2:] for e in ends])
    for z in range(plane_ref.shape[0]):
        for d in range(2):
            plane_ref[z, d * share : (d + 1) * share, :] = ends[d][0].astype(BF16)
        plane_ref[z, NORMERS:, :] = rows


def far_kernel(place_ref, near_ref, planes_ref, start_ref):
    planes, members = planes_ref.shape[0], near_ref.shape[0]
    share = NORMERS // 2
    place = place_ref[0]
    far = []
    for d in range(2):
        carry = nothing(share)
        for z in reversed(range(planes)) if d else range(planes):
            earlier = (z > place) if d else (z < place)
            after = passed(carry, planes_ref[z].astype(F32), d)
            carry = tuple(jnp.where(earlier, a, c) for a, c in zip(after, carry))
        far.append(carry)
    for i in range(members):
        normers, numbers = [], []
        for d in range(2):
            memory, normer, _, most = far[d]
            at = [NORMERS + 2 * n + d for n in range(3)]
            near_normer, head, near_most = (near_ref[i, r : r + 1, :] for r in at)
            moved = most + head
            new = jnp.maximum(moved, near_most)
            far_weight = jnp.exp(moved - new)
            near_weight = jnp.exp(near_most - new)
            near = near_ref[i, d * share : (d + 1) * share, :]
            start_ref[i, d * share : (d + 1) * share, :] = (
                near_weight * near + far_weight * memory
            ).astype(BF16)
            normers.append(near_weight * near_normer + far_weight * normer)
            numbers.append([new])
        rows = [n.astype(BF16) for n in normers]
        for (number,) in numbers:
            rows += in_terms(number)
        rows.append(jnp.zeros((ROWS - NORMERS - len(rows), 128), BF16))
        start_ref[i, NORMERS:, :] = jnp.concatenate(rows, axis=0)


def read_kernel(query_ref, key_ref, value_ref, column_ref, row_ref, gain_ref, conv_ref, start_ref, out_ref):
    length = query_ref.shape[0]
    queries = query_ref[...]
    values = value_ref[...]
    scale = DQK ** (-0.5)
    products = scale * lax.dot_general(
        queries, key_ref[...], (((1,), (1,)), ((), ())), preferred_element_type=F32
    )
    t = lax.broadcasted_iota(jnp.int32, (length, length), 0)
    s = lax.broadcasted_iota(jnp.int32, (length, length), 1)
    share = NORMERS // 2
    last = start_ref[0, NORMERS:, :].astype(F32)
    summed = None
    for d in range(2):
        memory = start_ref[:, d * share : (d + 1) * share, :].reshape(DV, DQK)
        normer = last[d : d + 1]
        stable = from_terms(last, 2 + 3 * d)[:, :1]
        running = column_ref[:, 2 + d : 3 + d]
        seen = (t <= s) if d else (t >= s)
        log_weight = jnp.where(
            seen, running - row_ref[d : d + 1, :] + row_ref[2 + d : 3 + d, :], -jnp.inf
        )
        carried = running + stable
        highest = jnp.maximum(carried, jnp.max(log_weight, axis=-1, keepdims=True))
        scores = products * jnp.exp(log_weight - highest)
        carry_weight = scale * jnp.exp(carried - highest)
        numerator = jnp.dot(scores.astype(BF16), values, preferred_element_type=F32)
        numerator += carry_weight * lax.dot_general(
            queries, memory, (((1,), (1,)), ((), ())), preferred_element_type=F32
        )
        denominator = jnp.sum(scores, axis=-1, keepdims=True)
        denominator += carry_weight * jnp.sum(
            queries.astype(F32) * normer, axis=-1, keepdims=True
        )
        result = numerator / jnp.maximum(jnp.abs(denominator), jnp.exp(-highest))
        summed = result if summed is None else summed + result
    inverse_rms = lax.rsqrt(jnp.mean(summed * summed, axis=-1, keepdims=True) + EPS)
    out = (summed * inverse_rms * gain_ref[...]).astype(BF16)
    for k in range(out_ref.shape[0]):
        out_ref[k, :, :DV] = out
        out_ref[k, :, DV:] = conv_ref[...]


WIDE = DQK + 3 * DV
CHUNKS = 8
AHEAD = 4


def project_kernel(
    normed_ref, edge_ref, tap_ref, whole_ref, query_ref, conv_ref, weight_ref, total_ref, sems
):
    depth = weight_ref.shape[1]
    length = query_ref.shape[0]

    def fetch(k):
        return pltpu.make_async_copy(
            whole_ref.at[pl.ds(k * depth, depth)], weight_ref.at[k], sems.at[k]
        )

    for k in range(AHEAD):
        fetch(k).start()
    for k in range(CHUNKS):
        fetch(k).wait()
        if k + AHEAD < CHUNKS:
            fetch(k + AHEAD).start()
        at = slice(k * depth, (k + 1) * depth)
        rows = jnp.concatenate([normed_ref[:, at], edge_ref[:, at]], axis=0)
        product = jnp.dot(rows, weight_ref[k, :, :WIDE], preferred_element_type=F32)
        if k:
            total_ref[...] += product
        else:
            total_ref[...] = product
    query_ref[...] = total_ref[:length, :DQK].astype(BF16)
    inner = total_ref[:, DQK : DQK + DV].astype(BF16).astype(F32)
    given = total_ref[:, DQK + DV : DQK + 2 * DV].astype(BF16).astype(F32)
    outer = total_ref[:length, DQK + 2 * DV :].astype(BF16).astype(F32)
    mixed = (inner * given).astype(BF16).astype(F32)
    here = mixed[:length]
    at = lax.broadcasted_iota(jnp.int32, (length, DV), 0)
    before = jnp.where(at == 0, mixed[length : length + 1], pltpu.roll(here, 1, 0))
    after = jnp.where(
        at == length - 1, mixed[length + 1 : length + 2], pltpu.roll(here, length - 1, 0)
    )
    taps = tap_ref[...].astype(F32)
    filtered = taps[0:1] * before + taps[1:2] * here + taps[2:3] * after
    conv_ref[...] = (outer * filtered).astype(BF16)


def output_kernel(joined_ref, left_ref, right_ref, out_ref):
    for side, weight_ref in enumerate((left_ref, right_ref)):
        total = None
        for k in range(joined_ref.shape[0]):
            product = jnp.dot(joined_ref[k], weight_ref[k], preferred_element_type=F32)
            total = product if total is None else total + product
        out_ref[:, side * 512 : (side + 1) * 512] = total.astype(BF16)


def ring(size, step):
    return [(i, (i + step) % size) for i in range(size)]


def on_core(kernel, out, *operands, scalars=0, remote=0, scratch=(), limit=20):
    vmem = pl.BlockSpec(memory_space=pltpu.VMEM)
    smem = pl.BlockSpec(memory_space=pltpu.SMEM)
    hbm = pl.BlockSpec(memory_space=pltpu.HBM)
    return pl.pallas_call(
        kernel,
        out_shape=out,
        in_specs=[smem] * scalars
        + [vmem] * (len(operands) - scalars - remote)
        + [hbm] * remote,
        out_specs=jax.tree.map(lambda _: vmem, out),
        scratch_shapes=scratch,
        compiler_params=pltpu.CompilerParams(vmem_limit_bytes=limit * 2**20),
    )(*operands)


def body(
    tokens,
    norm_gain,
    w_query,
    w_key,
    w_value,
    w_gates,
    input_bias,
    forget_bias,
    decay_shift,
    head_gain,
    w_conv_b,
    w_conv_c,
    w_conv_in,
    conv_taps,
    w_out,
):
    length = tokens.shape[0]
    size = lax.axis_size(SP)
    planes = lax.axis_size("sp_0")
    members = size // planes
    plane = lax.axis_index("sp_0")
    depth = w_out.shape[0]
    half = w_out.shape[1] // 2
    packed, block = on_core(
        pack_kernel,
        (
            jax.ShapeDtypeStruct((w_key.shape[0], WIDE + half), BF16),
            jax.ShapeDtypeStruct((planes, w_key.shape[0], DQK + DV), BF16),
        ),
        w_query,
        w_key,
        w_value,
        w_conv_b,
        w_conv_c,
        w_conv_in,
        w_out,
        limit=63,
    )
    block = swapped(block, "sp_0")
    whole = lax.all_gather(packed, SP, axis=0, tiled=True)
    core = lax.axis_index("sp_2")
    row = lax.axis_index("sp_1")
    normed = row_norm(tokens, norm_gain)

    gates = lax.dot_general(
        w_gates.reshape(-1, 4), normed, (((0,), (1,)), ((), ())), preferred_element_type=F32
    ).reshape(2, 2, length)
    in_gate = gates[:, 0] + input_bias
    log_forget = jax.nn.log_sigmoid(gates[:, 1] + forget_bias) + decay_shift[:, :, 0]
    rows, columns, numbers = on_core(
        gate_kernel,
        (
            jax.ShapeDtypeStruct((4, length), F32),
            jax.ShapeDtypeStruct((length, 8), F32),
            jax.ShapeDtypeStruct((4, 128), F32),
        ),
        log_forget,
        in_gate,
    )
    block, normed, rows, columns, numbers = lax.optimization_barrier(
        (block, normed, rows, columns, numbers)
    )
    up = down = block
    pieces = [block]
    for k in range(4):
        up = lax.ppermute(up, "sp_1", ring(8, 1))
        pieces.append(up)
        if k < 3:
            down = lax.ppermute(down, "sp_1", ring(8, -1))
            pieces.append(down)
    groups, at = [], 0
    for count in GROUPS:
        groups.append(jnp.stack(pieces[at : at + count]))
        at += count
    for count, group in zip(GROUPS, tuple(groups)):
        groups.append(lax.ppermute(group, "sp_2", ring(2, 1)))

    block = jax.ShapeDtypeStruct((members, ROWS, 128), BF16)
    state, keys, values = on_core(
        state_kernel,
        (
            block,
            jax.ShapeDtypeStruct((length, DQK), BF16),
            jax.ShapeDtypeStruct((length, DV), BF16),
        ),
        jnp.stack([core, row]),
        normed,
        columns,
        numbers,
        *groups,
        scalars=1,
        scratch=[pltpu.VMEM((normed.shape[1], DQK + DV), BF16)],
    )
    last, initial, keys = lax.optimization_barrier((normed[-1:], normed[:1], keys))
    state = swapped(state, PLANE)
    before, after = neighbour_rows(last, initial)
    edges = jnp.concatenate([before, after, jnp.zeros((14, normed.shape[1]), BF16)], axis=0)
    near, plane_state = on_core(
        plane_kernel,
        (
            jax.ShapeDtypeStruct((members, ROWS, 128), F32),
            jax.ShapeDtypeStruct((planes, ROWS, 128), BF16),
        ),
        state,
    )
    far = swapped(plane_state, "sp_0")
    queries, conv_out = on_core(
        project_kernel,
        (
            jax.ShapeDtypeStruct((length, DQK), BF16),
            jax.ShapeDtypeStruct((length, DV), BF16),
        ),
        normed,
        edges,
        conv_taps,
        whole,
        remote=1,
        scratch=[
            pltpu.VMEM((CHUNKS, whole.shape[0] // CHUNKS, whole.shape[1]), BF16),
            pltpu.VMEM((length + edges.shape[0], WIDE), F32),
            pltpu.SemaphoreType.DMA((CHUNKS,)),
        ],
        limit=50,
    )
    start = on_core(far_kernel, block, plane[None], near, far, scalars=1)
    start = swapped(start, PLANE)
    joined = on_core(
        read_kernel,
        jax.ShapeDtypeStruct((4, length, 2 * DV), BF16),
        queries,
        keys,
        values,
        columns,
        rows,
        head_gain[None],
        conv_out,
        start,
    )
    joined = swapped(joined, "tp")
    sides = whole[:, WIDE:].reshape(size, 2, depth, half)
    return on_core(
        output_kernel,
        jax.ShapeDtypeStruct((length, 2 * half), BF16),
        joined,
        *(sides[:, side].reshape(4, 2 * DV, half) for side in range(2)),
    )


def solution(mesh):
    torus = Mesh(mesh.devices.reshape(8, 8, 2, mesh.shape["tp"]), (*SP, "tp"))
    placed = (
        P(SP, None),
        P(),
        P(SP, "tp"),
        P(SP, "tp"),
        P(SP, "tp"),
        P(None, None, None, "tp"),
        P(None, "tp"),
        P(None, "tp"),
        P(None, SP, "tp"),
        P("tp"),
        P(SP, "tp"),
        P(SP, "tp"),
        P(SP, "tp"),
        P(None, "tp"),
        P(SP, "tp"),
    )

    return jax.shard_map(body, mesh=torus, in_specs=placed, out_specs=P(SP, "tp"), check_vma=False)
```

```python
import jax
import jax.numpy as jnp
from jax import lax
from jax.experimental import pallas as pl
from jax.experimental.pallas import tpu as pltpu
from jax.sharding import Mesh
from jax.sharding import PartitionSpec as P


DQK = 128
DV = 256
SP = ("sp_0", "sp_1", "sp_2")
PLANE = ("sp_1", "sp_2")
EPS = 1e-06
LOWEST = -1e30
F32 = jnp.float32
BF16 = jnp.bfloat16


def row_norm(tokens, norm_gain):
    values = tokens.astype(F32)
    inverse_rms = lax.rsqrt(jnp.mean(values * values, axis=-1, keepdims=True) + EPS)
    return (values * inverse_rms * norm_gain).astype(BF16)


def swapped(value, axes):
    return lax.all_to_all(value, axes, split_axis=0, concat_axis=0, tiled=True)


def neighbour_rows(last, initial):
    size = lax.axis_size(SP)
    up = [(i, i + 1) for i in range(size - 1)]
    before = lax.ppermute(last, SP, up)
    after = lax.ppermute(initial, SP, [(j, i) for i, j in up])
    return before, after


ROWS = 48
NORMERS = 32
NUMBERS = (34, 40)


def in_terms(number):
    high = number.astype(BF16)
    rest = number - high.astype(F32)
    middle = rest.astype(BF16)
    low = (rest - middle.astype(F32)).astype(BF16)
    return [high, middle, low]


def from_terms(block, row):
    return block[row : row + 1] + block[row + 1 : row + 2] + block[row + 2 : row + 3]


def numbered_rows(normers, numbers):
    rows = [n.astype(BF16) for n in normers]
    for pair in numbers:
        for number in pair:
            rows += in_terms(number)
    rows.append(jnp.zeros((ROWS - NORMERS - len(rows), 128), BF16))
    return jnp.concatenate(rows, axis=0)


ARRIVAL = (0, -1, 1, -2, 2, -3, 3, -4)
GROUPS = (3, 4, 1)


def pack_kernel(query_ref, key_ref, value_ref, outer_ref, inner_ref, given_ref, out_ref, whole_ref, block_ref):
    at = 0
    for ref in (query_ref, inner_ref, given_ref, outer_ref):
        whole_ref[:, at : at + ref.shape[1]] = ref[...]
        at += ref.shape[1]
    depth, columns = out_ref.shape
    for side in range(2):
        whole_ref[side * depth : (side + 1) * depth, at:] = out_ref[
            :, side * columns // 2 : (side + 1) * columns // 2
        ]
    for z in range(block_ref.shape[0]):
        block_ref[z, :, :DQK] = key_ref[...]
        block_ref[z, :, DQK:] = value_ref[...]


def gate_kernel(forget_ref, gate_ref, row_ref, column_ref, number_ref):
    length = forget_ref.shape[1]
    at = lax.broadcasted_iota(jnp.int32, (1, length), 1)
    running, update, numbers = [], [], []
    for d in range(2):
        value = forget_ref[d : d + 1]
        step = 1
        while step < length:
            moved = pltpu.roll(value, length - step if d else step, 1)
            inside = (at < length - step) if d else (at >= step)
            value = value + jnp.where(inside, moved, 0.0)
            step *= 2
        total = value[:, :1] if d else value[:, length - 1 :]
        log_update = total - value + gate_ref[d : d + 1]
        most = jnp.max(log_update, axis=1, keepdims=True)
        running.append(value)
        update.append(jnp.exp(log_update - most))
        numbers += [total, most]
    row_ref[...] = jnp.concatenate([*running, gate_ref[...]], axis=0)
    column_ref[...] = jnp.concatenate([*update, *running, *update, *running], axis=0).T
    for n, number in enumerate(numbers):
        number_ref[n : n + 1] = jnp.broadcast_to(number, (1, 128))


def state_kernel(place_ref, normed_ref, update_ref, number_ref, *refs):
    groups = len(GROUPS)
    state_ref, key_ref, value_ref, weight_ref = refs[2 * groups :]
    core, row = place_ref[0], place_ref[1]
    for side in range(2):
        cell = 1 - core if side else core
        arrivals = iter(ARRIVAL)
        for group_ref in refs[side * groups : (side + 1) * groups]:
            _, planes, depth, _ = group_ref.shape
            for k in range(group_ref.shape[0]):
                y = (row + next(arrivals) + 8) % 8
                for z in range(planes):
                    start = ((z * 8 + y) * 2 + cell) * depth
                    weight_ref[pl.ds(pl.multiple_of(start, depth), depth), :] = group_ref[k, z]
    both = jnp.dot(normed_ref[...], weight_ref[...], preferred_element_type=F32)
    both = both.astype(BF16)
    keys, values = both[:, :DQK], both[:, DQK:]
    key_ref[...] = keys
    value_ref[...] = values
    members = state_ref.shape[0]
    share = DV // members
    normers = []
    for d in range(2):
        weighted = keys.astype(F32) * update_ref[:, d : d + 1]
        normers.append(jnp.sum(weighted, axis=0, keepdims=True))
        memory = lax.dot_general(
            values, weighted.astype(BF16), (((0,), (0,)), ((), ())), preferred_element_type=F32
        )
        state_ref[:, d * share : (d + 1) * share, :] = memory.astype(BF16).reshape(
            members, share, DQK
        )
    numbers = [[number_ref[2 * d + n : 2 * d + n + 1] for n in range(2)] for d in range(2)]
    rows = numbered_rows(normers, numbers)
    for j in range(members):
        state_ref[j, NORMERS:, :] = rows


def passed(carry, block, d):
    memory, normer, total, most = carry
    block_total = from_terms(block, NUMBERS[d])
    block_most = from_terms(block, NUMBERS[d] + 3)
    new = jnp.maximum(most + block_total, block_most)
    old_weight = jnp.exp(most + block_total - new)
    block_weight = jnp.exp(block_most - new)
    share = memory.shape[0]
    memory = old_weight * memory + block_weight * block[d * share : (d + 1) * share]
    normer = old_weight * normer + block_weight * block[NORMERS + d : NORMERS + d + 1]
    return memory, normer, total + block_total, new


def nothing(share):
    row = jnp.zeros((1, 128), F32)
    return jnp.zeros((share, 128), F32), row, row, jnp.full((1, 128), LOWEST, F32)


def plane_kernel(state_ref, near_ref, plane_ref):
    members = state_ref.shape[0]
    share = NORMERS // 2
    ends = []
    for d in range(2):
        carry = nothing(share)
        for i in reversed(range(members)) if d else range(members):
            near_ref[i, d * share : (d + 1) * share, :] = carry[0]
            for n in range(3):
                near_ref[i, NORMERS + 2 * n + d : NORMERS + 2 * n + d + 1, :] = carry[1 + n]
            carry = passed(carry, state_ref[i].astype(F32), d)
        ends.append(carry)
    rows = numbered_rows([e[1] for e in ends], [e[2:] for e in ends])
    for z in range(plane_ref.shape[0]):
        for d in range(2):
            plane_ref[z, d * share : (d + 1) * share, :] = ends[d][0].astype(BF16)
        plane_ref[z, NORMERS:, :] = rows


def far_kernel(place_ref, near_ref, planes_ref, start_ref):
    planes, members = planes_ref.shape[0], near_ref.shape[0]
    share = NORMERS // 2
    place = place_ref[0]
    far = []
    for d in range(2):
        carry = nothing(share)
        for z in reversed(range(planes)) if d else range(planes):
            earlier = (z > place) if d else (z < place)
            after = passed(carry, planes_ref[z].astype(F32), d)
            carry = tuple(jnp.where(earlier, a, c) for a, c in zip(after, carry))
        far.append(carry)
    for i in range(members):
        normers, numbers = [], []
        for d in range(2):
            memory, normer, _, most = far[d]
            at = [NORMERS + 2 * n + d for n in range(3)]
            near_normer, head, near_most = (near_ref[i, r : r + 1, :] for r in at)
            moved = most + head
            new = jnp.maximum(moved, near_most)
            far_weight = jnp.exp(moved - new)
            near_weight = jnp.exp(near_most - new)
            near = near_ref[i, d * share : (d + 1) * share, :]
            start_ref[i, d * share : (d + 1) * share, :] = (
                near_weight * near + far_weight * memory
            ).astype(BF16)
            normers.append(near_weight * near_normer + far_weight * normer)
            numbers.append([new])
        rows = [n.astype(BF16) for n in normers]
        for (number,) in numbers:
            rows += in_terms(number)
        rows.append(jnp.zeros((ROWS - NORMERS - len(rows), 128), BF16))
        start_ref[i, NORMERS:, :] = jnp.concatenate(rows, axis=0)


def local_kernel(query_ref, key_ref, value_ref, column_ref, row_ref, local_ref, sum_ref):
    length = query_ref.shape[0]
    values = value_ref[...]
    products = DQK ** (-0.5) * lax.dot_general(
        query_ref[...], key_ref[...], (((1,), (1,)), ((), ())), preferred_element_type=F32
    )
    t = lax.broadcasted_iota(jnp.int32, (length, length), 0)
    s = lax.broadcasted_iota(jnp.int32, (length, length), 1)
    for d in range(2):
        running = column_ref[:, 2 + d : 3 + d]
        seen = (t <= s) if d else (t >= s)
        log_weight = jnp.where(
            seen, running - row_ref[d : d + 1, :] + row_ref[2 + d : 3 + d, :], -jnp.inf
        )
        most = jnp.max(log_weight, axis=-1, keepdims=True)
        scores = products * jnp.exp(log_weight - most)
        local_ref[d] = jnp.dot(scores.astype(BF16), values, preferred_element_type=F32)
        sum_ref[:, d : d + 1] = jnp.sum(scores, axis=-1, keepdims=True)
        sum_ref[:, 2 + d : 3 + d] = most


def read_kernel(query_ref, local_ref, sum_ref, column_ref, gain_ref, conv_ref, start_ref, out_ref):
    queries = query_ref[...]
    scale = DQK ** (-0.5)
    share = NORMERS // 2
    last = start_ref[0, NORMERS:, :].astype(F32)
    summed = None
    for d in range(2):
        memory = start_ref[:, d * share : (d + 1) * share, :].reshape(DV, DQK)
        normer = last[d : d + 1]
        stable = from_terms(last, 2 + 3 * d)[:, :1]
        carried = column_ref[:, 2 + d : 3 + d] + stable
        most = sum_ref[:, 2 + d : 3 + d]
        highest = jnp.maximum(carried, most)
        local_weight = jnp.exp(most - highest)
        carry_weight = scale * jnp.exp(carried - highest)
        numerator = local_weight * local_ref[d] + carry_weight * lax.dot_general(
            queries, memory, (((1,), (1,)), ((), ())), preferred_element_type=F32
        )
        denominator = local_weight * sum_ref[:, d : d + 1] + carry_weight * jnp.sum(
            queries.astype(F32) * normer, axis=-1, keepdims=True
        )
        result = numerator / jnp.maximum(jnp.abs(denominator), jnp.exp(-highest))
        summed = result if summed is None else summed + result
    inverse_rms = lax.rsqrt(jnp.mean(summed * summed, axis=-1, keepdims=True) + EPS)
    out = (summed * inverse_rms * gain_ref[...]).astype(BF16)
    for k in range(out_ref.shape[0]):
        out_ref[k, :, :DV] = out
        out_ref[k, :, DV:] = conv_ref[...]


WIDE = DQK + 3 * DV
CHUNKS = 8
AHEAD = 4


def project_kernel(
    normed_ref, edge_ref, tap_ref, whole_ref, query_ref, conv_ref, weight_ref, total_ref, sems
):
    depth = weight_ref.shape[1]
    length = query_ref.shape[0]

    def fetch(k):
        return pltpu.make_async_copy(
            whole_ref.at[pl.ds(k * depth, depth)], weight_ref.at[k], sems.at[k]
        )

    for k in range(AHEAD):
        fetch(k).start()
    for k in range(CHUNKS):
        fetch(k).wait()
        if k + AHEAD < CHUNKS:
            fetch(k + AHEAD).start()
        at = slice(k * depth, (k + 1) * depth)
        rows = jnp.concatenate([normed_ref[:, at], edge_ref[:, at]], axis=0)
        product = jnp.dot(rows, weight_ref[k, :, :WIDE], preferred_element_type=F32)
        if k:
            total_ref[...] += product
        else:
            total_ref[...] = product
    query_ref[...] = total_ref[:length, :DQK].astype(BF16)
    inner = total_ref[:, DQK : DQK + DV].astype(BF16).astype(F32)
    given = total_ref[:, DQK + DV : DQK + 2 * DV].astype(BF16).astype(F32)
    outer = total_ref[:length, DQK + 2 * DV :].astype(BF16).astype(F32)
    mixed = (inner * given).astype(BF16).astype(F32)
    here = mixed[:length]
    at = lax.broadcasted_iota(jnp.int32, (length, DV), 0)
    before = jnp.where(at == 0, mixed[length : length + 1], pltpu.roll(here, 1, 0))
    after = jnp.where(
        at == length - 1, mixed[length + 1 : length + 2], pltpu.roll(here, length - 1, 0)
    )
    taps = tap_ref[...].astype(F32)
    filtered = taps[0:1] * before + taps[1:2] * here + taps[2:3] * after
    conv_ref[...] = (outer * filtered).astype(BF16)


def output_kernel(joined_ref, left_ref, right_ref, out_ref):
    for side, weight_ref in enumerate((left_ref, right_ref)):
        total = None
        for k in range(joined_ref.shape[0]):
            product = jnp.dot(joined_ref[k], weight_ref[k], preferred_element_type=F32)
            total = product if total is None else total + product
        out_ref[:, side * 512 : (side + 1) * 512] = total.astype(BF16)


def ring(size, step):
    return [(i, (i + step) % size) for i in range(size)]


def on_core(kernel, out, *operands, scalars=0, remote=0, scratch=(), limit=20):
    vmem = pl.BlockSpec(memory_space=pltpu.VMEM)
    smem = pl.BlockSpec(memory_space=pltpu.SMEM)
    hbm = pl.BlockSpec(memory_space=pltpu.HBM)
    return pl.pallas_call(
        kernel,
        out_shape=out,
        in_specs=[smem] * scalars
        + [vmem] * (len(operands) - scalars - remote)
        + [hbm] * remote,
        out_specs=jax.tree.map(lambda _: vmem, out),
        scratch_shapes=scratch,
        compiler_params=pltpu.CompilerParams(vmem_limit_bytes=limit * 2**20),
    )(*operands)


def body(
    tokens,
    norm_gain,
    w_query,
    w_key,
    w_value,
    w_gates,
    input_bias,
    forget_bias,
    decay_shift,
    head_gain,
    w_conv_b,
    w_conv_c,
    w_conv_in,
    conv_taps,
    w_out,
):
    length = tokens.shape[0]
    size = lax.axis_size(SP)
    planes = lax.axis_size("sp_0")
    members = size // planes
    plane = lax.axis_index("sp_0")
    depth = w_out.shape[0]
    half = w_out.shape[1] // 2
    packed, block = on_core(
        pack_kernel,
        (
            jax.ShapeDtypeStruct((w_key.shape[0], WIDE + half), BF16),
            jax.ShapeDtypeStruct((planes, w_key.shape[0], DQK + DV), BF16),
        ),
        w_query,
        w_key,
        w_value,
        w_conv_b,
        w_conv_c,
        w_conv_in,
        w_out,
        limit=63,
    )
    block = swapped(block, "sp_0")
    whole = lax.all_gather(packed, SP, axis=0, tiled=True)
    core = lax.axis_index("sp_2")
    row = lax.axis_index("sp_1")
    normed = row_norm(tokens, norm_gain)

    gates = lax.dot_general(
        w_gates.reshape(-1, 4), normed, (((0,), (1,)), ((), ())), preferred_element_type=F32
    ).reshape(2, 2, length)
    in_gate = gates[:, 0] + input_bias
    log_forget = jax.nn.log_sigmoid(gates[:, 1] + forget_bias) + decay_shift[:, :, 0]
    rows, columns, numbers = on_core(
        gate_kernel,
        (
            jax.ShapeDtypeStruct((4, length), F32),
            jax.ShapeDtypeStruct((length, 8), F32),
            jax.ShapeDtypeStruct((4, 128), F32),
        ),
        log_forget,
        in_gate,
    )
    block, normed, rows, columns, numbers = lax.optimization_barrier(
        (block, normed, rows, columns, numbers)
    )
    up = down = block
    pieces = [block]
    for k in range(4):
        up = lax.ppermute(up, "sp_1", ring(8, 1))
        pieces.append(up)
        if k < 3:
            down = lax.ppermute(down, "sp_1", ring(8, -1))
            pieces.append(down)
    groups, at = [], 0
    for count in GROUPS:
        groups.append(jnp.stack(pieces[at : at + count]))
        at += count
    for count, group in zip(GROUPS, tuple(groups)):
        groups.append(lax.ppermute(group, "sp_2", ring(2, 1)))

    block = jax.ShapeDtypeStruct((members, ROWS, 128), BF16)
    state, keys, values = on_core(
        state_kernel,
        (
            block,
            jax.ShapeDtypeStruct((length, DQK), BF16),
            jax.ShapeDtypeStruct((length, DV), BF16),
        ),
        jnp.stack([core, row]),
        normed,
        columns,
        numbers,
        *groups,
        scalars=1,
        scratch=[pltpu.VMEM((normed.shape[1], DQK + DV), BF16)],
    )
    last, initial, keys = lax.optimization_barrier((normed[-1:], normed[:1], keys))
    state = swapped(state, PLANE)
    before, after = neighbour_rows(last, initial)
    edges = jnp.concatenate([before, after, jnp.zeros((14, normed.shape[1]), BF16)], axis=0)
    near, plane_state = on_core(
        plane_kernel,
        (
            jax.ShapeDtypeStruct((members, ROWS, 128), F32),
            jax.ShapeDtypeStruct((planes, ROWS, 128), BF16),
        ),
        state,
    )
    far = swapped(plane_state, "sp_0")
    queries, conv_out = on_core(
        project_kernel,
        (
            jax.ShapeDtypeStruct((length, DQK), BF16),
            jax.ShapeDtypeStruct((length, DV), BF16),
        ),
        normed,
        edges,
        conv_taps,
        whole,
        remote=1,
        scratch=[
            pltpu.VMEM((CHUNKS, whole.shape[0] // CHUNKS, whole.shape[1]), BF16),
            pltpu.VMEM((length + edges.shape[0], WIDE), F32),
            pltpu.SemaphoreType.DMA((CHUNKS,)),
        ],
        limit=50,
    )
    start = on_core(far_kernel, block, plane[None], near, far, scalars=1)
    start = swapped(start, PLANE)
    local, sums = on_core(
        local_kernel,
        (
            jax.ShapeDtypeStruct((2, length, DV), F32),
            jax.ShapeDtypeStruct((length, 4), F32),
        ),
        queries,
        keys,
        values,
        columns,
        rows,
    )
    start, local, sums = lax.optimization_barrier((start, local, sums))
    joined = on_core(
        read_kernel,
        jax.ShapeDtypeStruct((4, length, 2 * DV), BF16),
        queries,
        local,
        sums,
        columns,
        head_gain[None],
        conv_out,
        start,
    )
    joined = swapped(joined, "tp")
    sides = whole[:, WIDE:].reshape(size, 2, depth, half)
    return on_core(
        output_kernel,
        jax.ShapeDtypeStruct((length, 2 * half), BF16),
        joined,
        *(sides[:, side].reshape(4, 2 * DV, half) for side in range(2)),
    )


def solution(mesh):
    torus = Mesh(mesh.devices.reshape(8, 8, 2, mesh.shape["tp"]), (*SP, "tp"))
    placed = (
        P(SP, None),
        P(),
        P(SP, "tp"),
        P(SP, "tp"),
        P(SP, "tp"),
        P(None, None, None, "tp"),
        P(None, "tp"),
        P(None, "tp"),
        P(None, SP, "tp"),
        P("tp"),
        P(SP, "tp"),
        P(SP, "tp"),
        P(SP, "tp"),
        P(None, "tp"),
        P(SP, "tp"),
    )

    return jax.shard_map(body, mesh=torus, in_specs=placed, out_specs=P(SP, "tp"), check_vma=False)
```
